32 devices in a mesh: sp: 4 (over y, x), tp: 8 (over z, core).
Axes of the slice: x: 2, y: 2, z: 4, core: 2. Of those that a mesh axis runs over, the one named last changes fastest.
Arguments:
- conv_in: bfloat16 [1024, 16384], P('tp', 'sp'), may hold values from -6 to 6
- in_gate: bfloat16 [1024, 16384], P('tp', 'sp'), may hold values from -6 to 6
- out_gate: bfloat16 [1024, 16384], P('tp', 'sp'), may hold values from -6 to 6
- doc_ids: int32 [16384], P('sp'), may hold values from 0 to 1, never falling along the last dimension, each value on 1 to 12288 neighbouring positions
- conv_taps: float32 [1024, 3], P('tp'), may hold values from -3.5 to 3.5
- head_gain: float32 [1024], P('tp'), may hold values from 0.1 to 1.9
- out_proj: bfloat16 [1024, 2048], P('tp'), may hold values from -0.1875 to 0.1875
- resid: bfloat16 [16384, 2048], P(('sp', 'tp')), may hold values from -6 to 6
- norm_gain: float32 [2048], replicated, may hold values from 0.1 to 1.9
- route_ids: int32 [16384, 2], P(('sp', 'tp')), may hold values from 0 to 15, all different within a row; in each aligned block of 256 rows (0 to 255, 256 to 511, ...) at most 64 rows name the same one
- route_weight: float32 [16384, 2], P(('sp', 'tp')), may hold values from 0.1 to 1
- w_gate: bfloat16 [16, 2048, 512], P('sp'), may hold values from -0.125 to 0.125
- w_up: bfloat16 [16, 2048, 512], P('sp'), may hold values from -0.125 to 0.125
- w_down: bfloat16 [16, 512, 2048], P('sp'), may hold values from -0.25 to 0.25
Outputs:
- layer_out: bfloat16 [16384, 2048], P(('sp', 'tp'))
The draws below stay inside these ranges and needn't reach their ends.
Inputs may be any that keep to these rules, and one draw needn't show every extreme that they name: `doc_ids`: document numbers never fall along the sequence; every number from 0 to 1 is used; no document is longer than 12288 positions and one is exactly that long. `route_ids`: each position names 2 different experts. In every aligned block of 256 positions no expert is named by more than 64 positions, a bound that some block reaches.
All inputs are finite; a program needn't handle non-finite values.
Results may differ from the reference program's by a relative error of at most 0.0051.
Values may be sent and summed in bfloat16 or wider, within the bound.
A program may use at most 128 MiB of HBM per device.

```python
import math
import jax
import jax.numpy as jnp
import numpy as np
from jax import lax

D = 2048
HEAD = 64
CONV_CH = 1024
EXPERTS = 16
FF = 512
TOPK = 2
TOK_DEV = 4096
SEQ = 16384
HALF = 256
SLOT = 64
DOCS = 2


def level_of(own_key, dims, split, least, high):
    loudness, own = 1.0, jax.random.fold_in(own_key, 6)
    for axis_at, parts in split:
        draws = jnp.exp(jax.random.uniform(jax.random.fold_in(own, axis_at), (parts,), jnp.float32, least / len(split), high / len(split)))
        loudness = loudness * jnp.repeat(draws, dims[axis_at] // parts).reshape([-1 if axis == axis_at else 1 for axis in range(len(dims))])
    return loudness


def profile(number_of, total, most, skew):
    loads = [(1 << 20) // math.isqrt(grade ** skew) + 1 for grade in range(2, number_of + 1)]
    rest, given = total - most - (number_of - 1), [1] * (number_of - 1)
    while rest > 0:
        candidates = [i for i in range(number_of - 1) if given[i] < most]
        pool, left = sum([loads[i] for i in candidates]), rest
        for i in candidates:
            more = min(most - given[i], max(1, left * loads[i] // pool), rest)
            given[i] = given[i] + more
            rest = rest - more
    return np.array([most] + given)


def ragged_sizes(own_key, count, total, bound, lean):
    if count == 2:
        one = jax.random.randint(own_key, (), max(1, total - bound), min(bound, total - 1) + 1)
        return jnp.stack([one, total - one])
    sizes = jnp.asarray(profile(count, total, bound, lean), jnp.int32)
    twos = (count - 1) // 2
    source_of, receiver = sizes[1:1 + 2 * twos:2], sizes[2:2 + 2 * twos:2]
    room = jnp.minimum(source_of - 1, bound - receiver)
    passed = jax.random.randint(jax.random.fold_in(own_key, 1), (twos,), 0, 1 << 20) % (room + 1)
    sizes = sizes.at[1:1 + 2 * twos:2].set(source_of - passed).at[2:2 + 2 * twos:2].set(receiver + passed)
    return sizes[jax.random.permutation(jax.random.fold_in(own_key, 2), count)]


def assign_block(own_key, own, number, rows, number_of, top, limit, skew):
    ranking = jax.random.permutation(own_key, number_of)
    packed, common = load_shares(number_of, rows * top, limit, skew, True), load_shares(number_of, rows * top, limit, skew, False)
    places = jnp.arange(number_of)

    def named(lengths, offset_by):
        used = int((lengths > 0).sum())
        fixed = max(1, used // 4)
        shifted = fixed + (places - fixed + offset_by * (used - fixed)) % max(1, number_of - fixed)
        return jnp.zeros((number_of,), jnp.int32).at[ranking[jnp.where(places < fixed, places, shifted)]].set(jnp.asarray(lengths, jnp.int32))

    lengths = jnp.where(number % 4 == 0, named(packed, number // 4), named(common, number - number // 4 - 1))
    mixed = jax.random.permutation(jax.random.fold_in(own, 3), number_of)
    source_of, receiver = mixed[0:number_of // 2 * 2:2], mixed[1:number_of // 2 * 2:2]
    slack = jnp.minimum(lengths[source_of] - 1, limit - lengths[receiver]) // 2
    slack = jnp.where((source_of == ranking[0]) | (receiver == ranking[0]) | (lengths[receiver] == 0), 0, jnp.maximum(slack, 0))
    shifted = jax.random.randint(jax.random.fold_in(own, 4), (number_of // 2,), 0, 1 << 20) % (slack + 1)
    lengths = lengths.at[source_of].add(-shifted).at[receiver].add(shifted)
    members = jnp.searchsorted(jnp.cumsum(lengths), jnp.arange(rows * top), side="right").astype(jnp.int32)
    listing = members.reshape(top, rows).T
    listing = listing[jax.random.permutation(jax.random.fold_in(own, 1), rows)]
    offset_by = jax.random.randint(jax.random.fold_in(own, 2), (rows, 1), 0, top)
    return jnp.take_along_axis(listing, (jnp.arange(top)[None, :] + offset_by) % top, axis=1)


def load_shares(number_of, total, reach, skew, full):
    weights = [(1 << 20) // math.isqrt(rank ** skew) + 1 for rank in range(1, number_of + 1)]
    largest = reach if full else min(reach, max(-(-total // number_of), total * weights[0] // sum(weights)))
    least = 1 if total - largest >= number_of - 1 else 0
    counts, rest = [largest] + [least] * (number_of - 1), total - largest - least * (number_of - 1)
    while rest > 0:
        movable = [i for i in range(1, number_of) if counts[i] < largest] or [i for i in range(1, number_of) if counts[i] < reach]
        mass, budget = sum([weights[i] for i in movable]), rest
        for i in movable:
            extra = min(reach - counts[i], max(1, budget * weights[i] // mass), rest)
            counts[i] = counts[i] + extra
            rest = rest - extra
    return np.array(counts)


def centred(stream_key, extent, scale, limit, shards=(), held_as=jnp.bfloat16):
    factor_of = level_of(stream_key, extent, shards, -0.22, 0.18) if shards else 1.0
    values = jax.random.normal(stream_key, extent, jnp.float32) * scale * factor_of
    return jnp.minimum(jnp.maximum(values, -limit), limit).astype(held_as)


def setup_inputs(seed: int = 0) -> dict:
    key_of = jax.random.split(jax.random.key(seed), 15)
    conv_in = centred(key_of[0], (CONV_CH, SEQ), 1.0, 6.0, ((0, 8), (1, 4)))
    in_gate = centred(key_of[1], (CONV_CH, SEQ), 1.0, 6.0, ((0, 8), (1, 4)))
    out_gate = centred(key_of[2], (CONV_CH, SEQ), 1.0, 6.0, ((0, 8), (1, 4)))
    doc_ids = jnp.searchsorted(jnp.cumsum(ragged_sizes(key_of[3], DOCS, SEQ, 3 * TOK_DEV, 0)), jnp.arange(SEQ), side="right").astype(jnp.int32)
    conv_taps = centred(key_of[4], (CONV_CH, 3), 3 ** -0.5, 3.5, ((0, 8),), jnp.float32)
    head_gain = jnp.clip(1.0 + 0.18 * jax.random.normal(key_of[5], (CONV_CH,), jnp.float32), 0.1, 1.9)
    out_proj = centred(key_of[6], (CONV_CH, D), CONV_CH ** -0.5, 0.1875, ((0, 8),))
    resid = centred(key_of[7], (SEQ, D), 1.0, 6.0, ((0, 32),))
    norm_gain = jnp.clip(1.0 + 0.18 * jax.random.normal(key_of[8], (D,), jnp.float32), 0.1, 1.9)
    route_ids_keys = jax.random.split(jax.random.fold_in(key_of[9], 1), SEQ // HALF)
    route_ids_turns = jax.random.permutation(jax.random.fold_in(key_of[9], 3), SEQ // HALF)
    route_ids = jax.vmap(lambda own, number: assign_block(jax.random.fold_in(key_of[9], 2), own, number, HALF, EXPERTS, TOPK, SLOT, 1))(route_ids_keys, route_ids_turns).reshape((SEQ, TOPK))
    route_weight = jnp.clip(0.1 + 0.9 * jax.random.uniform(key_of[10], (SEQ, TOPK), jnp.float32) ** level_of(key_of[10], (SEQ, TOPK), ((0, 32),), -0.2, 0.2), 0.1, 1.0)
    w_gate = centred(key_of[11], (EXPERTS, D, FF), D ** -0.5, 0.125, ((0, 4),))
    w_up = centred(key_of[12], (EXPERTS, D, FF), D ** -0.5, 0.125, ((0, 4),))
    w_down = centred(key_of[13], (EXPERTS, FF, D), FF ** -0.5, 0.25, ((0, 4),))
    return {"conv_in": conv_in, "in_gate": in_gate, "out_gate": out_gate, "doc_ids": doc_ids, "conv_taps": conv_taps, "head_gain": head_gain, "out_proj": out_proj, "resid": resid, "norm_gain": norm_gain, "route_ids": route_ids, "route_weight": route_weight, "w_gate": w_gate, "w_up": w_up, "w_down": w_down}


norm_eps = 1e-06

def reference(conv_in, in_gate, out_gate, doc_ids, conv_taps, head_gain, out_proj, resid, norm_gain, route_ids, route_weight, w_gate, w_up, w_down):
    gated_in = in_gate.astype(jnp.float32) * conv_in.astype(jnp.float32)
    channels = gated_in.shape[0]
    earlier = jnp.concatenate([jnp.full((2,), -1, jnp.int32), doc_ids.astype(jnp.int32)])
    same_one = (earlier[1:-1] == doc_ids).astype(jnp.float32)
    same_two = (earlier[:-2] == doc_ids).astype(jnp.float32)
    padded = jnp.concatenate([jnp.zeros((channels, 2), jnp.float32), gated_in], axis=1)
    conv_out = conv_taps[:, 2:3] * gated_in + conv_taps[:, 1:2] * (padded[:, 1:-1] * same_one) + conv_taps[:, 0:1] * (padded[:, :-2] * same_two)
    gated_out = out_gate.astype(jnp.float32) * conv_out
    by_head = gated_out.reshape(channels // HEAD, HEAD, -1)
    by_head = by_head * lax.rsqrt(lax.optimization_barrier(jnp.mean(by_head * by_head, axis=1, keepdims=True)) + norm_eps)
    head_normed = (by_head.reshape(channels, -1) * head_gain[:, None]).astype(jnp.bfloat16)
    mixed = jnp.dot(head_normed.astype(jnp.float32).T, out_proj.astype(jnp.float32))
    stream = resid.astype(jnp.float32) + mixed
    expert_in = (stream * lax.rsqrt(lax.optimization_barrier(jnp.mean(stream * stream, axis=1, keepdims=True)) + norm_eps) * norm_gain).astype(jnp.bfloat16)
    flat_ids = route_ids.reshape(-1).astype(jnp.int32)
    flat_tok = (jnp.arange(flat_ids.shape[0], dtype=jnp.int32) // TOPK).astype(jnp.int32)
    flat_weight = route_weight.reshape(-1)
    most_rows = min(SEQ, SLOT * (SEQ // HALF))

    def one_expert(totals, inputs):
        gate_mat, up_mat, down_mat, number = inputs
        ranked = jnp.argsort((flat_ids != number).astype(jnp.int32), stable=True)[:most_rows]
        picked = flat_tok[ranked]
        weight = jnp.where(flat_ids[ranked] == number, flat_weight[ranked], jnp.zeros_like(flat_weight[ranked]))
        sel_rows = expert_in[picked].astype(jnp.float32)
        gate_part = jnp.dot(sel_rows, gate_mat.astype(jnp.float32))
        up_part = jnp.dot(sel_rows, up_mat.astype(jnp.float32))
        hidden = (jax.nn.silu(gate_part) * up_part).astype(jnp.bfloat16)
        expert_out = jnp.dot(hidden.astype(jnp.float32), down_mat.astype(jnp.float32)).astype(jnp.bfloat16)
        return (totals.at[picked].add(expert_out.astype(jnp.float32) * weight[:, None]), None)
    totals, _ = lax.scan(one_expert, jnp.zeros(stream.shape, jnp.float32), (w_gate, w_up, w_down, jnp.arange(EXPERTS, dtype=jnp.int32)))
    return (stream + totals).astype(jnp.bfloat16)
```

```python
import functools

import jax
import jax.numpy as jnp
from jax import lax
from jax.experimental import pallas as pl
from jax.experimental.pallas import tpu as pltpu
from jax.sharding import PartitionSpec as P

HEAD = 64


norm_eps = 1e-06


def shifted(value, axis, steps):
    count = lax.axis_size(axis)
    leading, last = (max(0, -steps), min(count, count - steps))
    return lax.ppermute(value, axis, [(source, source + steps) for source in range(leading, last)])


def slot_places(ids_block, slot, experts):
    flat = ids_block.reshape(-1)
    marks = (flat[:, None] == jnp.arange(experts, dtype=jnp.int32)[None, :]).astype(jnp.int32)
    before = jnp.sum((jnp.cumsum(marks, axis=0) - 1) * marks, axis=1)
    return (flat * slot + before).reshape(ids_block.shape)


def pack_rows(places, normed_rows, total_slots):
    targets = jnp.arange(total_slots, dtype=jnp.int32)
    table = jnp.any(targets[:, None, None] == places[None, :, :], axis=2).astype(jnp.bfloat16)
    return jnp.dot(table, normed_rows, preferred_element_type=jnp.float32).astype(jnp.bfloat16)


def combine_rows(returned, places, weights):
    totals = jnp.zeros((places.shape[0], returned.shape[1]), jnp.float32)
    for choice_k in range(places.shape[1]):
        totals = totals + weights[:, choice_k : choice_k + 1] * returned[
            places[:, choice_k]
        ].astype(jnp.float32)
    return totals


def neighbour(value, bit):
    count = lax.axis_size("sp")
    return lax.ppermute(value, "sp", [(source, source ^ bit) for source in range(count)])


def gather_near(value):
    return value, neighbour(value, 1), neighbour(value, 2)


def gather_far(value, from_one, from_two):
    middle = value.shape[0] // 2
    low = neighbour(from_one[:middle], 2)
    high = neighbour(from_two[middle:], 1)
    return [value, from_one, from_two, jnp.concatenate([low, high], axis=0)]


def scatter_four(parts):
    middle = parts[3].shape[0] // 2
    low = neighbour(parts[3][:middle], 1)
    high = neighbour(parts[3][middle:], 2)
    straight = neighbour(parts[1][:middle], 1), neighbour(parts[2][middle:], 2)
    return straight, (add(parts[1][middle:], high), add(parts[2][:middle], low))


def scatter_rest(straight, joined):
    one = jnp.concatenate([straight[0], neighbour(joined[0], 1)], axis=0)
    two = jnp.concatenate([neighbour(joined[1], 2), straight[1]], axis=0)
    return one, two


def add(left, right):
    return (left.astype(jnp.float32) + right.astype(jnp.float32)).astype(jnp.bfloat16)


def route_tables(ids, weights, local_experts, half, slot):
    me = lax.axis_index("sp")
    top = ids.shape[1]
    ids = ids.reshape(4, top, -1, half)
    weights = weights.reshape(4, top, -1, half)
    experts = me * local_experts + jnp.arange(local_experts, dtype=jnp.int32)
    hit = ids[:, :, :, None, :] == experts[None, None, None, :, None]
    marks = jnp.any(hit, axis=1)
    weight_of = jnp.sum(jnp.where(hit, weights[:, :, :, None], 0.0), axis=1)
    earlier = (
        jnp.arange(half)[:, None] < jnp.arange(half)[None, :]
    ).astype(jnp.bfloat16)
    rank = jnp.dot(
        marks.astype(jnp.bfloat16).reshape(-1, half), earlier, preferred_element_type=jnp.float32
    ).reshape(marks.shape)
    rank = jnp.where(marks, rank.astype(jnp.int32), -1)
    chosen = rank[:, :, :, None, :] == jnp.arange(slot, dtype=jnp.int32)[None, None, None, :, None]
    slot_weight = jnp.sum(jnp.where(chosen, weight_of[:, :, :, None, :], 0.0), axis=4)
    return chosen.astype(jnp.bfloat16), slot_weight


def experts_on(rows, table, slot_weight, w_gate, w_up, w_down, held, late):
    sources, local_experts, slot, half = table.shape
    width = rows.shape[2]
    packed = jnp.einsum("nest,ntd->ensd", table, rows, preferred_element_type=jnp.float32)
    packed = packed.astype(jnp.bfloat16).reshape(local_experts, sources * slot, width)
    gate_part = jnp.einsum("emd,edf->emf", packed, w_gate, preferred_element_type=jnp.float32)
    up_part = jnp.einsum("emd,edf->emf", packed, w_up, preferred_element_type=jnp.float32)
    hidden = (jax.nn.silu(gate_part) * up_part).astype(jnp.bfloat16)
    if late:
        hidden = lax.optimization_barrier(hidden)
    else:
        hidden, held = lax.optimization_barrier((hidden, held))
    down = jnp.einsum("emf,efd->emd", hidden, w_down, preferred_element_type=jnp.float32)
    scale = jnp.transpose(slot_weight, (1, 0, 2)).reshape(local_experts, sources * slot, 1)
    down = (down * scale).astype(jnp.bfloat16).reshape(local_experts, sources, slot, width)
    if late:
        down, held = lax.optimization_barrier((down, held))
    total = jnp.einsum("nest,ensd->ntd", table, down, preferred_element_type=jnp.float32)
    return total.astype(jnp.bfloat16), held


MESH = pl.DeviceIdType.MESH
SUB = 128


def front_kernel(
    tp_count,
    conv_in,
    in_gate,
    out_gate,
    doc_ids,
    taps_in,
    gain_in,
    out_proj,
    resid,
    norm_gain_in,
    ids,
    weights,
    rows_out,
    later_out,
    stream_out,
    ids_out,
    weights_out,
    in_buf,
    gate_buf,
    after_buf,
    doc_buf,
    taps,
    gain,
    norm_gain,
    proj,
    resid_buf,
    spread,
    outgoing,
    by_row,
    gathered,
    later,
    stream,
    local_sem,
    out_sem,
    edge_send,
    edge_recv,
    list_send,
    list_recv,
    slice_send,
    slice_recv,
    plane_send,
    plane_recv,
    corner_send,
    corner_recv,
    core_send,
    core_recv,
    trade_send,
    trade_recv,
    near_send,
    near_recv,
    far_send,
    far_recv,
):
    sp, tp = lax.axis_index("sp"), lax.axis_index("tp")
    z, core = tp // 2, tp % 2
    channels, width = out_proj.shape
    rows = resid.shape[0]
    half, subs = rows // 2, rows // SUB
    first = half // SUB
    planes = tp_count // 2
    near_of = [sp ^ 1, sp ^ 2]
    diagonal = sp ^ 3
    pending = []

    def remote(source, target, send_sem, recv_sem, to_sp, to_tp):
        return pltpu.make_async_remote_copy(
            src_ref=source,
            dst_ref=target,
            send_sem=send_sem,
            recv_sem=recv_sem,
            device_id=(to_sp, to_tp),
            device_id_type=MESH,
        )

    def send(source, target, send_sem, recv_sem, to_sp, to_tp):
        copy = remote(source, target, send_sem, recv_sem, to_sp, to_tp)
        copy.start()
        pending.append(copy)

    def arrive(region, send_sem, recv_sem):
        remote(region, region, send_sem, recv_sem, near_of[0], tp).wait_recv()

    tail = conv_in.shape[1] - SUB
    loads = [
        pltpu.make_async_copy(conv_in, in_buf.at[:, pl.ds(SUB, conv_in.shape[1])], local_sem.at[0]),
        pltpu.make_async_copy(in_gate, gate_buf.at[:, pl.ds(SUB, conv_in.shape[1])], local_sem.at[1]),
        pltpu.make_async_copy(out_gate, after_buf, local_sem.at[2]),
        pltpu.make_async_copy(doc_ids, doc_buf.at[:, pl.ds(SUB, conv_in.shape[1])], local_sem.at[3]),
        pltpu.make_async_copy(taps_in, taps, local_sem.at[6]),
        pltpu.make_async_copy(gain_in, gain, local_sem.at[7]),
        pltpu.make_async_copy(
            out_proj, proj.at[pl.ds(pl.multiple_of(tp * channels, channels), channels)], local_sem.at[4]
        ),
        pltpu.make_async_copy(resid, resid_buf, local_sem.at[5]),
        pltpu.make_async_copy(norm_gain_in, norm_gain, local_sem.at[8]),
        pltpu.make_async_copy(ids, ids_out.at[0], local_sem.at[9]),
        pltpu.make_async_copy(weights, weights_out.at[0], local_sem.at[10]),
    ]
    for copy in loads:
        copy.start()

    barrier = pltpu.get_barrier_semaphore()
    for d in range(1, tp_count):
        pl.semaphore_signal(barrier, inc=1, device_id=(sp, tp ^ d), device_id_type=MESH)
    for d in range(1, 4):
        pl.semaphore_signal(barrier, inc=1, device_id=(sp ^ d, tp), device_id_type=MESH)
    pl.semaphore_wait(barrier, tp_count + 2)

    after, before = (sp + 1) % 4, (sp + 3) % 4
    edge = pl.ds(0, SUB)
    for at, (source, target) in enumerate(
        ((conv_in, in_buf), (in_gate, gate_buf), (doc_ids, doc_buf))
    ):
        send(
            source.at[:, pl.ds(tail, SUB)],
            target.at[:, edge],
            edge_send.at[at],
            edge_recv.at[at],
            after,
            tp,
        )

    eighth = width // 8

    def columns(place, side):
        return pl.ds(pl.multiple_of(place * (2 * eighth) + side * eighth, eighth), eighth)

    my_rows = pl.ds(pl.multiple_of(tp * channels, channels), channels)
    slices = []
    for d in range(2, tp_count):
        side = core ^ (d & 1)
        copy = remote(
            out_proj.at[:, columns(sp, side)],
            proj.at[my_rows, columns(sp, side)],
            slice_send.at[d],
            slice_recv.at[d],
            sp,
            tp ^ d,
        )
        copy.start()
        slices.append(copy)
    send(out_proj, proj.at[my_rows], slice_send.at[1], slice_recv.at[1], sp, tp ^ 1)
    for d in range(1, 4):
        send(ids, ids_out.at[d], list_send.at[0, d], list_recv.at[0, d], sp ^ d, tp)
        send(weights, weights_out.at[d], list_send.at[1, d], list_recv.at[1, d], sp ^ d, tp)
    for copy in loads[:6]:
        copy.wait()
    for k in range(3):
        spread[k] = jnp.broadcast_to(taps[k : k + 1, :], (channels, channels)).T
    spread[3] = jnp.broadcast_to(gain[...], (channels, channels)).T
    def piece(owner, q):
        base = pl.multiple_of(owner * rows + q * SUB, SUB)
        wide = pl.ds(base, 2 * SUB)
        gated = gate_buf[:, wide].astype(jnp.float32) * in_buf[:, wide].astype(jnp.float32)
        docs = jnp.broadcast_to(doc_buf[:, wide], (8, 2 * SUB))
        now = docs[:, SUB:]
        same_one = (pltpu.roll(docs, 1, 1)[:, SUB:] == now).astype(jnp.float32)[:1]
        same_two = (pltpu.roll(docs, 2, 1)[:, SUB:] == now).astype(jnp.float32)[:1]
        conv = (
            spread[2] * gated[:, SUB:]
            + spread[1] * (pltpu.roll(gated, 1, 1)[:, SUB:] * same_one)
            + spread[0] * (pltpu.roll(gated, 2, 1)[:, SUB:] * same_two)
        )
        gated_out = after_buf[:, pl.ds(base, SUB)].astype(jnp.float32) * conv
        by_head = gated_out.reshape(channels // HEAD, HEAD, SUB)
        by_head = by_head * lax.rsqrt(
            jnp.mean(by_head * by_head, axis=1, keepdims=True) + norm_eps
        )
        normed = by_head.reshape(channels, SUB) * spread[3]
        return normed.T.astype(jnp.bfloat16)

    my_channels = pl.ds(pl.multiple_of(tp * channels, channels), channels)

    def trade(q, d):
        return remote(
            outgoing.at[q, d],
            by_row.at[q, :, my_channels],
            trade_send.at[q, d],
            trade_recv.at[q, d],
            sp,
            tp ^ d,
        )

    def start_trade(q):
        def begin(at, carry):
            trade(q, tp_count - 1 - at).start()
            return carry

        lax.fori_loop(0, tp_count - 1, begin, 0)

    def sent_trade(q):
        def sent(d, carry):
            trade(q, d).wait_send()
            return carry

        lax.fori_loop(1, tp_count, sent, 0)

    def block_rows(step):
        deep = 2 * channels
        return pl.ds(pl.multiple_of((z ^ step) * deep, deep), deep)

    def part_rows(step, upper):
        deep = 2 * channels
        return pl.ds(pl.multiple_of((z ^ step) * deep + upper * channels, channels), channels)

    def spread_slice(step):
        arrive_rows = [
            pl.ds(pl.multiple_of((tp ^ (2 * step + odd)) * channels, channels), channels)
            for odd in range(2)
        ]
        for odd in range(2):
            d = 2 * step + odd
            arrive(
                proj.at[arrive_rows[odd], columns(sp, core)], slice_send.at[d], slice_recv.at[d]
            )
        region = proj.at[block_rows(step), columns(sp, core)]
        for k in range(2):
            send(region, region, plane_send.at[k, step], plane_recv.at[k, step], near_of[k], tp)
        send(region, region, core_send.at[0, step], core_recv.at[0, step], sp, tp ^ 1)

    def spread_plane(step):
        for k in range(2):
            region = proj.at[block_rows(step), columns(near_of[k], core)]
            arrive(region, plane_send.at[k, step], plane_recv.at[k, step])
            part = proj.at[part_rows(step, k), columns(near_of[k], core)]
            send(part, part, corner_send.at[k, step], corner_recv.at[k, step], near_of[1 - k], tp)
            send(region, region, core_send.at[1 + k, step], core_recv.at[1 + k, step], sp, tp ^ 1)

    def spread_corner(step):
        for k in range(2):
            arrive(
                proj.at[part_rows(step, k), columns(diagonal, core)],
                corner_send.at[k, step],
                corner_recv.at[k, step],
            )
        region = proj.at[block_rows(step), columns(diagonal, core)]
        send(region, region, core_send.at[3, step], core_recv.at[3, step], sp, tp ^ 1)

    def others_done(step):
        other = 1 - core
        for k, place in enumerate((sp, near_of[0], near_of[1], diagonal)):
            arrive(
                proj.at[block_rows(step), columns(place, other)],
                core_send.at[k, step],
                core_recv.at[k, step],
            )

    order = [1, 0, *range(2, subs)]

    def convolve(q):
        def one(at, carry):
            d = tp_count - 1 - at
            outgoing[q, d] = piece(tp ^ d, q)
            return carry

        lax.fori_loop(0, tp_count - 1, one, 0)
        by_row[q, :, my_channels] = piece(tp, q)

    for q in range(1, subs):
        convolve(q)
    for step in range(1, planes):
        if step == planes - 1:
            for copy in slices:
                copy.wait_send()
            start_trade(order[0])
        spread_slice(step)
    for step in range(1, planes):
        spread_plane(step)
    for at, target in enumerate((in_buf, gate_buf, doc_buf)):
        arrive(target.at[:, edge], edge_send.at[at], edge_recv.at[at])
    doc_buf[:, edge] = jnp.where(sp == 0, -1, doc_buf[:, edge])
    convolve(0)
    for step in range(1, planes):
        spread_corner(step)
    sent_trade(order[0])
    start_trade(order[1])
    for copy in loads[6:]:
        copy.wait()
    arrive(
        proj.at[pl.ds(pl.multiple_of((tp ^ 1) * channels, channels), channels)],
        slice_send.at[1],
        slice_recv.at[1],
    )
    for step in range(1, planes):
        others_done(step)

    tile = width // 4
    stores = []
    for at_q, q in enumerate(order):
        if at_q > 0:
            sent_trade(q)
            if at_q + 1 < subs:
                start_trade(order[at_q + 1])

        def got(d, carry, q=q):
            theirs = pl.ds(pl.multiple_of((tp ^ d) * channels, channels), channels)
            arrive(by_row.at[q, :, theirs], trade_send.at[q, d], trade_recv.at[q, d])
            return carry

        lax.fori_loop(1, tp_count, got, 0)
        mine = pl.ds(q * SUB, SUB)

        def project(n, total, q=q, mine=mine):
            cols = pl.ds(pl.multiple_of(n * tile, tile), tile)
            value = resid_buf[mine, cols].astype(jnp.float32) + jnp.dot(
                by_row[q], proj[:, cols], preferred_element_type=jnp.float32
            )
            stream[mine, cols] = value
            return total + jnp.sum(value * value, axis=1, keepdims=True)

        total = lax.fori_loop(0, 4, project, jnp.zeros((SUB, 1), jnp.float32))
        scale = lax.rsqrt(total / width + norm_eps)

        def normalize(n, carry, q=q, mine=mine, scale=scale):
            cols = pl.ds(pl.multiple_of(n * tile, tile), tile)
            value = (stream[mine, cols] * scale * norm_gain[:, cols]).astype(jnp.bfloat16)
            if q < first:
                gathered[0, mine, cols] = value
            else:
                later[pl.ds((q - first) * SUB, SUB), cols] = value
            return carry

        lax.fori_loop(0, 4, normalize, 0)
        if q < first:
            region = gathered.at[0, mine]
            for k in range(2):
                send(
                    region,
                    gathered.at[1 + k, mine],
                    near_send.at[k, q],
                    near_recv.at[k, q],
                    near_of[k],
                    tp,
                )
    stores.append(pltpu.make_async_copy(stream, stream_out, out_sem.at[0]))
    stores.append(pltpu.make_async_copy(later, later_out, out_sem.at[1]))
    stores.append(pltpu.make_async_copy(gathered.at[0], rows_out.at[0], out_sem.at[2]))
    for copy in stores:
        copy.start()
    for d in range(1, 4):
        arrive(ids_out.at[d], list_send.at[0, d], list_recv.at[0, d])
        arrive(weights_out.at[d], list_send.at[1, d], list_recv.at[1, d])

    for q in range(first):
        for k in range(2):
            arrive(
                gathered.at[1 + k, pl.ds(q * SUB, SUB)], near_send.at[k, q], near_recv.at[k, q]
            )
            part = pl.ds(q * SUB + k * (SUB // 2), SUB // 2)
            send(
                gathered.at[1 + k, part],
                gathered.at[3, part],
                far_send.at[k, q],
                far_recv.at[k, q],
                near_of[1 - k],
                tp,
            )
    for k in range(2):
        store = pltpu.make_async_copy(gathered.at[1 + k], rows_out.at[1 + k], out_sem.at[3 + k])
        store.start()
        stores.append(store)
    for q in range(first):
        for k in range(2):
            part = pl.ds(q * SUB + k * (SUB // 2), SUB // 2)
            arrive(gathered.at[3, part], far_send.at[k, q], far_recv.at[k, q])
        store = pltpu.make_async_copy(
            gathered.at[3, pl.ds(q * SUB, SUB)],
            rows_out.at[3, pl.ds(q * SUB, SUB)],
            out_sem.at[5 + q],
        )
        store.start()
        stores.append(store)
    for copy in stores:
        copy.wait()
    for copy in pending:
        copy.wait_send()


def front(
    conv_in, in_gate, out_gate, doc_ids, conv_taps, head_gain, out_proj, resid, norm_gain,
    route_ids, route_weight,
):
    tp_count = lax.axis_size("tp")
    channels, width = out_proj.shape
    positions = conv_in.shape[1]
    rows = resid.shape[0]
    half, subs = rows // 2, rows // SUB
    first, planes = half // SUB, tp_count // 2
    top = route_ids.shape[1]
    hbm = pl.BlockSpec(memory_space=pltpu.HBM)
    vmem = pl.BlockSpec(memory_space=pltpu.VMEM)
    dma = pltpu.SemaphoreType.DMA
    return pl.pallas_call(
        functools.partial(front_kernel, tp_count),
        out_shape=(
            jax.ShapeDtypeStruct((4, half, width), jnp.bfloat16),
            jax.ShapeDtypeStruct((half, width), jnp.bfloat16),
            jax.ShapeDtypeStruct((rows, width), jnp.float32),
            jax.ShapeDtypeStruct((4, top, rows), jnp.int32),
            jax.ShapeDtypeStruct((4, top, rows), jnp.float32),
        ),
        in_specs=[hbm] * 11,
        out_specs=(hbm, hbm, hbm, vmem, vmem),
        scratch_shapes=[
            pltpu.VMEM((channels, SUB + positions), jnp.bfloat16),
            pltpu.VMEM((channels, SUB + positions), jnp.bfloat16),
            pltpu.VMEM((channels, positions), jnp.bfloat16),
            pltpu.VMEM((1, SUB + positions), jnp.int32),
            pltpu.VMEM((3, channels), jnp.float32),
            pltpu.VMEM((1, channels), jnp.float32),
            pltpu.VMEM((1, width), jnp.float32),
            pltpu.VMEM((tp_count * channels, width), jnp.bfloat16),
            pltpu.VMEM((rows, width), jnp.bfloat16),
            pltpu.VMEM((4, channels, SUB), jnp.float32),
            pltpu.VMEM((subs, tp_count, SUB, channels), jnp.bfloat16),
            pltpu.VMEM((subs, SUB, tp_count * channels), jnp.bfloat16),
            pltpu.VMEM((4, half, width), jnp.bfloat16),
            pltpu.VMEM((half, width), jnp.bfloat16),
            pltpu.VMEM((rows, width), jnp.float32),
            dma((11,)),
            dma((5 + first,)),
            dma((3,)),
            dma((3,)),
            dma((2, 4)),
            dma((2, 4)),
            dma((tp_count,)),
            dma((tp_count,)),
            dma((2, planes)),
            dma((2, planes)),
            dma((2, planes)),
            dma((2, planes)),
            dma((4, planes)),
            dma((4, planes)),
            dma((subs, tp_count)),
            dma((subs, tp_count)),
            dma((2, first)),
            dma((2, first)),
            dma((2, first)),
            dma((2, first)),
        ],
        compiler_params=pltpu.CompilerParams(
            collective_id=0, has_side_effects=True, vmem_limit_bytes=60 * 1024 * 1024
        ),
        name="front",
    )(
        conv_in,
        in_gate,
        out_gate,
        doc_ids[None],
        conv_taps.T,
        head_gain[None],
        out_proj,
        resid,
        norm_gain[None],
        route_ids.T,
        route_weight.T,
    )


def body(
    conv_in,
    in_gate,
    out_gate,
    doc_ids,
    conv_taps,
    head_gain,
    out_proj,
    resid,
    norm_gain,
    route_ids,
    route_weight,
    w_gate,
    w_up,
    w_down,
):
    channels, width = out_proj.shape
    rows = resid.shape[0]
    half = rows // 2
    slot = max(2, rows // 8)
    sp_count, tp_count = lax.axis_size("sp"), lax.axis_size("tp")
    local_experts = w_gate.shape[0]
    if (
        sp_count == 4
        and tp_count >= 4
        and tp_count & (tp_count - 1) == 0
        and channels == SUB
        and channels % HEAD == 0
        and width % 1024 == 0
        and rows % (2 * SUB) == 0
        and conv_in.shape[1] == tp_count * rows
        and rows <= 2 * local_experts * slot
    ):
        rows_of, later, stream, ids, weights = front(
            conv_in,
            in_gate,
            out_gate,
            doc_ids,
            conv_taps,
            head_gain,
            out_proj,
            resid,
            norm_gain,
            route_ids,
            route_weight,
        )
        tables, slot_weights = route_tables(ids, weights, local_experts, half, slot)
        held = gather_near(later)
        partials, sent = [], []
        for block_no in range(2):
            partial, held = experts_on(
                rows_of,
                tables[:, block_no],
                slot_weights[:, block_no],
                w_gate,
                w_up,
                w_down,
                held,
                block_no > 0,
            )
            if block_no == 0:
                rows_of = jnp.stack(gather_far(*held))
            else:
                sent.append(scatter_rest(*held))
            partials.append(partial[0])
            held = scatter_four([partial[distance] for distance in range(4)])
        sent.append(scatter_rest(*held))
        totals = []
        for block_no in range(2):
            one, two = sent[block_no]
            own = stream[block_no * half : (block_no + 1) * half]
            own = own + partials[block_no].astype(jnp.float32)
            totals.append(own + one.astype(jnp.float32) + two.astype(jnp.float32))
        return jnp.concatenate(totals, axis=0).astype(jnp.bfloat16)
    gated_in = in_gate.astype(jnp.float32) * conv_in.astype(jnp.float32)
    doc_value = doc_ids.astype(jnp.float32)
    edge = jnp.concatenate([gated_in[:, -2:], doc_value[None, -2:]], axis=0)
    edge = shifted(edge, "sp", 1)
    earlier_in, earlier_doc = edge[:-1], edge[-1]
    padded_in = jnp.concatenate([earlier_in, gated_in], axis=1)
    padded_doc = jnp.concatenate([earlier_doc, doc_value])
    same_one = (padded_doc[1:-1] == doc_value).astype(jnp.float32)
    same_two = (padded_doc[:-2] == doc_value).astype(jnp.float32)
    conv_out = (
        conv_taps[:, 2:3] * gated_in
        + conv_taps[:, 1:2] * (padded_in[:, 1:-1] * same_one)
        + conv_taps[:, 0:1] * (padded_in[:, :-2] * same_two)
    )
    gated_out = out_gate.astype(jnp.float32) * conv_out
    by_head = gated_out.reshape(channels // HEAD, HEAD, -1)
    by_head = by_head * lax.rsqrt(jnp.mean(by_head * by_head, axis=1, keepdims=True) + norm_eps)
    head_normed = (by_head.reshape(channels, -1) * head_gain[:, None]).astype(jnp.bfloat16)
    by_row = lax.all_to_all(head_normed, "tp", split_axis=1, concat_axis=0, tiled=True)
    mixed = lax.dot_general(
        by_row,
        lax.all_gather(out_proj, "tp", axis=0, tiled=True),
        (((0,), (0,)), ((), ())),
        preferred_element_type=jnp.float32,
    )
    stream = resid.astype(jnp.float32) + mixed
    expert_in = (
        stream * lax.rsqrt(jnp.mean(stream * stream, axis=1, keepdims=True) + norm_eps) * norm_gain
    ).astype(jnp.bfloat16)
    experts_total = local_experts * sp_count
    parts = []
    for block_no in range(2):
        block_ids = route_ids[block_no * half : (block_no + 1) * half]
        place = slot_places(block_ids, slot, experts_total)
        send = pack_rows(
            place, expert_in[block_no * half : (block_no + 1) * half], experts_total * slot
        ).reshape(sp_count, local_experts, slot, width)
        arrived = lax.all_to_all(send, "sp", split_axis=0, concat_axis=0, tiled=True)
        gate_part = jnp.einsum(
            "nesd,edf->nesf", arrived, w_gate, preferred_element_type=jnp.float32
        )
        up_part = jnp.einsum("nesd,edf->nesf", arrived, w_up, preferred_element_type=jnp.float32)
        hidden = (jax.nn.silu(gate_part) * up_part).astype(jnp.bfloat16)
        arrived = jnp.einsum(
            "nesf,efd->nesd", hidden, w_down, preferred_element_type=jnp.float32
        ).astype(jnp.bfloat16)
        returned = lax.all_to_all(arrived, "sp", split_axis=0, concat_axis=0, tiled=True).reshape(
            experts_total * slot, width
        )
        parts.append(
            combine_rows(returned, place, route_weight[block_no * half : (block_no + 1) * half])
        )
    mixture = jnp.concatenate(parts, axis=0)
    return (stream + mixture).astype(jnp.bfloat16)


def solution(mesh):
    return jax.shard_map(
        body,
        mesh=mesh,
        in_specs=(
            P("tp", "sp"),
            P("tp", "sp"),
            P("tp", "sp"),
            P("sp"),
            P("tp", None),
            P("tp"),
            P("tp", None),
            P(("sp", "tp"), None),
            P(),
            P(("sp", "tp"), None),
            P(("sp", "tp"), None),
            P("sp", None, None),
            P("sp", None, None),
            P("sp", None, None),
        ),
        out_specs=P(("sp", "tp"), None),
        check_vma=False,
    )
```

```python
import functools

import jax
import jax.numpy as jnp
from jax import lax
from jax.experimental import pallas as pl
from jax.experimental.pallas import tpu as pltpu
from jax.sharding import PartitionSpec as P

HEAD = 64


norm_eps = 1e-06


def shifted(value, axis, steps):
    count = lax.axis_size(axis)
    leading, last = (max(0, -steps), min(count, count - steps))
    return lax.ppermute(value, axis, [(source, source + steps) for source in range(leading, last)])


def slot_places(ids_block, slot, experts):
    flat = ids_block.reshape(-1)
    marks = (flat[:, None] == jnp.arange(experts, dtype=jnp.int32)[None, :]).astype(jnp.int32)
    before = jnp.sum((jnp.cumsum(marks, axis=0) - 1) * marks, axis=1)
    return (flat * slot + before).reshape(ids_block.shape)


def pack_rows(places, normed_rows, total_slots):
    targets = jnp.arange(total_slots, dtype=jnp.int32)
    table = jnp.any(targets[:, None, None] == places[None, :, :], axis=2).astype(jnp.bfloat16)
    return jnp.dot(table, normed_rows, preferred_element_type=jnp.float32).astype(jnp.bfloat16)


def combine_rows(returned, places, weights):
    totals = jnp.zeros((places.shape[0], returned.shape[1]), jnp.float32)
    for choice_k in range(places.shape[1]):
        totals = totals + weights[:, choice_k : choice_k + 1] * returned[
            places[:, choice_k]
        ].astype(jnp.float32)
    return totals


MESH = pl.DeviceIdType.MESH
SUB = 128


def front_kernel(
    tp_count,
    conv_in,
    in_gate,
    out_gate,
    doc_ids,
    taps_in,
    gain_in,
    out_proj,
    resid,
    norm_gain_in,
    ids,
    weights,
    w_gate,
    w_up,
    w_down,
    out_low,
    out_high,
    ids_out,
    weights_out,
    in_buf,
    gate_buf,
    after_buf,
    doc_buf,
    taps,
    gain,
    norm_gain,
    proj,
    resid_buf,
    spread,
    outgoing,
    by_row,
    gathered,
    stream,
    gate_now,
    up_now,
    down_now,
    marks,
    share,
    rank,
    table,
    slot_weight,
    packed,
    hidden,
    partial,
    inbox,
    back,
    local_sem,
    edge_send,
    edge_recv,
    list_send,
    list_recv,
    slice_send,
    slice_recv,
    plane_send,
    plane_recv,
    corner_send,
    corner_recv,
    core_send,
    core_recv,
    trade_send,
    trade_recv,
    near_send,
    near_recv,
    far_send,
    far_recv,
    weight_sem,
    first_send,
    first_recv,
    straight_send,
    straight_recv,
    merged_send,
    merged_recv,
):
    sp, tp = lax.axis_index("sp"), lax.axis_index("tp")
    z, core = tp // 2, tp % 2
    channels, width = out_proj.shape
    rows = resid.shape[0]
    half, subs = rows // 2, rows // SUB
    first = half // SUB
    planes = tp_count // 2
    near_of = [sp ^ 1, sp ^ 2]
    diagonal = sp ^ 3
    pending = []

    def remote(source, target, send_sem, recv_sem, to_sp, to_tp):
        return pltpu.make_async_remote_copy(
            src_ref=source,
            dst_ref=target,
            send_sem=send_sem,
            recv_sem=recv_sem,
            device_id=(to_sp, to_tp),
            device_id_type=MESH,
        )

    def send(source, target, send_sem, recv_sem, to_sp, to_tp):
        copy = remote(source, target, send_sem, recv_sem, to_sp, to_tp)
        copy.start()
        pending.append(copy)

    def arrive(region, send_sem, recv_sem):
        remote(region, region, send_sem, recv_sem, near_of[0], tp).wait_recv()

    tail = conv_in.shape[1] - SUB
    loads = [
        pltpu.make_async_copy(conv_in, in_buf.at[:, pl.ds(SUB, conv_in.shape[1])], local_sem.at[0]),
        pltpu.make_async_copy(in_gate, gate_buf.at[:, pl.ds(SUB, conv_in.shape[1])], local_sem.at[1]),
        pltpu.make_async_copy(out_gate, after_buf, local_sem.at[2]),
        pltpu.make_async_copy(doc_ids, doc_buf.at[:, pl.ds(SUB, conv_in.shape[1])], local_sem.at[3]),
        pltpu.make_async_copy(taps_in, taps, local_sem.at[6]),
        pltpu.make_async_copy(gain_in, gain, local_sem.at[7]),
        pltpu.make_async_copy(
            out_proj, proj.at[pl.ds(pl.multiple_of(tp * channels, channels), channels)], local_sem.at[4]
        ),
        pltpu.make_async_copy(resid, resid_buf, local_sem.at[5]),
        pltpu.make_async_copy(norm_gain_in, norm_gain, local_sem.at[8]),
        pltpu.make_async_copy(ids, ids_out.at[0], local_sem.at[9]),
        pltpu.make_async_copy(weights, weights_out.at[0], local_sem.at[10]),
    ]
    for copy in loads:
        copy.start()

    barrier = pltpu.get_barrier_semaphore()
    for d in range(1, tp_count):
        pl.semaphore_signal(barrier, inc=1, device_id=(sp, tp ^ d), device_id_type=MESH)
    for d in range(1, 4):
        pl.semaphore_signal(barrier, inc=1, device_id=(sp ^ d, tp), device_id_type=MESH)
    pl.semaphore_wait(barrier, tp_count + 2)

    after, before = (sp + 1) % 4, (sp + 3) % 4
    edge = pl.ds(0, SUB)
    for at, (source, target) in enumerate(
        ((conv_in, in_buf), (in_gate, gate_buf), (doc_ids, doc_buf))
    ):
        send(
            source.at[:, pl.ds(tail, SUB)],
            target.at[:, edge],
            edge_send.at[at],
            edge_recv.at[at],
            after,
            tp,
        )

    eighth = width // 8

    def columns(place, side):
        return pl.ds(pl.multiple_of(place * (2 * eighth) + side * eighth, eighth), eighth)

    my_rows = pl.ds(pl.multiple_of(tp * channels, channels), channels)
    slices = []
    for d in range(2, tp_count):
        side = core ^ (d & 1)
        copy = remote(
            out_proj.at[:, columns(sp, side)],
            proj.at[my_rows, columns(sp, side)],
            slice_send.at[d],
            slice_recv.at[d],
            sp,
            tp ^ d,
        )
        copy.start()
        slices.append(copy)
    send(out_proj, proj.at[my_rows], slice_send.at[1], slice_recv.at[1], sp, tp ^ 1)
    for d in range(1, 4):
        send(ids, ids_out.at[d], list_send.at[0, d], list_recv.at[0, d], sp ^ d, tp)
        send(weights, weights_out.at[d], list_send.at[1, d], list_recv.at[1, d], sp ^ d, tp)
    for copy in loads[:6]:
        copy.wait()
    for k in range(3):
        spread[k] = jnp.broadcast_to(taps[k : k + 1, :], (channels, channels)).T
    spread[3] = jnp.broadcast_to(gain[...], (channels, channels)).T
    def piece(owner, q):
        base = pl.multiple_of(owner * rows + q * SUB, SUB)
        wide = pl.ds(base, 2 * SUB)
        gated = gate_buf[:, wide].astype(jnp.float32) * in_buf[:, wide].astype(jnp.float32)
        docs = jnp.broadcast_to(doc_buf[:, wide], (8, 2 * SUB))
        now = docs[:, SUB:]
        same_one = (pltpu.roll(docs, 1, 1)[:, SUB:] == now).astype(jnp.float32)[:1]
        same_two = (pltpu.roll(docs, 2, 1)[:, SUB:] == now).astype(jnp.float32)[:1]
        conv = (
            spread[2] * gated[:, SUB:]
            + spread[1] * (pltpu.roll(gated, 1, 1)[:, SUB:] * same_one)
            + spread[0] * (pltpu.roll(gated, 2, 1)[:, SUB:] * same_two)
        )
        gated_out = after_buf[:, pl.ds(base, SUB)].astype(jnp.float32) * conv
        by_head = gated_out.reshape(channels // HEAD, HEAD, SUB)
        by_head = by_head * lax.rsqrt(
            jnp.mean(by_head * by_head, axis=1, keepdims=True) + norm_eps
        )
        normed = by_head.reshape(channels, SUB) * spread[3]
        return normed.T.astype(jnp.bfloat16)

    my_channels = pl.ds(pl.multiple_of(tp * channels, channels), channels)

    def trade(q, d):
        return remote(
            outgoing.at[q, d],
            by_row.at[q, :, my_channels],
            trade_send.at[q, d],
            trade_recv.at[q, d],
            sp,
            tp ^ d,
        )

    def start_trade(q):
        def begin(at, carry):
            trade(q, tp_count - 1 - at).start()
            return carry

        lax.fori_loop(0, tp_count - 1, begin, 0)

    def sent_trade(q):
        def sent(d, carry):
            trade(q, d).wait_send()
            return carry

        lax.fori_loop(1, tp_count, sent, 0)

    def block_rows(step):
        deep = 2 * channels
        return pl.ds(pl.multiple_of((z ^ step) * deep, deep), deep)

    def part_rows(step, upper):
        deep = 2 * channels
        return pl.ds(pl.multiple_of((z ^ step) * deep + upper * channels, channels), channels)

    def spread_slice(step):
        arrive_rows = [
            pl.ds(pl.multiple_of((tp ^ (2 * step + odd)) * channels, channels), channels)
            for odd in range(2)
        ]
        for odd in range(2):
            d = 2 * step + odd
            arrive(
                proj.at[arrive_rows[odd], columns(sp, core)], slice_send.at[d], slice_recv.at[d]
            )
        region = proj.at[block_rows(step), columns(sp, core)]
        for k in range(2):
            send(region, region, plane_send.at[k, step], plane_recv.at[k, step], near_of[k], tp)
        send(region, region, core_send.at[0, step], core_recv.at[0, step], sp, tp ^ 1)

    def spread_plane(step):
        for k in range(2):
            region = proj.at[block_rows(step), columns(near_of[k], core)]
            arrive(region, plane_send.at[k, step], plane_recv.at[k, step])
            part = proj.at[part_rows(step, k), columns(near_of[k], core)]
            send(part, part, corner_send.at[k, step], corner_recv.at[k, step], near_of[1 - k], tp)
            send(region, region, core_send.at[1 + k, step], core_recv.at[1 + k, step], sp, tp ^ 1)

    def spread_corner(step):
        for k in range(2):
            arrive(
                proj.at[part_rows(step, k), columns(diagonal, core)],
                corner_send.at[k, step],
                corner_recv.at[k, step],
            )
        region = proj.at[block_rows(step), columns(diagonal, core)]
        send(region, region, core_send.at[3, step], core_recv.at[3, step], sp, tp ^ 1)

    places = (sp, near_of[0], near_of[1], diagonal)

    def other_half(k):
        for step in range(1, planes):
            arrive(
                proj.at[block_rows(step), columns(places[k], 1 - core)],
                core_send.at[k, step],
                core_recv.at[k, step],
            )

    order = [1, 0, *range(2, subs)]

    def convolve(q):
        def one(at, carry):
            d = tp_count - 1 - at
            outgoing[q, d] = piece(tp ^ d, q)
            return carry

        lax.fori_loop(0, tp_count - 1, one, 0)
        by_row[q, :, my_channels] = piece(tp, q)

    for q in (1, 2):
        convolve(q)
    for step in range(1, planes):
        spread_slice(step)
        if step == 1:
            for at, target in enumerate((in_buf, gate_buf, doc_buf)):
                arrive(target.at[:, edge], edge_send.at[at], edge_recv.at[at])
            doc_buf[:, edge] = jnp.where(sp == 0, -1, doc_buf[:, edge])
            convolve(0)
    for copy in slices:
        copy.wait_send()
    start_trade(order[0])
    for step in range(1, planes):
        spread_plane(step)

    tile = width // 4
    local_experts, _, hidden_width = w_gate.shape
    slot = table.shape[2] // local_experts

    def load_weights(at):
        side, expert = at % 2, at % local_experts
        return [
            pltpu.make_async_copy(source.at[expert], target.at[side], weight_sem.at[k, side])
            for k, (source, target) in enumerate(
                ((w_gate, gate_now), (w_up, up_now), (w_down, down_now))
            )
        ]

    for at in range(2):
        for copy in load_weights(at):
            copy.start()

    def make_tables():
        for d in range(1, 4):
            arrive(ids_out.at[d], list_send.at[0, d], list_recv.at[0, d])
            arrive(weights_out.at[d], list_send.at[1, d], list_recv.at[1, d])
        deep = marks.shape[2]
        line = lax.broadcasted_iota(jnp.int32, (deep, half), 0)
        experts = sp * local_experts + line
        ahead = (
            lax.broadcasted_iota(jnp.int32, (half, half), 0)
            < lax.broadcasted_iota(jnp.int32, (half, half), 1)
        ).astype(jnp.bfloat16)
        for b in range(2):
            for n in range(4):
                hits, amount = jnp.zeros((deep, half)), jnp.zeros((deep, half))
                for k in range(ids.shape[0]):
                    here = pl.ds(b * half, half)
                    hit = (ids_out[n, pl.ds(k, 1), here] == experts) & (line < local_experts)
                    hits = hits + hit.astype(jnp.float32)
                    amount = amount + jnp.where(hit, weights_out[n, pl.ds(k, 1), here], 0.0)
                marks[b, n] = hits
                share[b, n] = amount
            flat = marks[b].reshape(4 * deep, half)
            order_of = jnp.dot(flat.astype(jnp.bfloat16), ahead, preferred_element_type=jnp.float32)
            rank[b] = jnp.where(flat > 0, order_of, -1.0).reshape(4, deep, half)

            def fill(n, carry, b=b):
                spots = lax.broadcasted_iota(jnp.int32, (slot, half), 0).astype(jnp.float32)
                for e in range(local_experts):
                    chosen = rank[b, n, pl.ds(e, 1), :] == spots
                    table[b, n, pl.ds(e * slot, slot), :] = chosen.astype(jnp.float32).astype(
                        jnp.bfloat16
                    )
                    total = jnp.sum(
                        jnp.where(chosen, share[b, n, pl.ds(e, 1), :], 0.0), axis=1, keepdims=True
                    )
                    slot_weight[b, e, pl.ds(pl.multiple_of(n * slot, slot), slot), :] = (
                        jnp.broadcast_to(total, (slot, slot_weight.shape[3]))
                    )
                return carry

            lax.fori_loop(0, 4, fill, 0)

    def near_region(place, q):
        return gathered.at[q // first, place, pl.ds(q % first * SUB, SUB)]

    def far_region(q, k):
        return gathered.at[q // first, 3, pl.ds(q % first * SUB + k * (SUB // 2), SUB // 2)]

    def got_rows(q):
        def got(d, carry):
            theirs = pl.ds(pl.multiple_of((tp ^ d) * channels, channels), channels)
            arrive(by_row.at[q, :, theirs], trade_send.at[q, d], trade_recv.at[q, d])
            return carry

        lax.fori_loop(1, tp_count, got, 0)

    def project_tile(q, place):
        mine = pl.ds(q * SUB, SUB)
        cols = pl.ds(pl.multiple_of(place * tile, tile), tile)
        value = resid_buf[mine, cols].astype(jnp.float32) + jnp.dot(
            by_row[q], proj[:, cols], preferred_element_type=jnp.float32
        )
        stream[mine, cols] = value
        return jnp.sum(value * value, axis=1, keepdims=True)

    def normalize_rows(q, total):
        mine = pl.ds(q * SUB, SUB)
        there = pl.ds(q % first * SUB, SUB)
        scale = lax.rsqrt(total / width + norm_eps)

        def normalize(n, carry):
            cols = pl.ds(pl.multiple_of(n * tile, tile), tile)
            value = (stream[mine, cols] * scale * norm_gain[:, cols]).astype(jnp.bfloat16)
            gathered[q // first, 0, there, cols] = value
            return carry

        lax.fori_loop(0, 4, normalize, 0)

    def project_rows(q):
        got_rows(q)
        total = lax.fori_loop(
            0, 4, lambda n, total: total + project_tile(q, n), jnp.zeros((SUB, 1), jnp.float32)
        )
        normalize_rows(q, total)

    def spread_rows(q):
        for k in range(2):
            send(
                near_region(0, q),
                near_region(1 + k, q),
                near_send.at[k, q],
                near_recv.at[k, q],
                near_of[k],
                tp,
            )

    far_copies = []

    def relay_rows(q):
        for k in range(2):
            arrive(near_region(1 + k, q), near_send.at[k, q], near_recv.at[k, q])
            part = gathered.at[
                q // first, 1 + k, pl.ds(q % first * SUB + k * (SUB // 2), SUB // 2)
            ]
            copy = remote(
                part, far_region(q, k), far_send.at[k, q], far_recv.at[k, q], near_of[1 - k], tp
            )
            copy.start()
            far_copies.append(copy)

    def far_rows(q):
        for k in range(2):
            arrive(far_region(q, k), far_send.at[k, q], far_recv.at[k, q])

    def run_experts(b, between=None):
        def pack(at, carry):
            n, cols = at // 4, pl.ds(pl.multiple_of(at % 4 * tile, tile), tile)
            rows_in = jnp.dot(
                table[b, n], gathered[b, n, :, cols], preferred_element_type=jnp.float32
            ).astype(jnp.bfloat16)
            for e in range(local_experts):
                packed[e, pl.ds(pl.multiple_of(n * slot, slot), slot), cols] = rows_in[
                    e * slot : (e + 1) * slot
                ]
            return carry

        lax.fori_loop(0, 16, pack, 0)

        def expert(e, carry):
            at = b * local_experts + e
            side = at % 2
            for copy in load_weights(at):
                copy.wait()
            piece_width = hidden_width // 2

            def up(c, carry):
                cols = pl.ds(pl.multiple_of(c * piece_width, piece_width), piece_width)
                gate = jnp.dot(
                    packed[e], gate_now[side, :, cols], preferred_element_type=jnp.float32
                )
                value = jnp.dot(
                    packed[e], up_now[side, :, cols], preferred_element_type=jnp.float32
                )
                hidden[:, cols] = (gate / (1.0 + jnp.exp(-gate)) * value).astype(jnp.bfloat16)
                return carry

            lax.fori_loop(0, 2, up, 0)

            def down(c, carry):
                cols = pl.ds(pl.multiple_of(c * tile, tile), tile)
                value = jnp.dot(
                    hidden[...], down_now[side, :, cols], preferred_element_type=jnp.float32
                )
                packed[e, :, cols] = (value * slot_weight[b, e, :, 0:1]).astype(jnp.bfloat16)
                return carry

            lax.fori_loop(0, 4, down, 0)

            @pl.when(at + 2 < 2 * local_experts)
            def _():
                for copy in load_weights(at + 2):
                    copy.start()

            return carry

        middle = local_experts if between is None else local_experts // 2
        lax.fori_loop(0, middle, expert, 0)
        if between is not None:
            between()
            lax.fori_loop(middle, local_experts, expert, 0)

    def combine(b, n):
        def one(c, carry):
            cols = pl.ds(pl.multiple_of(c * tile, tile), tile)
            pieces = jnp.concatenate(
                [packed[e, pl.ds(n * slot, slot), cols] for e in range(local_experts)], axis=0
            )
            partial[b, n, :, cols] = lax.dot_general(
                table[b, n], pieces, (((0,), (0,)), ((), ())), preferred_element_type=jnp.float32
            ).astype(jnp.bfloat16)
            return carry

        lax.fori_loop(0, 4, one, 0)

    part_of = [pl.ds(k * (half // 2), half // 2) for k in range(2)]

    def send_first(b):
        copies = []
        for k in range(2):
            copy = remote(
                partial.at[b, 3, part_of[k]],
                inbox.at[b, k],
                first_send.at[b, k],
                first_recv.at[b, k],
                near_of[k],
                tp,
            )
            copy.start()
            copies.append(copy)
        return copies

    def send_straight(b):
        for k in range(2):
            send(
                partial.at[b, 1 + k, part_of[k]],
                back.at[b, k, part_of[k]],
                straight_send.at[b, k],
                straight_recv.at[b, k],
                near_of[k],
                tp,
            )

    strip = 16

    def merge(b):
        for k in range(2):
            arrive(inbox.at[b, k], first_send.at[b, k], first_recv.at[b, k])

            def add(at, carry, k=k):
                there = pl.ds(pl.multiple_of(k * (half // 2) + at * strip, strip), strip)
                here = pl.ds(pl.multiple_of(at * strip, strip), strip)
                partial[b, 2 - k, there, :] = (
                    partial[b, 2 - k, there, :].astype(jnp.float32)
                    + inbox[b, k, here, :].astype(jnp.float32)
                ).astype(jnp.bfloat16)
                return carry

            lax.fori_loop(0, half // 2 // strip, add, 0)
            send(
                partial.at[b, 2 - k, part_of[k]],
                back.at[b, 1 - k, part_of[k]],
                merged_send.at[b, k],
                merged_recv.at[b, k],
                near_of[1 - k],
                tp,
            )

    def finish(b):
        for k in range(2):
            arrive(back.at[b, k, part_of[k]], straight_send.at[b, k], straight_recv.at[b, k])
        for k in range(2):
            arrive(back.at[b, 1 - k, part_of[k]], merged_send.at[b, k], merged_recv.at[b, k])

            def add(at, carry, k=k):
                here = pl.ds(pl.multiple_of(k * (half // 2) + at * strip, strip), strip)
                there = pl.ds(pl.multiple_of(b * half + k * (half // 2) + at * strip, strip), strip)
                value = stream[there, :] + partial[b, 0, here, :].astype(jnp.float32)
                value = value + back[b, 0, here, :].astype(jnp.float32)
                (out_low, out_high)[b][here, :] = (
                    value + back[b, 1, here, :].astype(jnp.float32)
                ).astype(jnp.bfloat16)
                return carry

            lax.fori_loop(0, half // 2 // strip, add, 0)

    got_rows(order[0])
    sent_trade(order[0])
    start_trade(order[1])
    for copy in loads[6:]:
        copy.wait()
    arrive(
        proj.at[pl.ds(pl.multiple_of((tp ^ 1) * channels, channels), channels)],
        slice_send.at[1],
        slice_recv.at[1],
    )
    total = jnp.zeros((SUB, 1), jnp.float32)
    for k in range(4):
        if k == 3:
            for step in range(1, planes):
                spread_corner(step)
        other_half(k)
        total = total + project_tile(order[0], places[k])
    normalize_rows(order[0], total)
    spread_rows(order[0])
    make_tables()
    for q in range(3, subs):
        convolve(q)
    for at_q in range(1, first):
        sent_trade(order[at_q])
        if at_q + 1 < subs:
            start_trade(order[at_q + 1])
        project_rows(order[at_q])
        spread_rows(order[at_q])
    for at_q in range(first):
        relay_rows(order[at_q])
        late = order[first + at_q]
        sent_trade(late)
        if first + at_q + 1 < subs:
            start_trade(order[first + at_q + 1])
        project_rows(late)
    for copy in far_copies[:2]:
        copy.wait_send()
    spread_rows(order[first])
    for at_q in range(first):
        far_rows(order[at_q])
    for at_q in range(1, first):
        spread_rows(order[first + at_q])
    run_experts(0, lambda: relay_rows(order[first]))
    for at_q in range(1, first):
        relay_rows(order[first + at_q])
    combine(0, 3)
    firsts = send_first(0)
    combine(0, 1)
    combine(0, 2)
    send_straight(0)
    combine(0, 0)
    merge(0)
    for at_q in range(first):
        far_rows(order[first + at_q])
    run_experts(1)
    combine(1, 3)
    firsts_two = send_first(1)
    combine(1, 1)
    combine(1, 2)
    combine(1, 0)
    for copy in firsts_two:
        copy.wait_send()
    send_straight(1)
    finish(0)
    merge(1)
    finish(1)
    for copy in firsts + far_copies[2:]:
        copy.wait_send()
    for copy in pending:
        copy.wait_send()


def front(
    conv_in, in_gate, out_gate, doc_ids, conv_taps, head_gain, out_proj, resid, norm_gain,
    route_ids, route_weight, w_gate, w_up, w_down,
):
    tp_count = lax.axis_size("tp")
    channels, width = out_proj.shape
    positions = conv_in.shape[1]
    rows = resid.shape[0]
    half, subs = rows // 2, rows // SUB
    first, planes = half // SUB, tp_count // 2
    top = route_ids.shape[1]
    local_experts, _, hidden_width = w_gate.shape
    slot = max(2, rows // 8)
    hbm = pl.BlockSpec(memory_space=pltpu.HBM)
    dma = pltpu.SemaphoreType.DMA
    return pl.pallas_call(
        functools.partial(front_kernel, tp_count),
        out_shape=[pltpu.VMEM((half, width), jnp.bfloat16)] * 2,
        in_specs=[hbm] * 14,
        out_specs=[pl.BlockSpec(memory_space=pltpu.VMEM)] * 2,
        scratch_shapes=[
            pltpu.VMEM((4, top, rows), jnp.int32),
            pltpu.VMEM((4, top, rows), jnp.float32),
            pltpu.VMEM((channels, SUB + positions), jnp.bfloat16),
            pltpu.VMEM((channels, SUB + positions), jnp.bfloat16),
            pltpu.VMEM((channels, positions), jnp.bfloat16),
            pltpu.VMEM((1, SUB + positions), jnp.int32),
            pltpu.VMEM((3, channels), jnp.float32),
            pltpu.VMEM((1, channels), jnp.float32),
            pltpu.VMEM((1, width), jnp.float32),
            pltpu.VMEM((tp_count * channels, width), jnp.bfloat16),
            pltpu.VMEM((rows, width), jnp.bfloat16),
            pltpu.VMEM((4, channels, SUB), jnp.float32),
            pltpu.VMEM((subs, tp_count, SUB, channels), jnp.bfloat16),
            pltpu.VMEM((subs, SUB, tp_count * channels), jnp.bfloat16),
            pltpu.VMEM((2, 4, half, width), jnp.bfloat16),
            pltpu.VMEM((rows, width), jnp.float32),
            pltpu.VMEM((2, width, hidden_width), jnp.bfloat16),
            pltpu.VMEM((2, width, hidden_width), jnp.bfloat16),
            pltpu.VMEM((2, hidden_width, width), jnp.bfloat16),
            pltpu.VMEM((2, 4, 8, half), jnp.float32),
            pltpu.VMEM((2, 4, 8, half), jnp.float32),
            pltpu.VMEM((2, 4, 8, half), jnp.float32),
            pltpu.VMEM((2, 4, local_experts * slot, half), jnp.bfloat16),
            pltpu.VMEM((2, local_experts, 4 * slot, 128), jnp.float32),
            pltpu.VMEM((local_experts, 4 * slot, width), jnp.bfloat16),
            pltpu.VMEM((4 * slot, hidden_width), jnp.bfloat16),
            pltpu.VMEM((2, 4, half, width), jnp.bfloat16),
            pltpu.VMEM((2, 2, half // 2, width), jnp.bfloat16),
            pltpu.VMEM((2, 2, half, width), jnp.bfloat16),
            dma((11,)),
            dma((3,)),
            dma((3,)),
            dma((2, 4)),
            dma((2, 4)),
            dma((tp_count,)),
            dma((tp_count,)),
            dma((2, planes)),
            dma((2, planes)),
            dma((2, planes)),
            dma((2, planes)),
            dma((4, planes)),
            dma((4, planes)),
            dma((subs, tp_count)),
            dma((subs, tp_count)),
            dma((2, subs)),
            dma((2, subs)),
            dma((2, subs)),
            dma((2, subs)),
            dma((3, 2)),
            dma((2, 2)),
            dma((2, 2)),
            dma((2, 2)),
            dma((2, 2)),
            dma((2, 2)),
            dma((2, 2)),
        ],
        compiler_params=pltpu.CompilerParams(
            collective_id=0, has_side_effects=True, vmem_limit_bytes=59944 * 1024
        ),
        name="front",
    )(
        conv_in,
        in_gate,
        out_gate,
        doc_ids[None],
        conv_taps.T,
        head_gain[None],
        out_proj,
        resid,
        norm_gain[None],
        route_ids.T,
        route_weight.T,
        w_gate,
        w_up,
        w_down,
    )


def body(
    conv_in,
    in_gate,
    out_gate,
    doc_ids,
    conv_taps,
    head_gain,
    out_proj,
    resid,
    norm_gain,
    route_ids,
    route_weight,
    w_gate,
    w_up,
    w_down,
):
    channels, width = out_proj.shape
    rows = resid.shape[0]
    half = rows // 2
    slot = max(2, rows // 8)
    sp_count, tp_count = lax.axis_size("sp"), lax.axis_size("tp")
    local_experts = w_gate.shape[0]
    if (
        sp_count == 4
        and tp_count >= 4
        and tp_count & (tp_count - 1) == 0
        and channels == SUB
        and channels % HEAD == 0
        and width % 1024 == 0
        and rows % (2 * SUB) == 0
        and conv_in.shape[1] == tp_count * rows
        and rows <= 2 * local_experts * slot
    ):
        halves = front(
            conv_in,
            in_gate,
            out_gate,
            doc_ids,
            conv_taps,
            head_gain,
            out_proj,
            resid,
            norm_gain,
            route_ids,
            route_weight,
            w_gate,
            w_up,
            w_down,
        )
        return jnp.concatenate(halves, axis=0)
    gated_in = in_gate.astype(jnp.float32) * conv_in.astype(jnp.float32)
    doc_value = doc_ids.astype(jnp.float32)
    edge = jnp.concatenate([gated_in[:, -2:], doc_value[None, -2:]], axis=0)
    edge = shifted(edge, "sp", 1)
    earlier_in, earlier_doc = edge[:-1], edge[-1]
    padded_in = jnp.concatenate([earlier_in, gated_in], axis=1)
    padded_doc = jnp.concatenate([earlier_doc, doc_value])
    same_one = (padded_doc[1:-1] == doc_value).astype(jnp.float32)
    same_two = (padded_doc[:-2] == doc_value).astype(jnp.float32)
    conv_out = (
        conv_taps[:, 2:3] * gated_in
        + conv_taps[:, 1:2] * (padded_in[:, 1:-1] * same_one)
        + conv_taps[:, 0:1] * (padded_in[:, :-2] * same_two)
    )
    gated_out = out_gate.astype(jnp.float32) * conv_out
    by_head = gated_out.reshape(channels // HEAD, HEAD, -1)
    by_head = by_head * lax.rsqrt(jnp.mean(by_head * by_head, axis=1, keepdims=True) + norm_eps)
    head_normed = (by_head.reshape(channels, -1) * head_gain[:, None]).astype(jnp.bfloat16)
    by_row = lax.all_to_all(head_normed, "tp", split_axis=1, concat_axis=0, tiled=True)
    mixed = lax.dot_general(
        by_row,
        lax.all_gather(out_proj, "tp", axis=0, tiled=True),
        (((0,), (0,)), ((), ())),
        preferred_element_type=jnp.float32,
    )
    stream = resid.astype(jnp.float32) + mixed
    expert_in = (
        stream * lax.rsqrt(jnp.mean(stream * stream, axis=1, keepdims=True) + norm_eps) * norm_gain
    ).astype(jnp.bfloat16)
    experts_total = local_experts * sp_count
    parts = []
    for block_no in range(2):
        block_ids = route_ids[block_no * half : (block_no + 1) * half]
        place = slot_places(block_ids, slot, experts_total)
        send = pack_rows(
            place, expert_in[block_no * half : (block_no + 1) * half], experts_total * slot
        ).reshape(sp_count, local_experts, slot, width)
        arrived = lax.all_to_all(send, "sp", split_axis=0, concat_axis=0, tiled=True)
        gate_part = jnp.einsum(
            "nesd,edf->nesf", arrived, w_gate, preferred_element_type=jnp.float32
        )
        up_part = jnp.einsum("nesd,edf->nesf", arrived, w_up, preferred_element_type=jnp.float32)
        hidden = (jax.nn.silu(gate_part) * up_part).astype(jnp.bfloat16)
        arrived = jnp.einsum(
            "nesf,efd->nesd", hidden, w_down, preferred_element_type=jnp.float32
        ).astype(jnp.bfloat16)
        returned = lax.all_to_all(arrived, "sp", split_axis=0, concat_axis=0, tiled=True).reshape(
            experts_total * slot, width
        )
        parts.append(
            combine_rows(returned, place, route_weight[block_no * half : (block_no + 1) * half])
        )
    mixture = jnp.concatenate(parts, axis=0)
    return (stream + mixture).astype(jnp.bfloat16)


def solution(mesh):
    return jax.shard_map(
        body,
        mesh=mesh,
        in_specs=(
            P("tp", "sp"),
            P("tp", "sp"),
            P("tp", "sp"),
            P("sp"),
            P("tp", None),
            P("tp"),
            P("tp", None),
            P(("sp", "tp"), None),
            P(),
            P(("sp", "tp"), None),
            P(("sp", "tp"), None),
            P("sp", None, None),
            P("sp", None, None),
            P("sp", None, None),
        ),
        out_specs=P(("sp", "tp"), None),
        check_vma=False,
    )
```

```python
import functools

import jax
import jax.numpy as jnp
from jax import lax
from jax.experimental import pallas as pl
from jax.experimental.pallas import tpu as pltpu
from jax.sharding import PartitionSpec as P

HEAD = 64


norm_eps = 1e-06


def shifted(value, axis, steps):
    count = lax.axis_size(axis)
    leading, last = (max(0, -steps), min(count, count - steps))
    return lax.ppermute(value, axis, [(source, source + steps) for source in range(leading, last)])


def slot_places(ids_block, slot, experts):
    flat = ids_block.reshape(-1)
    marks = (flat[:, None] == jnp.arange(experts, dtype=jnp.int32)[None, :]).astype(jnp.int32)
    before = jnp.sum((jnp.cumsum(marks, axis=0) - 1) * marks, axis=1)
    return (flat * slot + before).reshape(ids_block.shape)


def pack_rows(places, normed_rows, total_slots):
    targets = jnp.arange(total_slots, dtype=jnp.int32)
    table = jnp.any(targets[:, None, None] == places[None, :, :], axis=2).astype(jnp.bfloat16)
    return jnp.dot(table, normed_rows, preferred_element_type=jnp.float32).astype(jnp.bfloat16)


def combine_rows(returned, places, weights):
    totals = jnp.zeros((places.shape[0], returned.shape[1]), jnp.float32)
    for choice_k in range(places.shape[1]):
        totals = totals + weights[:, choice_k : choice_k + 1] * returned[
            places[:, choice_k]
        ].astype(jnp.float32)
    return totals


MESH = pl.DeviceIdType.MESH
SUB = 128
EARLY = 64


def front_kernel(
    tp_count,
    conv_in,
    in_gate,
    out_gate,
    doc_ids,
    taps_in,
    gain_in,
    out_proj,
    resid,
    norm_gain_in,
    ids,
    weights,
    w_gate,
    w_up,
    w_down,
    out_low,
    out_high,
    ids_out,
    weights_out,
    in_buf,
    gate_buf,
    after_buf,
    doc_buf,
    taps,
    gain,
    norm_gain,
    proj,
    resid_buf,
    spread,
    outgoing,
    by_row,
    gathered,
    stream,
    gate_now,
    up_now,
    down_now,
    marks,
    share,
    rank,
    table,
    slot_weight,
    packed,
    hidden,
    partial,
    inbox,
    back,
    early_resid,
    early_normed,
    local_sem,
    edge_send,
    edge_recv,
    list_send,
    list_recv,
    slice_send,
    slice_recv,
    plane_send,
    plane_recv,
    corner_send,
    corner_recv,
    core_send,
    core_recv,
    trade_send,
    trade_recv,
    near_send,
    near_recv,
    far_send,
    far_recv,
    weight_sem,
    first_send,
    first_recv,
    back_send,
    straight_recv,
    merged_recv,
    resid_send,
    resid_recv,
    normed_send,
    normed_recv,
):
    sp, tp = lax.axis_index("sp"), lax.axis_index("tp")
    z, core = tp // 2, tp % 2
    channels, width = out_proj.shape
    rows = resid.shape[0]
    half, subs = rows // 2, rows // SUB
    first = half // SUB
    planes = tp_count // 2
    near_of = [sp ^ 1, sp ^ 2]
    diagonal = sp ^ 3

    def remote(source, target, send_sem, recv_sem, to_sp, to_tp):
        return pltpu.make_async_remote_copy(
            src_ref=source,
            dst_ref=target,
            send_sem=send_sem,
            recv_sem=recv_sem,
            device_id=(to_sp, to_tp),
            device_id_type=MESH,
        )

    def send(source, target, send_sem, recv_sem, to_sp, to_tp):
        remote(source, target, send_sem, recv_sem, to_sp, to_tp).start()

    def left(region, send_sem):
        remote(region, region, send_sem, send_sem, near_of[0], tp).wait_send()

    def arrive(region, recv_sem):
        remote(region, region, recv_sem, recv_sem, near_of[0], tp).wait_recv()

    tail = conv_in.shape[1] - SUB
    loads = [
        pltpu.make_async_copy(conv_in, in_buf.at[:, pl.ds(SUB, conv_in.shape[1])], local_sem.at[0]),
        pltpu.make_async_copy(in_gate, gate_buf.at[:, pl.ds(SUB, conv_in.shape[1])], local_sem.at[1]),
        pltpu.make_async_copy(out_gate, after_buf, local_sem.at[2]),
        pltpu.make_async_copy(doc_ids, doc_buf.at[:, pl.ds(SUB, conv_in.shape[1])], local_sem.at[3]),
        pltpu.make_async_copy(taps_in, taps, local_sem.at[6]),
        pltpu.make_async_copy(gain_in, gain, local_sem.at[7]),
        pltpu.make_async_copy(
            out_proj, proj.at[pl.ds(pl.multiple_of(tp * channels, channels), channels)], local_sem.at[4]
        ),
        pltpu.make_async_copy(resid, resid_buf, local_sem.at[5]),
        pltpu.make_async_copy(norm_gain_in, norm_gain, local_sem.at[8]),
        pltpu.make_async_copy(ids, ids_out.at[0], local_sem.at[9]),
        pltpu.make_async_copy(weights, weights_out.at[0], local_sem.at[10]),
    ]
    for copy in loads:
        copy.start()

    barrier = pltpu.get_barrier_semaphore()
    for d in range(1, tp_count):
        pl.semaphore_signal(barrier, inc=1, device_id=(sp, tp ^ d), device_id_type=MESH)
    for d in range(1, 4):
        pl.semaphore_signal(barrier, inc=1, device_id=(sp ^ d, tp), device_id_type=MESH)
    pl.semaphore_wait(barrier, tp_count + 2)

    after, before = (sp + 1) % 4, (sp + 3) % 4
    edge = pl.ds(0, SUB)
    for at, (source, target) in enumerate(
        ((conv_in, in_buf), (in_gate, gate_buf), (doc_ids, doc_buf))
    ):
        send(
            source.at[:, pl.ds(tail, SUB)],
            target.at[:, edge],
            edge_send.at[at],
            edge_recv.at[at],
            after,
            tp,
        )

    eighth = width // 8

    def columns(place, side):
        return pl.ds(pl.multiple_of(place * (2 * eighth) + side * eighth, eighth), eighth)

    my_rows = pl.ds(pl.multiple_of(tp * channels, channels), channels)
    early = EARLY
    slices = []
    for d in range(2, tp_count):
        side = core ^ (d & 1)
        copy = remote(
            out_proj.at[:, columns(sp, side)],
            proj.at[my_rows, columns(sp, side)],
            slice_send.at[1],
            slice_recv.at[d // 2],
            sp,
            tp ^ d,
        )
        slices.append(copy)

    for copy in slices:
        copy.start()
    for k in range(2):
        send(
            resid.at[pl.ds(rows - early, early)],
            early_resid.at[k],
            resid_send.at[0],
            resid_recv.at[0],
            near_of[k],
            tp,
        )
    send(out_proj, proj.at[my_rows], slice_send.at[0], slice_recv.at[0], sp, tp ^ 1)
    for d in range(1, 4):
        send(ids, ids_out.at[d], list_send.at[0], list_recv.at[0], sp ^ d, tp)
        send(weights, weights_out.at[d], list_send.at[1], list_recv.at[1], sp ^ d, tp)
    for copy in loads[:6]:
        copy.wait()
    for k in range(3):
        spread[k] = jnp.broadcast_to(taps[k : k + 1, :], (channels, channels)).T
    spread[3] = jnp.broadcast_to(gain[...], (channels, channels)).T
    def piece(owner, q):
        base = pl.multiple_of(owner * rows + q * SUB, SUB)
        wide = pl.ds(base, 2 * SUB)
        gated = gate_buf[:, wide].astype(jnp.float32) * in_buf[:, wide].astype(jnp.float32)
        docs = jnp.broadcast_to(doc_buf[:, wide], (8, 2 * SUB))
        now = docs[:, SUB:]
        same_one = (pltpu.roll(docs, 1, 1)[:, SUB:] == now).astype(jnp.float32)[:1]
        same_two = (pltpu.roll(docs, 2, 1)[:, SUB:] == now).astype(jnp.float32)[:1]
        conv = (
            spread[2] * gated[:, SUB:]
            + spread[1] * (pltpu.roll(gated, 1, 1)[:, SUB:] * same_one)
            + spread[0] * (pltpu.roll(gated, 2, 1)[:, SUB:] * same_two)
        )
        gated_out = after_buf[:, pl.ds(base, SUB)].astype(jnp.float32) * conv
        by_head = gated_out.reshape(channels // HEAD, HEAD, SUB)
        by_head = by_head * lax.rsqrt(
            jnp.mean(by_head * by_head, axis=1, keepdims=True) + norm_eps
        )
        normed = by_head.reshape(channels, SUB) * spread[3]
        return normed.T.astype(jnp.bfloat16)

    my_channels = pl.ds(pl.multiple_of(tp * channels, channels), channels)

    def trade(q, d):
        return remote(
            outgoing.at[q, d],
            by_row.at[q, :, my_channels],
            trade_send.at[q],
            trade_recv.at[q],
            sp,
            tp ^ d,
        )

    def start_trade(q):
        def begin(at, carry):
            trade(q, tp_count - 1 - at).start()
            return carry

        lax.fori_loop(0, tp_count - 1, begin, 0)

    def sent_trade(q):
        left(outgoing.at[q, pl.ds(1, tp_count - 1)], trade_send.at[q])

    def block_rows(step):
        deep = 2 * channels
        return pl.ds(pl.multiple_of((z ^ step) * deep, deep), deep)

    def part_rows(step, upper):
        deep = 2 * channels
        return pl.ds(pl.multiple_of((z ^ step) * deep + upper * channels, channels), channels)

    def spread_slice(step):
        region = proj.at[block_rows(step), columns(sp, core)]
        arrive(region, slice_recv.at[step])
        for k in range(2):
            send(region, region, plane_send.at[0], plane_recv.at[k, step - 1], near_of[k], tp)
        send(region, region, core_send.at[0], core_recv.at[0, step - 1], sp, tp ^ 1)

    def spread_plane(step):
        for k in range(2):
            region = proj.at[block_rows(step), columns(near_of[k], core)]
            arrive(region, plane_recv.at[k, step - 1])
            part = proj.at[part_rows(step, k), columns(near_of[k], core)]
            send(part, part, corner_send.at[0], corner_recv.at[step - 1], near_of[1 - k], tp)
            send(region, region, core_send.at[0], core_recv.at[1 + k, step - 1], sp, tp ^ 1)

    def spread_corner(step):
        region = proj.at[block_rows(step), columns(diagonal, core)]
        arrive(region, corner_recv.at[step - 1])
        send(region, region, core_send.at[0], core_recv.at[3, step - 1], sp, tp ^ 1)

    places = (sp, near_of[0], near_of[1], diagonal)

    def other_half(k):
        for step in range(1, planes):
            arrive(
                proj.at[block_rows(step), columns(places[k], 1 - core)],
                core_recv.at[k, step - 1],
            )

    order = [1, 0, *range(2, subs)]

    def convolve(q):
        def one(at, carry):
            d = tp_count - 1 - at
            outgoing[q, d] = piece(tp ^ d, q)
            return carry

        lax.fori_loop(0, tp_count - 1, one, 0)
        by_row[q, :, my_channels] = piece(tp, q)

    convolve(1)
    convolve(2)
    steps = list(range(1, planes))
    for at, step in enumerate(steps):
        spread_slice(step)
        if at == 0:
            for k, target in enumerate((in_buf, gate_buf, doc_buf)):
                arrive(target.at[:, edge], edge_recv.at[k])
            doc_buf[:, edge] = jnp.where(sp == 0, -1, doc_buf[:, edge])
            convolve(0)
    left(proj.at[pl.ds(0, 2 * (planes - 1) * channels // 8)], slice_send.at[1])
    start_trade(order[0])
    for step in steps:
        spread_plane(step)

    tile = width // 4
    local_experts, _, hidden_width = w_gate.shape
    slot = table.shape[2] // local_experts

    def load_weights(at):
        side, expert = at % 2, at % local_experts
        return [
            pltpu.make_async_copy(source.at[expert], target.at[side], weight_sem.at[k, side])
            for k, (source, target) in enumerate(
                ((w_gate, gate_now), (w_up, up_now), (w_down, down_now))
            )
        ]

    for at in range(2):
        for copy in load_weights(at):
            copy.start()

    def make_tables():
        arrive(ids_out.at[pl.ds(1, 3)], list_recv.at[0])
        arrive(weights_out.at[pl.ds(1, 3)], list_recv.at[1])
        deep = marks.shape[2]
        line = lax.broadcasted_iota(jnp.int32, (deep, half), 0)
        experts = sp * local_experts + line
        ahead = (
            lax.broadcasted_iota(jnp.int32, (half, half), 0)
            < lax.broadcasted_iota(jnp.int32, (half, half), 1)
        ).astype(jnp.bfloat16)
        for b in range(2):
            for n in range(4):
                hits, amount = jnp.zeros((deep, half)), jnp.zeros((deep, half))
                for k in range(ids.shape[0]):
                    here = pl.ds(b * half, half)
                    hit = (ids_out[n, pl.ds(k, 1), here] == experts) & (line < local_experts)
                    hits = hits + hit.astype(jnp.float32)
                    amount = amount + jnp.where(hit, weights_out[n, pl.ds(k, 1), here], 0.0)
                marks[b, n] = hits
                share[b, n] = amount
            flat = marks[b].reshape(4 * deep, half)
            order_of = jnp.dot(flat.astype(jnp.bfloat16), ahead, preferred_element_type=jnp.float32)
            rank[b] = jnp.where(flat > 0, order_of, -1.0).reshape(4, deep, half)

            def fill(n, carry, b=b):
                spots = lax.broadcasted_iota(jnp.int32, (slot, half), 0).astype(jnp.float32)
                for e in range(local_experts):
                    chosen = rank[b, n, pl.ds(e, 1), :] == spots
                    table[b, n, pl.ds(e * slot, slot), :] = chosen.astype(jnp.float32).astype(
                        jnp.bfloat16
                    )
                    total = jnp.sum(
                        jnp.where(chosen, share[b, n, pl.ds(e, 1), :], 0.0), axis=1, keepdims=True
                    )
                    slot_weight[b, e, pl.ds(pl.multiple_of(n * slot, slot), slot), :] = (
                        jnp.broadcast_to(total, (slot, slot_weight.shape[3]))
                    )
                return carry

            lax.fori_loop(0, 4, fill, 0)

    def early_region(place, k):
        part = pl.ds(half - early + k * (early // 2), early // 2)
        return gathered.at[1, place, part]

    def project_early():
        arrive(early_resid, resid_recv.at[0])
        arrive(early_normed, normed_recv.at[0])
        deep = 2 * early

        def stream_of(n):
            cols = pl.ds(pl.multiple_of(n * tile, tile), tile)
            value = early_resid[:, :, cols].astype(jnp.float32).reshape(deep, tile)
            return cols, value + jnp.dot(
                early_normed[...].reshape(deep, tp_count * channels),
                proj[:, cols],
                preferred_element_type=jnp.float32,
            )

        def project(n, total):
            value = stream_of(n)[1]
            return total + jnp.sum(value * value, axis=1, keepdims=True)

        total = lax.fori_loop(0, 4, project, jnp.zeros((deep, 1), jnp.float32))
        scale = lax.rsqrt(total / width + norm_eps)

        def normalize(n, carry):
            cols, value = stream_of(n)
            value = (value * scale * norm_gain[:, cols]).astype(jnp.bfloat16)
            for k in range(2):
                gathered[1, 1 + k, pl.ds(half - early, early), cols] = value[
                    k * early : (k + 1) * early
                ]
            return carry

        lax.fori_loop(0, 4, normalize, 0)
        for k in range(2):
            send(
                early_region(1 + k, k),
                early_region(3, k),
                normed_send.at[1],
                normed_recv.at[1],
                near_of[1 - k],
                tp,
            )

    def span(q):
        return SUB - early if q == subs - 1 else SUB

    def near_region(place, q):
        return gathered.at[q // first, place, pl.ds(q % first * SUB, span(q))]

    def far_region(q, k, place=3):
        part = span(q) // 2
        return gathered.at[q // first, place, pl.ds(q % first * SUB + k * part, part)]

    def got_rows(q):
        arrive(by_row.at[q, :, pl.ds(0, (tp_count - 1) * channels)], trade_recv.at[q])

    def project_tile(q, place):
        mine = pl.ds(q * SUB, SUB)
        cols = pl.ds(pl.multiple_of(place * tile, tile), tile)
        value = resid_buf[mine, cols].astype(jnp.float32) + jnp.dot(
            by_row[q], proj[:, cols], preferred_element_type=jnp.float32
        )
        stream[mine, cols] = value
        return jnp.sum(value * value, axis=1, keepdims=True)

    def normalize_rows(q, total):
        mine = pl.ds(q * SUB, SUB)
        there = pl.ds(q % first * SUB, SUB)
        scale = lax.rsqrt(total / width + norm_eps)

        def normalize(n, carry):
            cols = pl.ds(pl.multiple_of(n * tile, tile), tile)
            value = (stream[mine, cols] * scale * norm_gain[:, cols]).astype(jnp.bfloat16)
            gathered[q // first, 0, there, cols] = value
            return carry

        lax.fori_loop(0, 4, normalize, 0)

    def project_rows(q):
        got_rows(q)
        total = lax.fori_loop(
            0, 4, lambda n, total: total + project_tile(q, n), jnp.zeros((SUB, 1), jnp.float32)
        )
        normalize_rows(q, total)

    def spread_rows(q):
        for k in range(2):
            send(
                near_region(0, q),
                near_region(1 + k, q),
                near_send.at[q],
                near_recv.at[k, q],
                near_of[k],
                tp,
            )

    def relay_rows(q):
        for k in range(2):
            arrive(near_region(1 + k, q), near_recv.at[k, q])
            send(
                far_region(q, k, 1 + k),
                far_region(q, k),
                far_send.at[q],
                far_recv.at[q],
                near_of[1 - k],
                tp,
            )

    def far_rows(q):
        arrive(near_region(3, q), far_recv.at[q])

    def run_experts(b, between=None):
        def pack(at, carry):
            n, cols = at // 4, pl.ds(pl.multiple_of(at % 4 * tile, tile), tile)
            rows_in = jnp.dot(
                table[b, n], gathered[b, n, :, cols], preferred_element_type=jnp.float32
            ).astype(jnp.bfloat16)
            for e in range(local_experts):
                packed[e, pl.ds(pl.multiple_of(n * slot, slot), slot), cols] = rows_in[
                    e * slot : (e + 1) * slot
                ]
            return carry

        lax.fori_loop(0, 16, pack, 0)

        def expert(e, carry):
            at = b * local_experts + e
            side = at % 2
            for copy in load_weights(at):
                copy.wait()
            piece_width = hidden_width // 2

            def up(c, carry):
                cols = pl.ds(pl.multiple_of(c * piece_width, piece_width), piece_width)
                gate = jnp.dot(
                    packed[e], gate_now[side, :, cols], preferred_element_type=jnp.float32
                )
                value = jnp.dot(
                    packed[e], up_now[side, :, cols], preferred_element_type=jnp.float32
                )
                hidden[:, cols] = (gate / (1.0 + jnp.exp(-gate)) * value).astype(jnp.bfloat16)
                return carry

            lax.fori_loop(0, 2, up, 0)

            def down(c, carry):
                cols = pl.ds(pl.multiple_of(c * tile, tile), tile)
                value = jnp.dot(
                    hidden[...], down_now[side, :, cols], preferred_element_type=jnp.float32
                )
                packed[e, :, cols] = (value * slot_weight[b, e, :, 0:1]).astype(jnp.bfloat16)
                return carry

            lax.fori_loop(0, 4, down, 0)

            @pl.when(at + 2 < 2 * local_experts)
            def _():
                for copy in load_weights(at + 2):
                    copy.start()

            return carry

        middle = local_experts if between is None else local_experts // 2
        lax.fori_loop(0, middle, expert, 0)
        if between is not None:
            between()
            lax.fori_loop(middle, local_experts, expert, 0)

    def combine(b, n):
        def one(c, carry):
            cols = pl.ds(pl.multiple_of(c * tile, tile), tile)
            pieces = jnp.concatenate(
                [packed[e, pl.ds(n * slot, slot), cols] for e in range(local_experts)], axis=0
            )
            partial[b, n, :, cols] = lax.dot_general(
                table[b, n], pieces, (((0,), (0,)), ((), ())), preferred_element_type=jnp.float32
            ).astype(jnp.bfloat16)
            return carry

        lax.fori_loop(0, 4, one, 0)

    part_of = [pl.ds(k * (half // 2), half // 2) for k in range(2)]

    def send_first(b):
        for k in range(2):
            send(
                partial.at[b, 3, part_of[k]],
                inbox.at[b, k],
                first_send.at[b],
                first_recv.at[b, k],
                near_of[k],
                tp,
            )

    def send_straight(b):
        for k in range(2):
            send(
                partial.at[b, 1 + k, part_of[k]],
                back.at[b, k, part_of[k]],
                back_send.at[b],
                straight_recv.at[b, k],
                near_of[k],
                tp,
            )

    strip = 16

    def merge(b):
        for k in range(2):
            arrive(inbox.at[b, k], first_recv.at[b, k])

            def add(at, carry, k=k):
                there = pl.ds(pl.multiple_of(k * (half // 2) + at * strip, strip), strip)
                here = pl.ds(pl.multiple_of(at * strip, strip), strip)
                partial[b, 2 - k, there, :] = (
                    partial[b, 2 - k, there, :].astype(jnp.float32)
                    + inbox[b, k, here, :].astype(jnp.float32)
                ).astype(jnp.bfloat16)
                return carry

            lax.fori_loop(0, half // 2 // strip, add, 0)
            send(
                partial.at[b, 2 - k, part_of[k]],
                back.at[b, 1 - k, part_of[k]],
                back_send.at[b],
                merged_recv.at[b, k],
                near_of[1 - k],
                tp,
            )

    def finish(b):
        for k in range(2):
            arrive(back.at[b, k, part_of[k]], straight_recv.at[b, k])
        for k in range(2):
            arrive(back.at[b, 1 - k, part_of[k]], merged_recv.at[b, k])

            def add(at, carry, k=k):
                here = pl.ds(pl.multiple_of(k * (half // 2) + at * strip, strip), strip)
                there = pl.ds(pl.multiple_of(b * half + k * (half // 2) + at * strip, strip), strip)
                value = stream[there, :] + partial[b, 0, here, :].astype(jnp.float32)
                value = value + back[b, 0, here, :].astype(jnp.float32)
                (out_low, out_high)[b][here, :] = (
                    value + back[b, 1, here, :].astype(jnp.float32)
                ).astype(jnp.bfloat16)
                return carry

            lax.fori_loop(0, half // 2 // strip, add, 0)

    got_rows(order[0])
    sent_trade(order[0])
    start_trade(order[1])
    for copy in loads[6:]:
        copy.wait()
    arrive(
        proj.at[pl.ds(pl.multiple_of((tp ^ 1) * channels, channels), channels)],
        slice_recv.at[0],
    )
    total = jnp.zeros((SUB, 1), jnp.float32)
    for k in range(4):
        if k == 3:
            for step in steps:
                spread_corner(step)
        other_half(k)
        total = total + project_tile(order[0], places[k])
    normalize_rows(order[0], total)
    spread_rows(order[0])
    make_tables()
    for q in range(3, subs):
        convolve(q)
    for at_q in range(1, first):
        sent_trade(order[at_q])
        if at_q + 1 < subs:
            start_trade(order[at_q + 1])
        project_rows(order[at_q])
        spread_rows(order[at_q])
    for at_q in range(first):
        relay_rows(order[at_q])
        late = order[first + at_q]
        sent_trade(late)
        if first + at_q + 1 < subs:
            start_trade(order[first + at_q + 1])
        project_rows(late)
    left(near_region(0, order[0]), far_send.at[order[0]])
    spread_rows(order[first])
    for at_q in range(first):
        far_rows(order[at_q])
    for at_q in range(1, first):
        spread_rows(order[first + at_q])
    for k in range(2):
        send(
            by_row.at[subs - 1, pl.ds(SUB - early, early)],
            early_normed.at[k],
            normed_send.at[0],
            normed_recv.at[0],
            near_of[k],
            tp,
        )
    run_experts(0, lambda: relay_rows(order[first]))
    combine(0, 3)
    send_first(0)
    for at_q in range(1, first):
        relay_rows(order[first + at_q])
    project_early()
    combine(0, 1)
    combine(0, 2)
    send_straight(0)
    combine(0, 0)
    merge(0)
    for at_q in range(first):
        far_rows(order[first + at_q])
    arrive(gathered.at[1, 3, pl.ds(half - early, early)], normed_recv.at[1])
    run_experts(1)
    combine(1, 3)
    send_first(1)
    combine(1, 1)
    combine(1, 2)
    combine(1, 0)
    left(partial.at[1, 3], first_send.at[1])
    send_straight(1)
    finish(0)
    merge(1)
    finish(1)
    for at, target in enumerate((in_buf, gate_buf, doc_buf)):
        left(target.at[:, edge], edge_send.at[at])
    left(ids_out.at[pl.ds(1, 3)], list_send.at[0])
    left(weights_out.at[pl.ds(1, 3)], list_send.at[1])
    left(proj.at[my_rows], slice_send.at[0])
    left(proj.at[pl.ds(0, (planes - 1) * channels // 2)], plane_send.at[0])
    left(proj.at[pl.ds(0, (planes - 1) * channels // 4)], corner_send.at[0])
    left(proj.at[pl.ds(0, (planes - 1) * channels)], core_send.at[0])
    left(early_resid, resid_send.at[0])
    left(early_normed, normed_send.at[0])
    left(gathered.at[1, 3, pl.ds(half - early, early)], normed_send.at[1])
    for q in range(subs):
        left(
            gathered.at[q // first, pl.ds(0, 2), pl.ds(q % first * SUB, span(q))],
            near_send.at[q],
        )
        if q != order[0]:
            left(near_region(0, q), far_send.at[q])
    left(partial.at[0, 3], first_send.at[0])
    for b in range(2):
        left(back.at[b], back_send.at[b])


def front(
    conv_in, in_gate, out_gate, doc_ids, conv_taps, head_gain, out_proj, resid, norm_gain,
    route_ids, route_weight, w_gate, w_up, w_down,
):
    tp_count = lax.axis_size("tp")
    channels, width = out_proj.shape
    positions = conv_in.shape[1]
    rows = resid.shape[0]
    half, subs = rows // 2, rows // SUB
    first, planes = half // SUB, tp_count // 2
    top = route_ids.shape[1]
    local_experts, _, hidden_width = w_gate.shape
    slot = max(2, rows // 8)
    hbm = pl.BlockSpec(memory_space=pltpu.HBM)
    dma = pltpu.SemaphoreType.DMA
    return pl.pallas_call(
        functools.partial(front_kernel, tp_count),
        out_shape=[pltpu.VMEM((half, width), jnp.bfloat16)] * 2,
        in_specs=[hbm] * 14,
        out_specs=[pl.BlockSpec(memory_space=pltpu.VMEM)] * 2,
        scratch_shapes=[
            pltpu.VMEM((4, top, rows), jnp.int32),
            pltpu.VMEM((4, top, rows), jnp.float32),
            pltpu.VMEM((channels, SUB + positions), jnp.bfloat16),
            pltpu.VMEM((channels, SUB + positions), jnp.bfloat16),
            pltpu.VMEM((channels, positions), jnp.bfloat16),
            pltpu.VMEM((1, SUB + positions), jnp.int32),
            pltpu.VMEM((3, channels), jnp.float32),
            pltpu.VMEM((1, channels), jnp.float32),
            pltpu.VMEM((1, width), jnp.float32),
            pltpu.VMEM((tp_count * channels, width), jnp.bfloat16),
            pltpu.VMEM((rows, width), jnp.bfloat16),
            pltpu.VMEM((4, channels, SUB), jnp.float32),
            pltpu.VMEM((subs, tp_count, SUB, channels), jnp.bfloat16),
            pltpu.VMEM((subs, SUB, tp_count * channels), jnp.bfloat16),
            pltpu.VMEM((2, 4, half, width), jnp.bfloat16),
            pltpu.VMEM((rows, width), jnp.float32),
            pltpu.VMEM((2, width, hidden_width), jnp.bfloat16),
            pltpu.VMEM((2, width, hidden_width), jnp.bfloat16),
            pltpu.VMEM((2, hidden_width, width), jnp.bfloat16),
            pltpu.VMEM((2, 4, 8, half), jnp.float32),
            pltpu.VMEM((2, 4, 8, half), jnp.float32),
            pltpu.VMEM((2, 4, 8, half), jnp.float32),
            pltpu.VMEM((2, 4, local_experts * slot, half), jnp.bfloat16),
            pltpu.VMEM((2, local_experts, 4 * slot, 128), jnp.float32),
            pltpu.VMEM((local_experts, 4 * slot, width), jnp.bfloat16),
            pltpu.VMEM((4 * slot, hidden_width), jnp.bfloat16),
            pltpu.VMEM((2, 4, half, width), jnp.bfloat16),
            pltpu.VMEM((2, 2, half // 2, width), jnp.bfloat16),
            pltpu.VMEM((2, 2, half, width), jnp.bfloat16),
            pltpu.VMEM((2, EARLY, width), jnp.bfloat16),
            pltpu.VMEM((2, EARLY, tp_count * channels), jnp.bfloat16),
            dma((11,)),
            dma((3,)),
            dma((3,)),
            dma((2,)),
            dma((2,)),
            dma((2,)),
            dma((planes,)),
            dma((1,)),
            dma((2, planes - 1)),
            dma((1,)),
            dma((planes - 1,)),
            dma((1,)),
            dma((4, planes - 1)),
            dma((subs,)),
            dma((subs,)),
            dma((subs,)),
            dma((2, subs)),
            dma((subs,)),
            dma((subs,)),
            dma((3, 2)),
            dma((2,)),
            dma((2, 2)),
            dma((2,)),
            dma((2, 2)),
            dma((2, 2)),
            dma((1,)),
            dma((1,)),
            dma((2,)),
            dma((2,)),
        ],
        compiler_params=pltpu.CompilerParams(
            collective_id=0, has_side_effects=True, vmem_limit_bytes=59944 * 1024
        ),
        name="front",
    )(
        conv_in,
        in_gate,
        out_gate,
        doc_ids[None],
        conv_taps.T,
        head_gain[None],
        out_proj,
        resid,
        norm_gain[None],
        route_ids.T,
        route_weight.T,
        w_gate,
        w_up,
        w_down,
    )


def body(
    conv_in,
    in_gate,
    out_gate,
    doc_ids,
    conv_taps,
    head_gain,
    out_proj,
    resid,
    norm_gain,
    route_ids,
    route_weight,
    w_gate,
    w_up,
    w_down,
):
    channels, width = out_proj.shape
    rows = resid.shape[0]
    half = rows // 2
    slot = max(2, rows // 8)
    sp_count, tp_count = lax.axis_size("sp"), lax.axis_size("tp")
    local_experts = w_gate.shape[0]
    if (
        sp_count == 4
        and tp_count >= 4
        and tp_count & (tp_count - 1) == 0
        and channels == SUB
        and channels % HEAD == 0
        and width % 1024 == 0
        and rows % (2 * SUB) == 0
        and conv_in.shape[1] == tp_count * rows
        and rows <= 2 * local_experts * slot
    ):
        halves = front(
            conv_in,
            in_gate,
            out_gate,
            doc_ids,
            conv_taps,
            head_gain,
            out_proj,
            resid,
            norm_gain,
            route_ids,
            route_weight,
            w_gate,
            w_up,
            w_down,
        )
        return jnp.concatenate(halves, axis=0)
    gated_in = in_gate.astype(jnp.float32) * conv_in.astype(jnp.float32)
    doc_value = doc_ids.astype(jnp.float32)
    edge = jnp.concatenate([gated_in[:, -2:], doc_value[None, -2:]], axis=0)
    edge = shifted(edge, "sp", 1)
    earlier_in, earlier_doc = edge[:-1], edge[-1]
    padded_in = jnp.concatenate([earlier_in, gated_in], axis=1)
    padded_doc = jnp.concatenate([earlier_doc, doc_value])
    same_one = (padded_doc[1:-1] == doc_value).astype(jnp.float32)
    same_two = (padded_doc[:-2] == doc_value).astype(jnp.float32)
    conv_out = (
        conv_taps[:, 2:3] * gated_in
        + conv_taps[:, 1:2] * (padded_in[:, 1:-1] * same_one)
        + conv_taps[:, 0:1] * (padded_in[:, :-2] * same_two)
    )
    gated_out = out_gate.astype(jnp.float32) * conv_out
    by_head = gated_out.reshape(channels // HEAD, HEAD, -1)
    by_head = by_head * lax.rsqrt(jnp.mean(by_head * by_head, axis=1, keepdims=True) + norm_eps)
    head_normed = (by_head.reshape(channels, -1) * head_gain[:, None]).astype(jnp.bfloat16)
    by_row = lax.all_to_all(head_normed, "tp", split_axis=1, concat_axis=0, tiled=True)
    mixed = lax.dot_general(
        by_row,
        lax.all_gather(out_proj, "tp", axis=0, tiled=True),
        (((0,), (0,)), ((), ())),
        preferred_element_type=jnp.float32,
    )
    stream = resid.astype(jnp.float32) + mixed
    expert_in = (
        stream * lax.rsqrt(jnp.mean(stream * stream, axis=1, keepdims=True) + norm_eps) * norm_gain
    ).astype(jnp.bfloat16)
    experts_total = local_experts * sp_count
    parts = []
    for block_no in range(2):
        block_ids = route_ids[block_no * half : (block_no + 1) * half]
        place = slot_places(block_ids, slot, experts_total)
        send = pack_rows(
            place, expert_in[block_no * half : (block_no + 1) * half], experts_total * slot
        ).reshape(sp_count, local_experts, slot, width)
        arrived = lax.all_to_all(send, "sp", split_axis=0, concat_axis=0, tiled=True)
        gate_part = jnp.einsum(
            "nesd,edf->nesf", arrived, w_gate, preferred_element_type=jnp.float32
        )
        up_part = jnp.einsum("nesd,edf->nesf", arrived, w_up, preferred_element_type=jnp.float32)
        hidden = (jax.nn.silu(gate_part) * up_part).astype(jnp.bfloat16)
        arrived = jnp.einsum(
            "nesf,efd->nesd", hidden, w_down, preferred_element_type=jnp.float32
        ).astype(jnp.bfloat16)
        returned = lax.all_to_all(arrived, "sp", split_axis=0, concat_axis=0, tiled=True).reshape(
            experts_total * slot, width
        )
        parts.append(
            combine_rows(returned, place, route_weight[block_no * half : (block_no + 1) * half])
        )
    mixture = jnp.concatenate(parts, axis=0)
    return (stream + mixture).astype(jnp.bfloat16)


def solution(mesh):
    return jax.shard_map(
        body,
        mesh=mesh,
        in_specs=(
            P("tp", "sp"),
            P("tp", "sp"),
            P("tp", "sp"),
            P("sp"),
            P("tp", None),
            P("tp"),
            P("tp", None),
            P(("sp", "tp"), None),
            P(),
            P(("sp", "tp"), None),
            P(("sp", "tp"), None),
            P("sp", None, None),
            P("sp", None, None),
            P("sp", None, None),
        ),
        out_specs=P(("sp", "tp"), None),
        check_vma=False,
    )
```

```python
import functools

import jax
import jax.numpy as jnp
from jax import lax
from jax.experimental import pallas as pl
from jax.experimental.pallas import tpu as pltpu
from jax.sharding import PartitionSpec as P

HEAD = 64


norm_eps = 1e-06


def shifted(value, axis, steps):
    count = lax.axis_size(axis)
    leading, last = (max(0, -steps), min(count, count - steps))
    return lax.ppermute(value, axis, [(source, source + steps) for source in range(leading, last)])


def slot_places(ids_block, slot, experts):
    flat = ids_block.reshape(-1)
    marks = (flat[:, None] == jnp.arange(experts, dtype=jnp.int32)[None, :]).astype(jnp.int32)
    before = jnp.sum((jnp.cumsum(marks, axis=0) - 1) * marks, axis=1)
    return (flat * slot + before).reshape(ids_block.shape)


def pack_rows(places, normed_rows, total_slots):
    targets = jnp.arange(total_slots, dtype=jnp.int32)
    table = jnp.any(targets[:, None, None] == places[None, :, :], axis=2).astype(jnp.bfloat16)
    return jnp.dot(table, normed_rows, preferred_element_type=jnp.float32).astype(jnp.bfloat16)


def combine_rows(returned, places, weights):
    totals = jnp.zeros((places.shape[0], returned.shape[1]), jnp.float32)
    for choice_k in range(places.shape[1]):
        totals = totals + weights[:, choice_k : choice_k + 1] * returned[
            places[:, choice_k]
        ].astype(jnp.float32)
    return totals


MESH = pl.DeviceIdType.MESH
SUB = 128
EARLY = 64


def front_kernel(
    tp_count,
    conv_in,
    in_gate,
    out_gate,
    doc_ids,
    taps_in,
    gain_in,
    out_proj,
    resid,
    norm_gain_in,
    ids,
    weights,
    w_gate,
    w_up,
    w_down,
    out_low,
    out_high,
    ids_out,
    weights_out,
    in_buf,
    gate_buf,
    after_buf,
    doc_buf,
    taps,
    gain,
    norm_gain,
    proj,
    resid_buf,
    spread,
    outgoing,
    by_row,
    gathered,
    stream,
    gate_now,
    up_now,
    down_now,
    marks,
    share,
    rank,
    table,
    slot_weight,
    packed,
    hidden,
    partial,
    inbox,
    back,
    early_resid,
    early_normed,
    scales,
    local_sem,
    edge_send,
    edge_recv,
    list_send,
    list_recv,
    slice_send,
    slice_recv,
    plane_send,
    plane_recv,
    corner_send,
    corner_recv,
    core_send,
    core_recv,
    trade_send,
    trade_recv,
    near_send,
    near_recv,
    far_send,
    far_recv,
    weight_sem,
    first_send,
    first_recv,
    back_send,
    straight_recv,
    merged_recv,
    resid_send,
    resid_recv,
    normed_send,
    normed_recv,
    scale_send,
    scale_recv,
):
    sp, tp = lax.axis_index("sp"), lax.axis_index("tp")
    z, core = tp // 2, tp % 2
    channels, width = out_proj.shape
    rows = resid.shape[0]
    half, subs = rows // 2, rows // SUB
    first = half // SUB
    planes = tp_count // 2
    near_of = [sp ^ 1, sp ^ 2]
    diagonal = sp ^ 3

    def remote(source, target, send_sem, recv_sem, to_sp, to_tp):
        return pltpu.make_async_remote_copy(
            src_ref=source,
            dst_ref=target,
            send_sem=send_sem,
            recv_sem=recv_sem,
            device_id=(to_sp, to_tp),
            device_id_type=MESH,
        )

    def send(source, target, send_sem, recv_sem, to_sp, to_tp):
        remote(source, target, send_sem, recv_sem, to_sp, to_tp).start()

    def left(region, send_sem):
        remote(region, region, send_sem, send_sem, near_of[0], tp).wait_send()

    def arrive(region, recv_sem):
        remote(region, region, recv_sem, recv_sem, near_of[0], tp).wait_recv()

    tail = conv_in.shape[1] - SUB
    loads = [
        pltpu.make_async_copy(conv_in, in_buf.at[:, pl.ds(SUB, conv_in.shape[1])], local_sem.at[0]),
        pltpu.make_async_copy(in_gate, gate_buf.at[:, pl.ds(SUB, conv_in.shape[1])], local_sem.at[1]),
        pltpu.make_async_copy(out_gate, after_buf, local_sem.at[2]),
        pltpu.make_async_copy(doc_ids, doc_buf.at[:, pl.ds(SUB, conv_in.shape[1])], local_sem.at[3]),
        pltpu.make_async_copy(taps_in, taps, local_sem.at[6]),
        pltpu.make_async_copy(gain_in, gain, local_sem.at[7]),
        pltpu.make_async_copy(
            out_proj, proj.at[pl.ds(pl.multiple_of(tp * channels, channels), channels)], local_sem.at[4]
        ),
        pltpu.make_async_copy(resid, resid_buf, local_sem.at[5]),
        pltpu.make_async_copy(norm_gain_in, norm_gain, local_sem.at[8]),
        pltpu.make_async_copy(ids, ids_out.at[0], local_sem.at[9]),
        pltpu.make_async_copy(weights, weights_out.at[0], local_sem.at[10]),
    ]
    for copy in loads:
        copy.start()

    barrier = pltpu.get_barrier_semaphore()
    for d in range(1, tp_count):
        pl.semaphore_signal(barrier, inc=1, device_id=(sp, tp ^ d), device_id_type=MESH)
    for d in range(1, 4):
        pl.semaphore_signal(barrier, inc=1, device_id=(sp ^ d, tp), device_id_type=MESH)
    pl.semaphore_wait(barrier, tp_count + 2)

    after, before = (sp + 1) % 4, (sp + 3) % 4
    edge = pl.ds(0, SUB)
    for at, (source, target) in enumerate(
        ((conv_in, in_buf), (in_gate, gate_buf), (doc_ids, doc_buf))
    ):
        send(
            source.at[:, pl.ds(tail, SUB)],
            target.at[:, edge],
            edge_send.at[at],
            edge_recv.at[at],
            after,
            tp,
        )

    eighth = width // 8

    def columns(place, side):
        return pl.ds(pl.multiple_of(place * (2 * eighth) + side * eighth, eighth), eighth)

    my_rows = pl.ds(pl.multiple_of(tp * channels, channels), channels)
    early = EARLY
    slices = []
    for d in range(2, tp_count):
        side = core ^ (d & 1)
        copy = remote(
            out_proj.at[:, columns(sp, side)],
            proj.at[my_rows, columns(sp, side)],
            slice_send.at[1],
            slice_recv.at[d // 2],
            sp,
            tp ^ d,
        )
        slices.append(copy)

    for copy in slices:
        copy.start()
    for k in range(2):
        send(
            resid.at[pl.ds(rows - early, early)],
            early_resid.at[k],
            resid_send.at[0],
            resid_recv.at[0],
            near_of[k],
            tp,
        )
    send(out_proj, proj.at[my_rows], slice_send.at[0], slice_recv.at[0], sp, tp ^ 1)
    for d in range(1, 4):
        send(ids, ids_out.at[d], list_send.at[0], list_recv.at[0], sp ^ d, tp)
        send(weights, weights_out.at[d], list_send.at[1], list_recv.at[1], sp ^ d, tp)
    for copy in loads[:6]:
        copy.wait()
    for k in range(3):
        spread[k] = jnp.broadcast_to(taps[k : k + 1, :], (channels, channels)).T
    spread[3] = jnp.broadcast_to(gain[...], (channels, channels)).T
    def piece(owner, q):
        base = pl.multiple_of(owner * rows + q * SUB, SUB)
        wide = pl.ds(base, 2 * SUB)
        gated = gate_buf[:, wide].astype(jnp.float32) * in_buf[:, wide].astype(jnp.float32)
        docs = jnp.broadcast_to(doc_buf[:, wide], (8, 2 * SUB))
        now = docs[:, SUB:]
        same_one = (pltpu.roll(docs, 1, 1)[:, SUB:] == now).astype(jnp.float32)[:1]
        same_two = (pltpu.roll(docs, 2, 1)[:, SUB:] == now).astype(jnp.float32)[:1]
        conv = (
            spread[2] * gated[:, SUB:]
            + spread[1] * (pltpu.roll(gated, 1, 1)[:, SUB:] * same_one)
            + spread[0] * (pltpu.roll(gated, 2, 1)[:, SUB:] * same_two)
        )
        gated_out = after_buf[:, pl.ds(base, SUB)].astype(jnp.float32) * conv
        by_head = gated_out.reshape(channels // HEAD, HEAD, SUB)
        by_head = by_head * lax.rsqrt(
            jnp.mean(by_head * by_head, axis=1, keepdims=True) + norm_eps
        )
        normed = by_head.reshape(channels, SUB) * spread[3]
        return normed.T.astype(jnp.bfloat16)

    my_channels = pl.ds(pl.multiple_of(tp * channels, channels), channels)

    def trade(q, d):
        return remote(
            outgoing.at[q, d],
            by_row.at[q, :, my_channels],
            trade_send.at[q],
            trade_recv.at[q],
            sp,
            tp ^ d,
        )

    def start_trade(q):
        def begin(at, carry):
            trade(q, tp_count - 1 - at).start()
            return carry

        lax.fori_loop(0, tp_count - 1, begin, 0)

    def sent_trade(q):
        left(outgoing.at[q, pl.ds(1, tp_count - 1)], trade_send.at[q])

    def block_rows(step):
        deep = 2 * channels
        return pl.ds(pl.multiple_of((z ^ step) * deep, deep), deep)

    def part_rows(step, upper):
        deep = 2 * channels
        return pl.ds(pl.multiple_of((z ^ step) * deep + upper * channels, channels), channels)

    def spread_slice(step):
        region = proj.at[block_rows(step), columns(sp, core)]
        arrive(region, slice_recv.at[step])
        for k in range(2):
            send(region, region, plane_send.at[0], plane_recv.at[k, step - 1], near_of[k], tp)
        send(region, region, core_send.at[0], core_recv.at[0, step - 1], sp, tp ^ 1)

    def spread_plane(step):
        for k in range(2):
            region = proj.at[block_rows(step), columns(near_of[k], core)]
            arrive(region, plane_recv.at[k, step - 1])
            part = proj.at[part_rows(step, k), columns(near_of[k], core)]
            send(part, part, corner_send.at[0], corner_recv.at[step - 1], near_of[1 - k], tp)
            send(region, region, core_send.at[0], core_recv.at[1 + k, step - 1], sp, tp ^ 1)

    def spread_corner(step):
        region = proj.at[block_rows(step), columns(diagonal, core)]
        arrive(region, corner_recv.at[step - 1])
        send(region, region, core_send.at[0], core_recv.at[3, step - 1], sp, tp ^ 1)

    places = (sp, near_of[0], near_of[1], diagonal)

    def other_half(k):
        for step in range(1, planes):
            arrive(
                proj.at[block_rows(step), columns(places[k], 1 - core)],
                core_recv.at[k, step - 1],
            )

    order = [1, 0, *range(2, subs)]

    def convolve(q):
        def one(at, carry):
            d = tp_count - 1 - at
            outgoing[q, d] = piece(tp ^ d, q)
            return carry

        lax.fori_loop(0, tp_count - 1, one, 0)
        by_row[q, :, my_channels] = piece(tp, q)

    convolve(1)
    for step in range(1, planes):
        spread_slice(step)
    left(proj.at[pl.ds(0, 2 * (planes - 1) * channels // 8)], slice_send.at[1])
    start_trade(order[0])
    for k, target in enumerate((in_buf, gate_buf, doc_buf)):
        arrive(target.at[:, edge], edge_recv.at[k])
    doc_buf[:, edge] = jnp.where(sp == 0, -1, doc_buf[:, edge])
    convolve(0)
    for step in range(1, planes):
        spread_plane(step)

    tile = width // 4
    local_experts, _, hidden_width = w_gate.shape
    slot = table.shape[2] // local_experts

    def load_weights(at):
        side, expert = at % 2, at % local_experts
        return [
            pltpu.make_async_copy(source.at[expert], target.at[side], weight_sem.at[k, side])
            for k, (source, target) in enumerate(
                ((w_gate, gate_now), (w_up, up_now), (w_down, down_now))
            )
        ]

    for at in range(2):
        for copy in load_weights(at):
            copy.start()

    def make_tables():
        arrive(ids_out.at[pl.ds(1, 3)], list_recv.at[0])
        arrive(weights_out.at[pl.ds(1, 3)], list_recv.at[1])
        deep = marks.shape[2]
        line = lax.broadcasted_iota(jnp.int32, (deep, half), 0)
        experts = sp * local_experts + line
        ahead = (
            lax.broadcasted_iota(jnp.int32, (half, half), 0)
            < lax.broadcasted_iota(jnp.int32, (half, half), 1)
        ).astype(jnp.bfloat16)
        for b in range(2):
            for n in range(4):
                hits, amount = jnp.zeros((deep, half)), jnp.zeros((deep, half))
                for k in range(ids.shape[0]):
                    here = pl.ds(b * half, half)
                    hit = (ids_out[n, pl.ds(k, 1), here] == experts) & (line < local_experts)
                    hits = hits + hit.astype(jnp.float32)
                    amount = amount + jnp.where(hit, weights_out[n, pl.ds(k, 1), here], 0.0)
                marks[b, n] = hits
                share[b, n] = amount
            flat = marks[b].reshape(4 * deep, half)
            order_of = jnp.dot(flat.astype(jnp.bfloat16), ahead, preferred_element_type=jnp.float32)
            rank[b] = jnp.where(flat > 0, order_of, -1.0).reshape(4, deep, half)

            def fill(n, carry, b=b):
                spots = lax.broadcasted_iota(jnp.int32, (slot, half), 0).astype(jnp.float32)
                for e in range(local_experts):
                    chosen = rank[b, n, pl.ds(e, 1), :] == spots
                    table[b, n, pl.ds(e * slot, slot), :] = chosen.astype(jnp.float32).astype(
                        jnp.bfloat16
                    )
                    total = jnp.sum(
                        jnp.where(chosen, share[b, n, pl.ds(e, 1), :], 0.0), axis=1, keepdims=True
                    )
                    slot_weight[b, e, pl.ds(pl.multiple_of(n * slot, slot), slot), :] = (
                        jnp.broadcast_to(total, (slot, slot_weight.shape[3]))
                    )
                return carry

            lax.fori_loop(0, 4, fill, 0)

    def early_region(place, k):
        part = pl.ds(half - early + k * (early // 2), early // 2)
        return gathered.at[1, place, part]

    def project_early():
        arrive(early_resid, resid_recv.at[0])
        arrive(early_normed, normed_recv.at[0])
        deep = 2 * early

        def stream_of(n):
            cols = pl.ds(pl.multiple_of(n * tile, tile), tile)
            value = early_resid[:, :, cols].astype(jnp.float32).reshape(deep, tile)
            return cols, value + jnp.dot(
                early_normed[...].reshape(deep, tp_count * channels),
                proj[:, cols],
                preferred_element_type=jnp.float32,
            )

        def project(n, total):
            value = stream_of(n)[1]
            return total + jnp.sum(value * value, axis=1, keepdims=True)

        total = lax.fori_loop(0, 4, project, jnp.zeros((deep, 1), jnp.float32))
        scale = lax.rsqrt(total / width + norm_eps)

        def normalize(n, carry):
            cols, value = stream_of(n)
            value = (value * scale * norm_gain[:, cols]).astype(jnp.bfloat16)
            for k in range(2):
                gathered[1, 1 + k, pl.ds(half - early, early), cols] = value[
                    k * early : (k + 1) * early
                ]
            return carry

        lax.fori_loop(0, 4, normalize, 0)
        for k in range(2):
            send(
                early_region(1 + k, k),
                early_region(3, k),
                normed_send.at[1],
                normed_recv.at[1],
                near_of[1 - k],
                tp,
            )

    def span(q):
        return SUB - early if q == subs - 1 else SUB

    def near_region(place, q):
        return gathered.at[q // first, place, pl.ds(q % first * SUB, span(q))]

    def far_region(q, k, place=3):
        part = span(q) // 2
        return gathered.at[q // first, place, pl.ds(q % first * SUB + k * part, part)]

    def got_rows(q):
        arrive(by_row.at[q, :, pl.ds(0, (tp_count - 1) * channels)], trade_recv.at[q])

    def project_tile(q, place):
        mine = pl.ds(q * SUB, SUB)
        cols = pl.ds(pl.multiple_of(place * tile, tile), tile)
        value = resid_buf[mine, cols].astype(jnp.float32) + jnp.dot(
            by_row[q], proj[:, cols], preferred_element_type=jnp.float32
        )
        stream[mine, cols] = value
        return jnp.sum(value * value, axis=1, keepdims=True)

    def normalize_rows(q, total):
        mine = pl.ds(q * SUB, SUB)
        there = pl.ds(q % first * SUB, SUB)
        scale = lax.rsqrt(total / width + norm_eps)

        def normalize(n, carry):
            cols = pl.ds(pl.multiple_of(n * tile, tile), tile)
            value = (stream[mine, cols] * scale * norm_gain[:, cols]).astype(jnp.bfloat16)
            gathered[q // first, 0, there, cols] = value
            return carry

        lax.fori_loop(0, 4, normalize, 0)

    def project_rows(q):
        got_rows(q)
        total = lax.fori_loop(
            0, 4, lambda n, total: total + project_tile(q, n), jnp.zeros((SUB, 1), jnp.float32)
        )
        normalize_rows(q, total)

    def spread_tile(q, place):
        cols = pl.ds(pl.multiple_of(place * tile, tile), tile)
        there = pl.ds(q % first * SUB, SUB)
        value = stream[pl.ds(q * SUB, SUB), cols] * norm_gain[:, cols]
        gathered[q // first, 0, there, cols] = value.astype(jnp.bfloat16)
        for k in range(2):
            send(
                gathered.at[q // first, 0, there, cols],
                gathered.at[q // first, 1 + k, there, cols],
                near_send.at[q],
                near_recv.at[k, q],
                near_of[k],
                tp,
            )

    def send_scales(total):
        scale = jnp.broadcast_to(lax.rsqrt(total / width + norm_eps), (SUB, SUB))
        scales[0] = scale.T[:8]
        for d in range(1, 4):
            send(scales.at[0], scales.at[d], scale_send.at[0], scale_recv.at[0], sp ^ d, tp)

    def place_scales():
        arrive(scales.at[pl.ds(1, 3)], scale_recv.at[0])

        def fill(n, carry):
            ones = jnp.ones((1, SUB), jnp.float32)
            line = jnp.concatenate(
                [scales[n, 0:1, :] if q == order[0] else ones for q in range(first)], axis=1
            )
            lanes = lax.broadcasted_iota(jnp.int32, (slot, slot_weight.shape[3]), 1)
            for e in range(local_experts):
                chosen = table[0, n, pl.ds(e * slot, slot), :].astype(jnp.float32)
                total = jnp.sum(chosen * line, axis=1, keepdims=True)
                here = pl.ds(pl.multiple_of(n * slot, slot), slot)
                slot_weight[0, e, here, :] = jnp.where(
                    lanes < slot_weight.shape[3] // 2, slot_weight[0, e, here, :], total
                )
            return carry

        lax.fori_loop(0, 4, fill, 0)

    def spread_rows(q):
        for k in range(2):
            send(
                near_region(0, q),
                near_region(1 + k, q),
                near_send.at[q],
                near_recv.at[k, q],
                near_of[k],
                tp,
            )

    def relay_rows(q):
        for k in range(2):
            arrive(near_region(1 + k, q), near_recv.at[k, q])
            send(
                far_region(q, k, 1 + k),
                far_region(q, k),
                far_send.at[q],
                far_recv.at[q],
                near_of[1 - k],
                tp,
            )

    def far_rows(q):
        arrive(near_region(3, q), far_recv.at[q])

    def run_experts(b, between=None):
        def pack(at, carry):
            n, cols = at // 4, pl.ds(pl.multiple_of(at % 4 * tile, tile), tile)
            rows_in = jnp.dot(
                table[b, n], gathered[b, n, :, cols], preferred_element_type=jnp.float32
            ).astype(jnp.bfloat16)
            for e in range(local_experts):
                packed[e, pl.ds(pl.multiple_of(n * slot, slot), slot), cols] = rows_in[
                    e * slot : (e + 1) * slot
                ]
            return carry

        lax.fori_loop(0, 16, pack, 0)

        def expert(e, carry):
            at = b * local_experts + e
            side = at % 2
            for copy in load_weights(at):
                copy.wait()
            piece_width = hidden_width // 2

            def up(c, carry):
                cols = pl.ds(pl.multiple_of(c * piece_width, piece_width), piece_width)
                gate = jnp.dot(
                    packed[e], gate_now[side, :, cols], preferred_element_type=jnp.float32
                )
                value = jnp.dot(
                    packed[e], up_now[side, :, cols], preferred_element_type=jnp.float32
                )
                if b == 0:
                    middle = slot_weight.shape[3] // 2
                    factor = slot_weight[b, e, :, middle : middle + 1]
                    gate, value = gate * factor, value * factor
                hidden[:, cols] = (gate / (1.0 + jnp.exp(-gate)) * value).astype(jnp.bfloat16)
                return carry

            lax.fori_loop(0, 2, up, 0)

            def down(c, carry):
                cols = pl.ds(pl.multiple_of(c * tile, tile), tile)
                value = jnp.dot(
                    hidden[...], down_now[side, :, cols], preferred_element_type=jnp.float32
                )
                packed[e, :, cols] = (value * slot_weight[b, e, :, 0:1]).astype(jnp.bfloat16)
                return carry

            lax.fori_loop(0, 4, down, 0)

            @pl.when(at + 2 < 2 * local_experts)
            def _():
                for copy in load_weights(at + 2):
                    copy.start()

            return carry

        middle = local_experts if between is None else local_experts // 2
        lax.fori_loop(0, middle, expert, 0)
        if between is not None:
            between()
            lax.fori_loop(middle, local_experts, expert, 0)

    def combine(b, n):
        def one(c, carry):
            cols = pl.ds(pl.multiple_of(c * tile, tile), tile)
            pieces = jnp.concatenate(
                [packed[e, pl.ds(n * slot, slot), cols] for e in range(local_experts)], axis=0
            )
            partial[b, n, :, cols] = lax.dot_general(
                table[b, n], pieces, (((0,), (0,)), ((), ())), preferred_element_type=jnp.float32
            ).astype(jnp.bfloat16)
            return carry

        lax.fori_loop(0, 4, one, 0)

    part_of = [pl.ds(k * (half // 2), half // 2) for k in range(2)]

    def send_first(b):
        for k in range(2):
            send(
                partial.at[b, 3, part_of[k]],
                inbox.at[b, k],
                first_send.at[b],
                first_recv.at[b, k],
                near_of[k],
                tp,
            )

    def send_straight(b):
        for k in range(2):
            send(
                partial.at[b, 1 + k, part_of[k]],
                back.at[b, k, part_of[k]],
                back_send.at[b],
                straight_recv.at[b, k],
                near_of[k],
                tp,
            )

    strip = 16

    def merge(b):
        for k in range(2):
            arrive(inbox.at[b, k], first_recv.at[b, k])

            def add(at, carry, k=k):
                there = pl.ds(pl.multiple_of(k * (half // 2) + at * strip, strip), strip)
                here = pl.ds(pl.multiple_of(at * strip, strip), strip)
                partial[b, 2 - k, there, :] = (
                    partial[b, 2 - k, there, :].astype(jnp.float32)
                    + inbox[b, k, here, :].astype(jnp.float32)
                ).astype(jnp.bfloat16)
                return carry

            lax.fori_loop(0, half // 2 // strip, add, 0)
            send(
                partial.at[b, 2 - k, part_of[k]],
                back.at[b, 1 - k, part_of[k]],
                back_send.at[b],
                merged_recv.at[b, k],
                near_of[1 - k],
                tp,
            )

    def finish(b):
        for k in range(2):
            arrive(back.at[b, k, part_of[k]], straight_recv.at[b, k])
        for k in range(2):
            arrive(back.at[b, 1 - k, part_of[k]], merged_recv.at[b, k])

            def add(at, carry, k=k):
                here = pl.ds(pl.multiple_of(k * (half // 2) + at * strip, strip), strip)
                there = pl.ds(pl.multiple_of(b * half + k * (half // 2) + at * strip, strip), strip)
                value = stream[there, :] + partial[b, 0, here, :].astype(jnp.float32)
                value = value + back[b, 0, here, :].astype(jnp.float32)
                (out_low, out_high)[b][here, :] = (
                    value + back[b, 1, here, :].astype(jnp.float32)
                ).astype(jnp.bfloat16)
                return carry

            lax.fori_loop(0, half // 2 // strip, add, 0)

    got_rows(order[0])
    sent_trade(order[0])
    start_trade(order[1])
    for copy in loads[6:]:
        copy.wait()
    arrive(
        proj.at[pl.ds(pl.multiple_of((tp ^ 1) * channels, channels), channels)],
        slice_recv.at[0],
    )
    total = jnp.zeros((SUB, 1), jnp.float32)
    for k in range(4):
        if k == 3:
            for step in range(1, planes):
                spread_corner(step)
        other_half(k)
        total = total + project_tile(order[0], places[k])
        spread_tile(order[0], places[k])
    send_scales(total)
    make_tables()
    for q in range(2, subs):
        convolve(q)
    for at_q in range(1, first):
        sent_trade(order[at_q])
        if at_q + 1 < subs:
            start_trade(order[at_q + 1])
        project_rows(order[at_q])
        spread_rows(order[at_q])
    for at_q in range(first):
        relay_rows(order[at_q])
        late = order[first + at_q]
        sent_trade(late)
        if first + at_q + 1 < subs:
            start_trade(order[first + at_q + 1])
        project_rows(late)
    left(near_region(0, order[0]), far_send.at[order[0]])
    spread_rows(order[first])
    for at_q in range(first):
        far_rows(order[at_q])
    for at_q in range(1, first):
        spread_rows(order[first + at_q])
    for k in range(2):
        send(
            by_row.at[subs - 1, pl.ds(SUB - early, early)],
            early_normed.at[k],
            normed_send.at[0],
            normed_recv.at[0],
            near_of[k],
            tp,
        )
    place_scales()
    run_experts(0, lambda: relay_rows(order[first]))
    combine(0, 3)
    send_first(0)
    for at_q in range(1, first):
        relay_rows(order[first + at_q])
    project_early()
    combine(0, 1)
    combine(0, 2)
    send_straight(0)
    combine(0, 0)
    merge(0)
    for at_q in range(first):
        far_rows(order[first + at_q])
    arrive(gathered.at[1, 3, pl.ds(half - early, early)], normed_recv.at[1])
    run_experts(1)
    combine(1, 3)
    send_first(1)
    combine(1, 1)
    combine(1, 2)
    combine(1, 0)
    left(partial.at[1, 3], first_send.at[1])
    send_straight(1)
    finish(0)
    merge(1)
    finish(1)
    for at, target in enumerate((in_buf, gate_buf, doc_buf)):
        left(target.at[:, edge], edge_send.at[at])
    left(ids_out.at[pl.ds(1, 3)], list_send.at[0])
    left(weights_out.at[pl.ds(1, 3)], list_send.at[1])
    left(proj.at[my_rows], slice_send.at[0])
    left(proj.at[pl.ds(0, (planes - 1) * channels // 2)], plane_send.at[0])
    left(proj.at[pl.ds(0, (planes - 1) * channels // 4)], corner_send.at[0])
    left(proj.at[pl.ds(0, (planes - 1) * channels)], core_send.at[0])
    left(early_resid, resid_send.at[0])
    left(scales.at[pl.ds(1, 3)], scale_send.at[0])
    left(early_normed, normed_send.at[0])
    left(gathered.at[1, 3, pl.ds(half - early, early)], normed_send.at[1])
    for q in range(subs):
        left(
            gathered.at[q // first, pl.ds(0, 2), pl.ds(q % first * SUB, span(q))],
            near_send.at[q],
        )
        if q != order[0]:
            left(near_region(0, q), far_send.at[q])
    left(partial.at[0, 3], first_send.at[0])
    for b in range(2):
        left(back.at[b], back_send.at[b])


def front(
    conv_in, in_gate, out_gate, doc_ids, conv_taps, head_gain, out_proj, resid, norm_gain,
    route_ids, route_weight, w_gate, w_up, w_down,
):
    tp_count = lax.axis_size("tp")
    channels, width = out_proj.shape
    positions = conv_in.shape[1]
    rows = resid.shape[0]
    half, subs = rows // 2, rows // SUB
    first, planes = half // SUB, tp_count // 2
    top = route_ids.shape[1]
    local_experts, _, hidden_width = w_gate.shape
    slot = max(2, rows // 8)
    hbm = pl.BlockSpec(memory_space=pltpu.HBM)
    dma = pltpu.SemaphoreType.DMA
    return pl.pallas_call(
        functools.partial(front_kernel, tp_count),
        out_shape=[pltpu.VMEM((half, width), jnp.bfloat16)] * 2,
        in_specs=[hbm] * 14,
        out_specs=[pl.BlockSpec(memory_space=pltpu.VMEM)] * 2,
        scratch_shapes=[
            pltpu.VMEM((4, top, rows), jnp.int32),
            pltpu.VMEM((4, top, rows), jnp.float32),
            pltpu.VMEM((channels, SUB + positions), jnp.bfloat16),
            pltpu.VMEM((channels, SUB + positions), jnp.bfloat16),
            pltpu.VMEM((channels, positions), jnp.bfloat16),
            pltpu.VMEM((1, SUB + positions), jnp.int32),
            pltpu.VMEM((3, channels), jnp.float32),
            pltpu.VMEM((1, channels), jnp.float32),
            pltpu.VMEM((1, width), jnp.float32),
            pltpu.VMEM((tp_count * channels, width), jnp.bfloat16),
            pltpu.VMEM((rows, width), jnp.bfloat16),
            pltpu.VMEM((4, channels, SUB), jnp.float32),
            pltpu.VMEM((subs, tp_count, SUB, channels), jnp.bfloat16),
            pltpu.VMEM((subs, SUB, tp_count * channels), jnp.bfloat16),
            pltpu.VMEM((2, 4, half, width), jnp.bfloat16),
            pltpu.VMEM((rows, width), jnp.float32),
            pltpu.VMEM((2, width, hidden_width), jnp.bfloat16),
            pltpu.VMEM((2, width, hidden_width), jnp.bfloat16),
            pltpu.VMEM((2, hidden_width, width), jnp.bfloat16),
            pltpu.VMEM((2, 4, 8, half), jnp.float32),
            pltpu.VMEM((2, 4, 8, half), jnp.float32),
            pltpu.VMEM((2, 4, 8, half), jnp.float32),
            pltpu.VMEM((2, 4, local_experts * slot, half), jnp.bfloat16),
            pltpu.VMEM((2, local_experts, 4 * slot, 128), jnp.float32),
            pltpu.VMEM((local_experts, 4 * slot, width), jnp.bfloat16),
            pltpu.VMEM((4 * slot, hidden_width), jnp.bfloat16),
            pltpu.VMEM((2, 4, half, width), jnp.bfloat16),
            pltpu.VMEM((2, 2, half // 2, width), jnp.bfloat16),
            pltpu.VMEM((2, 2, half, width), jnp.bfloat16),
            pltpu.VMEM((2, EARLY, width), jnp.bfloat16),
            pltpu.VMEM((2, EARLY, tp_count * channels), jnp.bfloat16),
            pltpu.VMEM((4, 8, SUB), jnp.float32),
            dma((11,)),
            dma((3,)),
            dma((3,)),
            dma((2,)),
            dma((2,)),
            dma((2,)),
            dma((planes,)),
            dma((1,)),
            dma((2, planes - 1)),
            dma((1,)),
            dma((planes - 1,)),
            dma((1,)),
            dma((4, planes - 1)),
            dma((subs,)),
            dma((subs,)),
            dma((subs,)),
            dma((2, subs)),
            dma((subs,)),
            dma((subs,)),
            dma((3, 2)),
            dma((2,)),
            dma((2, 2)),
            dma((2,)),
            dma((2, 2)),
            dma((2, 2)),
            dma((1,)),
            dma((1,)),
            dma((2,)),
            dma((2,)),
            dma((1,)),
            dma((1,)),
        ],
        compiler_params=pltpu.CompilerParams(
            collective_id=0, has_side_effects=True, vmem_limit_bytes=59944 * 1024
        ),
        name="front",
    )(
        conv_in,
        in_gate,
        out_gate,
        doc_ids[None],
        conv_taps.T,
        head_gain[None],
        out_proj,
        resid,
        norm_gain[None],
        route_ids.T,
        route_weight.T,
        w_gate,
        w_up,
        w_down,
    )


def body(
    conv_in,
    in_gate,
    out_gate,
    doc_ids,
    conv_taps,
    head_gain,
    out_proj,
    resid,
    norm_gain,
    route_ids,
    route_weight,
    w_gate,
    w_up,
    w_down,
):
    channels, width = out_proj.shape
    rows = resid.shape[0]
    half = rows // 2
    slot = max(2, rows // 8)
    sp_count, tp_count = lax.axis_size("sp"), lax.axis_size("tp")
    local_experts = w_gate.shape[0]
    if (
        sp_count == 4
        and tp_count >= 4
        and tp_count & (tp_count - 1) == 0
        and channels == SUB
        and channels % HEAD == 0
        and width % 1024 == 0
        and rows % (2 * SUB) == 0
        and conv_in.shape[1] == tp_count * rows
        and rows <= 2 * local_experts * slot
    ):
        halves = front(
            conv_in,
            in_gate,
            out_gate,
            doc_ids,
            conv_taps,
            head_gain,
            out_proj,
            resid,
            norm_gain,
            route_ids,
            route_weight,
            w_gate,
            w_up,
            w_down,
        )
        return jnp.concatenate(halves, axis=0)
    gated_in = in_gate.astype(jnp.float32) * conv_in.astype(jnp.float32)
    doc_value = doc_ids.astype(jnp.float32)
    edge = jnp.concatenate([gated_in[:, -2:], doc_value[None, -2:]], axis=0)
    edge = shifted(edge, "sp", 1)
    earlier_in, earlier_doc = edge[:-1], edge[-1]
    padded_in = jnp.concatenate([earlier_in, gated_in], axis=1)
    padded_doc = jnp.concatenate([earlier_doc, doc_value])
    same_one = (padded_doc[1:-1] == doc_value).astype(jnp.float32)
    same_two = (padded_doc[:-2] == doc_value).astype(jnp.float32)
    conv_out = (
        conv_taps[:, 2:3] * gated_in
        + conv_taps[:, 1:2] * (padded_in[:, 1:-1] * same_one)
        + conv_taps[:, 0:1] * (padded_in[:, :-2] * same_two)
    )
    gated_out = out_gate.astype(jnp.float32) * conv_out
    by_head = gated_out.reshape(channels // HEAD, HEAD, -1)
    by_head = by_head * lax.rsqrt(jnp.mean(by_head * by_head, axis=1, keepdims=True) + norm_eps)
    head_normed = (by_head.reshape(channels, -1) * head_gain[:, None]).astype(jnp.bfloat16)
    by_row = lax.all_to_all(head_normed, "tp", split_axis=1, concat_axis=0, tiled=True)
    mixed = lax.dot_general(
        by_row,
        lax.all_gather(out_proj, "tp", axis=0, tiled=True),
        (((0,), (0,)), ((), ())),
        preferred_element_type=jnp.float32,
    )
    stream = resid.astype(jnp.float32) + mixed
    expert_in = (
        stream * lax.rsqrt(jnp.mean(stream * stream, axis=1, keepdims=True) + norm_eps) * norm_gain
    ).astype(jnp.bfloat16)
    experts_total = local_experts * sp_count
    parts = []
    for block_no in range(2):
        block_ids = route_ids[block_no * half : (block_no + 1) * half]
        place = slot_places(block_ids, slot, experts_total)
        send = pack_rows(
            place, expert_in[block_no * half : (block_no + 1) * half], experts_total * slot
        ).reshape(sp_count, local_experts, slot, width)
        arrived = lax.all_to_all(send, "sp", split_axis=0, concat_axis=0, tiled=True)
        gate_part = jnp.einsum(
            "nesd,edf->nesf", arrived, w_gate, preferred_element_type=jnp.float32
        )
        up_part = jnp.einsum("nesd,edf->nesf", arrived, w_up, preferred_element_type=jnp.float32)
        hidden = (jax.nn.silu(gate_part) * up_part).astype(jnp.bfloat16)
        arrived = jnp.einsum(
            "nesf,efd->nesd", hidden, w_down, preferred_element_type=jnp.float32
        ).astype(jnp.bfloat16)
        returned = lax.all_to_all(arrived, "sp", split_axis=0, concat_axis=0, tiled=True).reshape(
            experts_total * slot, width
        )
        parts.append(
            combine_rows(returned, place, route_weight[block_no * half : (block_no + 1) * half])
        )
    mixture = jnp.concatenate(parts, axis=0)
    return (stream + mixture).astype(jnp.bfloat16)


def solution(mesh):
    return jax.shard_map(
        body,
        mesh=mesh,
        in_specs=(
            P("tp", "sp"),
            P("tp", "sp"),
            P("tp", "sp"),
            P("sp"),
            P("tp", None),
            P("tp"),
            P("tp", None),
            P(("sp", "tp"), None),
            P(),
            P(("sp", "tp"), None),
            P(("sp", "tp"), None),
            P("sp", None, None),
            P("sp", None, None),
            P("sp", None, None),
        ),
        out_specs=P(("sp", "tp"), None),
        check_vma=False,
    )
```

```python
import functools

import jax
import jax.numpy as jnp
from jax import lax
from jax.experimental import pallas as pl
from jax.experimental.pallas import tpu as pltpu
from jax.sharding import PartitionSpec as P

HEAD = 64


norm_eps = 1e-06


def shifted(value, axis, steps):
    count = lax.axis_size(axis)
    leading, last = (max(0, -steps), min(count, count - steps))
    return lax.ppermute(value, axis, [(source, source + steps) for source in range(leading, last)])


def slot_places(ids_block, slot, experts):
    flat = ids_block.reshape(-1)
    marks = (flat[:, None] == jnp.arange(experts, dtype=jnp.int32)[None, :]).astype(jnp.int32)
    before = jnp.sum((jnp.cumsum(marks, axis=0) - 1) * marks, axis=1)
    return (flat * slot + before).reshape(ids_block.shape)


def pack_rows(places, normed_rows, total_slots):
    targets = jnp.arange(total_slots, dtype=jnp.int32)
    table = jnp.any(targets[:, None, None] == places[None, :, :], axis=2).astype(jnp.bfloat16)
    return jnp.dot(table, normed_rows, preferred_element_type=jnp.float32).astype(jnp.bfloat16)


def combine_rows(returned, places, weights):
    totals = jnp.zeros((places.shape[0], returned.shape[1]), jnp.float32)
    for choice_k in range(places.shape[1]):
        totals = totals + weights[:, choice_k : choice_k + 1] * returned[
            places[:, choice_k]
        ].astype(jnp.float32)
    return totals


MESH = pl.DeviceIdType.MESH
SUB = 128
EARLY = 64


def front_kernel(
    tp_count,
    conv_in,
    in_gate,
    out_gate,
    doc_ids,
    taps_in,
    gain_in,
    out_proj,
    resid,
    norm_gain_in,
    ids,
    weights,
    w_gate,
    w_up,
    w_down,
    out_low,
    out_high,
    ids_out,
    weights_out,
    in_buf,
    gate_buf,
    after_buf,
    doc_buf,
    taps,
    gain,
    norm_gain,
    proj,
    resid_buf,
    spread,
    outgoing,
    by_row,
    gathered,
    stream,
    gate_now,
    up_now,
    down_now,
    marks,
    share,
    rank,
    table,
    slot_weight,
    packed,
    hidden,
    partial,
    inbox,
    back,
    early_resid,
    early_normed,
    scales,
    tails,
    local_sem,
    edge_send,
    edge_recv,
    list_send,
    list_recv,
    slice_send,
    slice_recv,
    plane_send,
    plane_recv,
    corner_send,
    corner_recv,
    core_send,
    core_recv,
    trade_send,
    trade_recv,
    near_send,
    near_recv,
    far_send,
    far_recv,
    weight_sem,
    first_send,
    first_recv,
    back_send,
    straight_recv,
    merged_recv,
    resid_send,
    resid_recv,
    normed_send,
    normed_recv,
    scale_send,
    scale_recv,
):
    sp, tp = lax.axis_index("sp"), lax.axis_index("tp")
    z, core = tp // 2, tp % 2
    channels, width = out_proj.shape
    rows = resid.shape[0]
    half, subs = rows // 2, rows // SUB
    first = half // SUB
    planes = tp_count // 2
    near_of = [sp ^ 1, sp ^ 2]
    diagonal = sp ^ 3

    def remote(source, target, send_sem, recv_sem, to_sp, to_tp):
        return pltpu.make_async_remote_copy(
            src_ref=source,
            dst_ref=target,
            send_sem=send_sem,
            recv_sem=recv_sem,
            device_id=(to_sp, to_tp),
            device_id_type=MESH,
        )

    def send(source, target, send_sem, recv_sem, to_sp, to_tp):
        remote(source, target, send_sem, recv_sem, to_sp, to_tp).start()

    def left(region, send_sem):
        remote(region, region, send_sem, send_sem, near_of[0], tp).wait_send()

    def arrive(region, recv_sem):
        remote(region, region, recv_sem, recv_sem, near_of[0], tp).wait_recv()

    tail = conv_in.shape[1] - SUB
    loads = [
        pltpu.make_async_copy(conv_in, in_buf.at[:, pl.ds(SUB, conv_in.shape[1])], local_sem.at[0]),
        pltpu.make_async_copy(in_gate, gate_buf.at[:, pl.ds(SUB, conv_in.shape[1])], local_sem.at[1]),
        pltpu.make_async_copy(out_gate, after_buf, local_sem.at[2]),
        pltpu.make_async_copy(doc_ids, doc_buf.at[:, pl.ds(SUB, conv_in.shape[1])], local_sem.at[3]),
        pltpu.make_async_copy(taps_in, taps, local_sem.at[6]),
        pltpu.make_async_copy(gain_in, gain, local_sem.at[7]),
        pltpu.make_async_copy(
            out_proj, proj.at[pl.ds(pl.multiple_of(tp * channels, channels), channels)], local_sem.at[4]
        ),
        pltpu.make_async_copy(resid, resid_buf, local_sem.at[5]),
        pltpu.make_async_copy(norm_gain_in, norm_gain, local_sem.at[8]),
        pltpu.make_async_copy(ids, ids_out.at[0], local_sem.at[9]),
        pltpu.make_async_copy(weights, weights_out.at[0], local_sem.at[10]),
    ]
    for copy in loads:
        copy.start()

    barrier = pltpu.get_barrier_semaphore()
    for d in range(1, tp_count):
        pl.semaphore_signal(barrier, inc=1, device_id=(sp, tp ^ d), device_id_type=MESH)
    for d in range(1, 4):
        pl.semaphore_signal(barrier, inc=1, device_id=(sp ^ d, tp), device_id_type=MESH)
    pl.semaphore_wait(barrier, tp_count + 2)

    after, before = (sp + 1) % 4, (sp + 3) % 4
    edge = pl.ds(0, SUB)
    send(
        doc_ids.at[:, pl.ds(tail, SUB)],
        doc_buf.at[:, edge],
        edge_send.at[0],
        edge_recv.at[0],
        after,
        tp,
    )

    eighth = width // 8

    def columns(place, side):
        return pl.ds(pl.multiple_of(place * (2 * eighth) + side * eighth, eighth), eighth)

    my_rows = pl.ds(pl.multiple_of(tp * channels, channels), channels)
    early = EARLY
    slices = []
    for d in range(2, tp_count):
        side = core ^ (d & 1)
        copy = remote(
            out_proj.at[:, columns(sp, side)],
            proj.at[my_rows, columns(sp, side)],
            slice_send.at[1],
            slice_recv.at[d // 2],
            sp,
            tp ^ d,
        )
        slices.append(copy)

    for copy in slices:
        copy.start()
    for k in range(2):
        send(
            resid.at[pl.ds(rows - early, early)],
            early_resid.at[k],
            resid_send.at[0],
            resid_recv.at[0],
            near_of[k],
            tp,
        )
    send(out_proj, proj.at[my_rows], slice_send.at[0], slice_recv.at[0], sp, tp ^ 1)
    for d in range(1, 4):
        send(ids, ids_out.at[d], list_send.at[0], list_recv.at[0], sp ^ d, tp)
        send(weights, weights_out.at[d], list_send.at[1], list_recv.at[1], sp ^ d, tp)
    for copy in loads[:6]:
        copy.wait()
    for k in range(3):
        spread[k] = jnp.broadcast_to(taps[k : k + 1, :], (channels, channels)).T
    spread[3] = jnp.broadcast_to(gain[...], (channels, channels)).T
    for at, source in enumerate((in_buf, gate_buf)):
        last = source[:, pl.ds(tail + SUB, SUB)].astype(jnp.float32).T
        tails[0, at] = last[SUB - 8 :].astype(jnp.bfloat16)
    send(tails.at[0], tails.at[1], edge_send.at[1], edge_recv.at[1], after, tp)
    def piece(owner, q):
        base = pl.multiple_of(owner * rows + q * SUB, SUB)
        wide = pl.ds(base, 2 * SUB)
        gated = gate_buf[:, wide].astype(jnp.float32) * in_buf[:, wide].astype(jnp.float32)
        docs = jnp.broadcast_to(doc_buf[:, wide], (8, 2 * SUB))
        now = docs[:, SUB:]
        same_one = (pltpu.roll(docs, 1, 1)[:, SUB:] == now).astype(jnp.float32)[:1]
        same_two = (pltpu.roll(docs, 2, 1)[:, SUB:] == now).astype(jnp.float32)[:1]
        conv = (
            spread[2] * gated[:, SUB:]
            + spread[1] * (pltpu.roll(gated, 1, 1)[:, SUB:] * same_one)
            + spread[0] * (pltpu.roll(gated, 2, 1)[:, SUB:] * same_two)
        )
        gated_out = after_buf[:, pl.ds(base, SUB)].astype(jnp.float32) * conv
        by_head = gated_out.reshape(channels // HEAD, HEAD, SUB)
        by_head = by_head * lax.rsqrt(
            jnp.mean(by_head * by_head, axis=1, keepdims=True) + norm_eps
        )
        normed = by_head.reshape(channels, SUB) * spread[3]
        return normed.T.astype(jnp.bfloat16)

    my_channels = pl.ds(pl.multiple_of(tp * channels, channels), channels)

    def trade(q, d):
        return remote(
            outgoing.at[q, d],
            by_row.at[q, :, my_channels],
            trade_send.at[q],
            trade_recv.at[q],
            sp,
            tp ^ d,
        )

    def start_trade(q):
        def begin(at, carry):
            trade(q, tp_count - 1 - at).start()
            return carry

        lax.fori_loop(0, tp_count - 1, begin, 0)

    def sent_trade(q):
        left(outgoing.at[q, pl.ds(1, tp_count - 1)], trade_send.at[q])

    def block_rows(step):
        deep = 2 * channels
        return pl.ds(pl.multiple_of((z ^ step) * deep, deep), deep)

    def part_rows(step, upper):
        deep = 2 * channels
        return pl.ds(pl.multiple_of((z ^ step) * deep + upper * channels, channels), channels)

    def spread_slice(step):
        region = proj.at[block_rows(step), columns(sp, core)]
        arrive(region, slice_recv.at[step])
        for k in range(2):
            send(region, region, plane_send.at[0], plane_recv.at[k, step - 1], near_of[k], tp)
        send(region, region, core_send.at[0], core_recv.at[0], sp, tp ^ 1)

    def spread_plane(step):
        for k in range(2):
            region = proj.at[block_rows(step), columns(near_of[k], core)]
            arrive(region, plane_recv.at[k, step - 1])
            part = proj.at[part_rows(step, k), columns(near_of[k], core)]
            send(part, part, corner_send.at[0], corner_recv.at[step - 1], near_of[1 - k], tp)
            send(region, region, core_send.at[0], core_recv.at[1 + k], sp, tp ^ 1)

    def spread_corner(step):
        region = proj.at[block_rows(step), columns(diagonal, core)]
        arrive(region, corner_recv.at[step - 1])
        send(region, region, core_send.at[0], core_recv.at[3], sp, tp ^ 1)

    places = (sp, near_of[0], near_of[1], diagonal)

    def other_half(k):
        arrive(proj.at[pl.ds(0, (planes - 1) * channels // 4)], core_recv.at[k])

    order = [1, 0, *range(2, subs)]

    def convolve(q):
        def one(at, carry):
            d = tp_count - 1 - at
            outgoing[q, d] = piece(tp ^ d, q)
            return carry

        lax.fori_loop(0, tp_count - 1, one, 0)
        by_row[q, :, my_channels] = piece(tp, q)

    convolve(1)
    for step in range(1, planes):
        spread_slice(step)
    left(proj.at[pl.ds(0, 2 * (planes - 1) * channels // 8)], slice_send.at[1])
    start_trade(order[0])
    arrive(doc_buf.at[:, edge], edge_recv.at[0])
    arrive(tails.at[1], edge_recv.at[1])
    for at, target in enumerate((in_buf, gate_buf)):
        filler = jnp.zeros((SUB - 8, channels), jnp.float32)
        last = jnp.concatenate([filler, tails[1, at].astype(jnp.float32)], axis=0)
        target[:, edge] = last.T.astype(jnp.bfloat16)
    doc_buf[:, edge] = jnp.where(sp == 0, -1, doc_buf[:, edge])
    convolve(0)
    for step in range(1, planes):
        spread_plane(step)

    tile = width // 4
    local_experts, _, hidden_width = w_gate.shape
    slot = table.shape[2] // local_experts

    def load_weights(at):
        side, expert = at % 2, at % local_experts
        return [
            pltpu.make_async_copy(source.at[expert], target.at[side], weight_sem.at[k, side])
            for k, (source, target) in enumerate(
                ((w_gate, gate_now), (w_up, up_now), (w_down, down_now))
            )
        ]

    for at in range(2):
        for copy in load_weights(at):
            copy.start()

    def make_tables():
        arrive(ids_out.at[pl.ds(1, 3)], list_recv.at[0])
        arrive(weights_out.at[pl.ds(1, 3)], list_recv.at[1])
        deep = marks.shape[2]
        line = lax.broadcasted_iota(jnp.int32, (deep, half), 0)
        experts = sp * local_experts + line
        ahead = (
            lax.broadcasted_iota(jnp.int32, (half, half), 0)
            < lax.broadcasted_iota(jnp.int32, (half, half), 1)
        ).astype(jnp.bfloat16)
        for b in range(2):
            for n in range(4):
                hits, amount = jnp.zeros((deep, half)), jnp.zeros((deep, half))
                for k in range(ids.shape[0]):
                    here = pl.ds(b * half, half)
                    hit = (ids_out[n, pl.ds(k, 1), here] == experts) & (line < local_experts)
                    hits = hits + hit.astype(jnp.float32)
                    amount = amount + jnp.where(hit, weights_out[n, pl.ds(k, 1), here], 0.0)
                marks[b, n] = hits
                share[b, n] = amount
            flat = marks[b].reshape(4 * deep, half)
            order_of = jnp.dot(flat.astype(jnp.bfloat16), ahead, preferred_element_type=jnp.float32)
            rank[b] = jnp.where(flat > 0, order_of, -1.0).reshape(4, deep, half)

            def fill(n, carry, b=b):
                spots = lax.broadcasted_iota(jnp.int32, (slot, half), 0).astype(jnp.float32)
                for e in range(local_experts):
                    chosen = rank[b, n, pl.ds(e, 1), :] == spots
                    table[b, n, pl.ds(e * slot, slot), :] = chosen.astype(jnp.float32).astype(
                        jnp.bfloat16
                    )
                    total = jnp.sum(
                        jnp.where(chosen, share[b, n, pl.ds(e, 1), :], 0.0), axis=1, keepdims=True
                    )
                    slot_weight[b, e, pl.ds(pl.multiple_of(n * slot, slot), slot), :] = (
                        jnp.broadcast_to(total, (slot, slot_weight.shape[3]))
                    )
                return carry

            lax.fori_loop(0, 4, fill, 0)

    def early_region(place, k):
        part = pl.ds(half - early + k * (early // 2), early // 2)
        return gathered.at[1, place, part]

    def project_early():
        arrive(early_resid, resid_recv.at[0])
        arrive(early_normed, normed_recv.at[0])
        deep = 2 * early

        def stream_of(n):
            cols = pl.ds(pl.multiple_of(n * tile, tile), tile)
            value = early_resid[:, :, cols].astype(jnp.float32).reshape(deep, tile)
            return cols, value + jnp.dot(
                early_normed[...].reshape(deep, tp_count * channels),
                proj[:, cols],
                preferred_element_type=jnp.float32,
            )

        def project(n, total):
            value = stream_of(n)[1]
            return total + jnp.sum(value * value, axis=1, keepdims=True)

        total = lax.fori_loop(0, 4, project, jnp.zeros((deep, 1), jnp.float32))
        scale = lax.rsqrt(total / width + norm_eps)

        def normalize(n, carry):
            cols, value = stream_of(n)
            value = (value * scale * norm_gain[:, cols]).astype(jnp.bfloat16)
            for k in range(2):
                gathered[1, 1 + k, pl.ds(half - early, early), cols] = value[
                    k * early : (k + 1) * early
                ]
            return carry

        lax.fori_loop(0, 4, normalize, 0)
        for k in range(2):
            send(
                early_region(1 + k, k),
                early_region(3, k),
                normed_send.at[1],
                normed_recv.at[1],
                near_of[1 - k],
                tp,
            )

    def span(q):
        return SUB - early if q == subs - 1 else SUB

    def near_region(place, q):
        return gathered.at[q // first, place, pl.ds(q % first * SUB, span(q))]

    def far_region(q, k, place=3):
        part = span(q) // 2
        return gathered.at[q // first, place, pl.ds(q % first * SUB + k * part, part)]

    def got_rows(q):
        arrive(by_row.at[q, :, pl.ds(0, (tp_count - 1) * channels)], trade_recv.at[q])

    def project_tile(q, place):
        mine = pl.ds(q * SUB, SUB)
        cols = pl.ds(pl.multiple_of(place * tile, tile), tile)
        value = resid_buf[mine, cols].astype(jnp.float32) + jnp.dot(
            by_row[q], proj[:, cols], preferred_element_type=jnp.float32
        )
        stream[mine, cols] = value
        return jnp.sum(value * value, axis=1, keepdims=True)

    def normalize_rows(q, total):
        mine = pl.ds(q * SUB, SUB)
        there = pl.ds(q % first * SUB, SUB)
        scale = lax.rsqrt(total / width + norm_eps)

        def normalize(n, carry):
            cols = pl.ds(pl.multiple_of(n * tile, tile), tile)
            value = (stream[mine, cols] * scale * norm_gain[:, cols]).astype(jnp.bfloat16)
            gathered[q // first, 0, there, cols] = value
            return carry

        lax.fori_loop(0, 4, normalize, 0)

    def project_rows(q):
        got_rows(q)
        total = lax.fori_loop(
            0, 4, lambda n, total: total + project_tile(q, n), jnp.zeros((SUB, 1), jnp.float32)
        )
        normalize_rows(q, total)

    def spread_tile(q, place):
        cols = pl.ds(pl.multiple_of(place * tile, tile), tile)
        there = pl.ds(q % first * SUB, SUB)
        value = stream[pl.ds(q * SUB, SUB), cols] * norm_gain[:, cols]
        gathered[q // first, 0, there, cols] = value.astype(jnp.bfloat16)
        for k in range(2):
            send(
                gathered.at[q // first, 0, there, cols],
                gathered.at[q // first, 1 + k, there, cols],
                near_send.at[q],
                near_recv.at[k, q],
                near_of[k],
                tp,
            )

    def send_scales(total):
        scale = jnp.broadcast_to(lax.rsqrt(total / width + norm_eps), (SUB, SUB))
        scales[0] = scale.T[:8]
        for d in range(1, 4):
            send(scales.at[0], scales.at[d], scale_send.at[0], scale_recv.at[0], sp ^ d, tp)

    def place_scales():
        arrive(scales.at[pl.ds(1, 3)], scale_recv.at[0])

        def fill(n, carry):
            ones = jnp.ones((1, SUB), jnp.float32)
            line = jnp.concatenate(
                [scales[n, 0:1, :] if q == order[0] else ones for q in range(first)], axis=1
            )
            lanes = lax.broadcasted_iota(jnp.int32, (slot, slot_weight.shape[3]), 1)
            for e in range(local_experts):
                chosen = table[0, n, pl.ds(e * slot, slot), :].astype(jnp.float32)
                total = jnp.sum(chosen * line, axis=1, keepdims=True)
                here = pl.ds(pl.multiple_of(n * slot, slot), slot)
                slot_weight[0, e, here, :] = jnp.where(
                    lanes < slot_weight.shape[3] // 2, slot_weight[0, e, here, :], total
                )
            return carry

        lax.fori_loop(0, 4, fill, 0)

    def spread_rows(q):
        for k in range(2):
            send(
                near_region(0, q),
                near_region(1 + k, q),
                near_send.at[q],
                near_recv.at[k, q],
                near_of[k],
                tp,
            )

    def relay_rows(q):
        for k in range(2):
            arrive(near_region(1 + k, q), near_recv.at[k, q])
            send(
                far_region(q, k, 1 + k),
                far_region(q, k),
                far_send.at[q],
                far_recv.at[q],
                near_of[1 - k],
                tp,
            )

    def far_rows(q):
        arrive(near_region(3, q), far_recv.at[q])

    def run_experts(b, between=None):
        def pack(at, carry):
            n, cols = at // 4, pl.ds(pl.multiple_of(at % 4 * tile, tile), tile)
            rows_in = jnp.dot(
                table[b, n], gathered[b, n, :, cols], preferred_element_type=jnp.float32
            ).astype(jnp.bfloat16)
            for e in range(local_experts):
                packed[e, pl.ds(pl.multiple_of(n * slot, slot), slot), cols] = rows_in[
                    e * slot : (e + 1) * slot
                ]
            return carry

        lax.fori_loop(0, 16, pack, 0)

        def expert(e, carry):
            at = b * local_experts + e
            side = at % 2
            for copy in load_weights(at):
                copy.wait()
            piece_width = hidden_width // 2

            def up(c, carry):
                cols = pl.ds(pl.multiple_of(c * piece_width, piece_width), piece_width)
                gate = jnp.dot(
                    packed[e], gate_now[side, :, cols], preferred_element_type=jnp.float32
                )
                value = jnp.dot(
                    packed[e], up_now[side, :, cols], preferred_element_type=jnp.float32
                )
                if b == 0:
                    middle = slot_weight.shape[3] // 2
                    factor = slot_weight[b, e, :, middle : middle + 1]
                    gate, value = gate * factor, value * factor
                hidden[:, cols] = (gate / (1.0 + jnp.exp(-gate)) * value).astype(jnp.bfloat16)
                return carry

            lax.fori_loop(0, 2, up, 0)

            def down(c, carry):
                cols = pl.ds(pl.multiple_of(c * tile, tile), tile)
                value = jnp.dot(
                    hidden[...], down_now[side, :, cols], preferred_element_type=jnp.float32
                )
                packed[e, :, cols] = (value * slot_weight[b, e, :, 0:1]).astype(jnp.bfloat16)
                return carry

            lax.fori_loop(0, 4, down, 0)

            @pl.when(at + 2 < 2 * local_experts)
            def _():
                for copy in load_weights(at + 2):
                    copy.start()

            return carry

        middle = local_experts if between is None else local_experts // 2
        lax.fori_loop(0, middle, expert, 0)
        if between is not None:
            between()
            lax.fori_loop(middle, local_experts, expert, 0)

    def combine(b, n):
        def one(c, carry):
            cols = pl.ds(pl.multiple_of(c * tile, tile), tile)
            pieces = jnp.concatenate(
                [packed[e, pl.ds(n * slot, slot), cols] for e in range(local_experts)], axis=0
            )
            partial[b, n, :, cols] = lax.dot_general(
                table[b, n], pieces, (((0,), (0,)), ((), ())), preferred_element_type=jnp.float32
            ).astype(jnp.bfloat16)
            return carry

        lax.fori_loop(0, 4, one, 0)

    part_of = [pl.ds(k * (half // 2), half // 2) for k in range(2)]

    def send_first(b):
        for k in range(2):
            send(
                partial.at[b, 3, part_of[k]],
                inbox.at[b, k],
                first_send.at[b],
                first_recv.at[b, k],
                near_of[k],
                tp,
            )

    def send_straight(b):
        for k in range(2):
            send(
                partial.at[b, 1 + k, part_of[k]],
                back.at[b, k, part_of[k]],
                back_send.at[b],
                straight_recv.at[b],
                near_of[k],
                tp,
            )

    strip = 32

    def merge(b):
        for k in range(2):
            arrive(inbox.at[b, k], first_recv.at[b, k])

            def add(at, carry, k=k):
                there = pl.ds(pl.multiple_of(k * (half // 2) + at * strip, strip), strip)
                here = pl.ds(pl.multiple_of(at * strip, strip), strip)
                partial[b, 2 - k, there, :] = (
                    partial[b, 2 - k, there, :].astype(jnp.float32)
                    + inbox[b, k, here, :].astype(jnp.float32)
                ).astype(jnp.bfloat16)
                return carry

            lax.fori_loop(0, half // 2 // strip, add, 0)
            send(
                partial.at[b, 2 - k, part_of[k]],
                back.at[b, 1 - k, part_of[k]],
                back_send.at[b],
                merged_recv.at[b],
                near_of[1 - k],
                tp,
            )

    def finish(b):
        arrive(back.at[b, 0], straight_recv.at[b])
        arrive(back.at[b, 1], merged_recv.at[b])
        for k in range(2):

            def add(at, carry, k=k):
                here = pl.ds(pl.multiple_of(k * (half // 2) + at * strip, strip), strip)
                there = pl.ds(pl.multiple_of(b * half + k * (half // 2) + at * strip, strip), strip)
                value = stream[there, :] + partial[b, 0, here, :].astype(jnp.float32)
                value = value + back[b, 0, here, :].astype(jnp.float32)
                (out_low, out_high)[b][here, :] = (
                    value + back[b, 1, here, :].astype(jnp.float32)
                ).astype(jnp.bfloat16)
                return carry

            lax.fori_loop(0, half // 2 // strip, add, 0)

    got_rows(order[0])
    sent_trade(order[0])
    start_trade(order[1])
    for copy in loads[6:]:
        copy.wait()
    arrive(
        proj.at[pl.ds(pl.multiple_of((tp ^ 1) * channels, channels), channels)],
        slice_recv.at[0],
    )
    total = jnp.zeros((SUB, 1), jnp.float32)
    for k in range(4):
        if k == 3:
            for step in range(1, planes):
                spread_corner(step)
        other_half(k)
        total = total + project_tile(order[0], places[k])
        spread_tile(order[0], places[k])
    send_scales(total)
    make_tables()
    for q in range(2, subs):
        convolve(q)
    for at_q in range(1, first):
        sent_trade(order[at_q])
        if at_q + 1 < subs:
            start_trade(order[at_q + 1])
        project_rows(order[at_q])
        spread_rows(order[at_q])
    for at_q in range(first):
        relay_rows(order[at_q])
        late = order[first + at_q]
        sent_trade(late)
        if first + at_q + 1 < subs:
            start_trade(order[first + at_q + 1])
        project_rows(late)
    left(near_region(0, order[0]), far_send.at[order[0]])
    spread_rows(order[first])
    for at_q in range(first):
        far_rows(order[at_q])
    for at_q in range(1, first):
        spread_rows(order[first + at_q])
    for k in range(2):
        send(
            by_row.at[subs - 1, pl.ds(SUB - early, early)],
            early_normed.at[k],
            normed_send.at[0],
            normed_recv.at[0],
            near_of[k],
            tp,
        )
    place_scales()
    run_experts(0, lambda: relay_rows(order[first]))
    combine(0, 3)
    send_first(0)
    for at_q in range(1, first):
        relay_rows(order[first + at_q])
    project_early()
    combine(0, 1)
    combine(0, 2)
    send_straight(0)
    combine(0, 0)
    merge(0)
    for at_q in range(first):
        far_rows(order[first + at_q])
    arrive(gathered.at[1, 3, pl.ds(half - early, early)], normed_recv.at[1])
    run_experts(1)
    combine(1, 3)
    send_first(1)
    combine(1, 1)
    combine(1, 2)
    combine(1, 0)
    left(partial.at[1, 3], first_send.at[1])
    send_straight(1)
    finish(0)
    merge(1)
    finish(1)
    left(doc_buf.at[:, edge], edge_send.at[0])
    left(tails.at[0], edge_send.at[1])
    left(ids_out.at[pl.ds(1, 3)], list_send.at[0])
    left(weights_out.at[pl.ds(1, 3)], list_send.at[1])
    left(proj.at[my_rows], slice_send.at[0])
    left(proj.at[pl.ds(0, (planes - 1) * channels // 2)], plane_send.at[0])
    left(proj.at[pl.ds(0, (planes - 1) * channels // 4)], corner_send.at[0])
    left(proj.at[pl.ds(0, (planes - 1) * channels)], core_send.at[0])
    left(early_resid, resid_send.at[0])
    left(scales.at[pl.ds(1, 3)], scale_send.at[0])
    left(early_normed, normed_send.at[0])
    left(gathered.at[1, 3, pl.ds(half - early, early)], normed_send.at[1])
    for q in range(subs):
        left(
            gathered.at[q // first, pl.ds(0, 2), pl.ds(q % first * SUB, span(q))],
            near_send.at[q],
        )
        if q != order[0]:
            left(near_region(0, q), far_send.at[q])
    left(partial.at[0, 3], first_send.at[0])
    for b in range(2):
        left(back.at[b], back_send.at[b])


def front(
    conv_in, in_gate, out_gate, doc_ids, conv_taps, head_gain, out_proj, resid, norm_gain,
    route_ids, route_weight, w_gate, w_up, w_down,
):
    tp_count = lax.axis_size("tp")
    channels, width = out_proj.shape
    positions = conv_in.shape[1]
    rows = resid.shape[0]
    half, subs = rows // 2, rows // SUB
    first, planes = half // SUB, tp_count // 2
    top = route_ids.shape[1]
    local_experts, _, hidden_width = w_gate.shape
    slot = max(2, rows // 8)
    hbm = pl.BlockSpec(memory_space=pltpu.HBM)
    dma = pltpu.SemaphoreType.DMA
    return pl.pallas_call(
        functools.partial(front_kernel, tp_count),
        out_shape=[pltpu.VMEM((half, width), jnp.bfloat16)] * 2,
        in_specs=[hbm] * 14,
        out_specs=[pl.BlockSpec(memory_space=pltpu.VMEM)] * 2,
        scratch_shapes=[
            pltpu.VMEM((4, top, rows), jnp.int32),
            pltpu.VMEM((4, top, rows), jnp.float32),
            pltpu.VMEM((channels, SUB + positions), jnp.bfloat16),
            pltpu.VMEM((channels, SUB + positions), jnp.bfloat16),
            pltpu.VMEM((channels, positions), jnp.bfloat16),
            pltpu.VMEM((1, SUB + positions), jnp.int32),
            pltpu.VMEM((3, channels), jnp.float32),
            pltpu.VMEM((1, channels), jnp.float32),
            pltpu.VMEM((1, width), jnp.float32),
            pltpu.VMEM((tp_count * channels, width), jnp.bfloat16),
            pltpu.VMEM((rows, width), jnp.bfloat16),
            pltpu.VMEM((4, channels, SUB), jnp.float32),
            pltpu.VMEM((subs, tp_count, SUB, channels), jnp.bfloat16),
            pltpu.VMEM((subs, SUB, tp_count * channels), jnp.bfloat16),
            pltpu.VMEM((2, 4, half, width), jnp.bfloat16),
            pltpu.VMEM((rows, width), jnp.float32),
            pltpu.VMEM((2, width, hidden_width), jnp.bfloat16),
            pltpu.VMEM((2, width, hidden_width), jnp.bfloat16),
            pltpu.VMEM((2, hidden_width, width), jnp.bfloat16),
            pltpu.VMEM((2, 4, 8, half), jnp.float32),
            pltpu.VMEM((2, 4, 8, half), jnp.float32),
            pltpu.VMEM((2, 4, 8, half), jnp.float32),
            pltpu.VMEM((2, 4, local_experts * slot, half), jnp.bfloat16),
            pltpu.VMEM((2, local_experts, 4 * slot, 128), jnp.float32),
            pltpu.VMEM((local_experts, 4 * slot, width), jnp.bfloat16),
            pltpu.VMEM((4 * slot, hidden_width), jnp.bfloat16),
            pltpu.VMEM((2, 4, half, width), jnp.bfloat16),
            pltpu.VMEM((2, 2, half // 2, width), jnp.bfloat16),
            pltpu.VMEM((2, 2, half, width), jnp.bfloat16),
            pltpu.VMEM((2, EARLY, width), jnp.bfloat16),
            pltpu.VMEM((2, EARLY, tp_count * channels), jnp.bfloat16),
            pltpu.VMEM((4, 8, SUB), jnp.float32),
            pltpu.VMEM((2, 2, 8, SUB), jnp.bfloat16),
            dma((11,)),
            dma((2,)),
            dma((2,)),
            dma((2,)),
            dma((2,)),
            dma((2,)),
            dma((planes,)),
            dma((1,)),
            dma((2, planes - 1)),
            dma((1,)),
            dma((planes - 1,)),
            dma((1,)),
            dma((4,)),
            dma((subs,)),
            dma((subs,)),
            dma((subs,)),
            dma((2, subs)),
            dma((subs,)),
            dma((subs,)),
            dma((3, 2)),
            dma((2,)),
            dma((2, 2)),
            dma((2,)),
            dma((2,)),
            dma((2,)),
            dma((1,)),
            dma((1,)),
            dma((2,)),
            dma((2,)),
            dma((1,)),
            dma((1,)),
        ],
        compiler_params=pltpu.CompilerParams(
            collective_id=0, has_side_effects=True, vmem_limit_bytes=59944 * 1024
        ),
        name="front",
    )(
        conv_in,
        in_gate,
        out_gate,
        doc_ids[None],
        conv_taps.T,
        head_gain[None],
        out_proj,
        resid,
        norm_gain[None],
        route_ids.T,
        route_weight.T,
        w_gate,
        w_up,
        w_down,
    )


def body(
    conv_in,
    in_gate,
    out_gate,
    doc_ids,
    conv_taps,
    head_gain,
    out_proj,
    resid,
    norm_gain,
    route_ids,
    route_weight,
    w_gate,
    w_up,
    w_down,
):
    channels, width = out_proj.shape
    rows = resid.shape[0]
    half = rows // 2
    slot = max(2, rows // 8)
    sp_count, tp_count = lax.axis_size("sp"), lax.axis_size("tp")
    local_experts = w_gate.shape[0]
    if (
        sp_count == 4
        and tp_count >= 4
        and tp_count & (tp_count - 1) == 0
        and channels == SUB
        and channels % HEAD == 0
        and width % 1024 == 0
        and rows % (2 * SUB) == 0
        and conv_in.shape[1] == tp_count * rows
        and rows <= 2 * local_experts * slot
    ):
        halves = front(
            conv_in,
            in_gate,
            out_gate,
            doc_ids,
            conv_taps,
            head_gain,
            out_proj,
            resid,
            norm_gain,
            route_ids,
            route_weight,
            w_gate,
            w_up,
            w_down,
        )
        return jnp.concatenate(halves, axis=0)
    gated_in = in_gate.astype(jnp.float32) * conv_in.astype(jnp.float32)
    doc_value = doc_ids.astype(jnp.float32)
    edge = jnp.concatenate([gated_in[:, -2:], doc_value[None, -2:]], axis=0)
    edge = shifted(edge, "sp", 1)
    earlier_in, earlier_doc = edge[:-1], edge[-1]
    padded_in = jnp.concatenate([earlier_in, gated_in], axis=1)
    padded_doc = jnp.concatenate([earlier_doc, doc_value])
    same_one = (padded_doc[1:-1] == doc_value).astype(jnp.float32)
    same_two = (padded_doc[:-2] == doc_value).astype(jnp.float32)
    conv_out = (
        conv_taps[:, 2:3] * gated_in
        + conv_taps[:, 1:2] * (padded_in[:, 1:-1] * same_one)
        + conv_taps[:, 0:1] * (padded_in[:, :-2] * same_two)
    )
    gated_out = out_gate.astype(jnp.float32) * conv_out
    by_head = gated_out.reshape(channels // HEAD, HEAD, -1)
    by_head = by_head * lax.rsqrt(jnp.mean(by_head * by_head, axis=1, keepdims=True) + norm_eps)
    head_normed = (by_head.reshape(channels, -1) * head_gain[:, None]).astype(jnp.bfloat16)
    by_row = lax.all_to_all(head_normed, "tp", split_axis=1, concat_axis=0, tiled=True)
    mixed = lax.dot_general(
        by_row,
        lax.all_gather(out_proj, "tp", axis=0, tiled=True),
        (((0,), (0,)), ((), ())),
        preferred_element_type=jnp.float32,
    )
    stream = resid.astype(jnp.float32) + mixed
    expert_in = (
        stream * lax.rsqrt(jnp.mean(stream * stream, axis=1, keepdims=True) + norm_eps) * norm_gain
    ).astype(jnp.bfloat16)
    experts_total = local_experts * sp_count
    parts = []
    for block_no in range(2):
        block_ids = route_ids[block_no * half : (block_no + 1) * half]
        place = slot_places(block_ids, slot, experts_total)
        send = pack_rows(
            place, expert_in[block_no * half : (block_no + 1) * half], experts_total * slot
        ).reshape(sp_count, local_experts, slot, width)
        arrived = lax.all_to_all(send, "sp", split_axis=0, concat_axis=0, tiled=True)
        gate_part = jnp.einsum(
            "nesd,edf->nesf", arrived, w_gate, preferred_element_type=jnp.float32
        )
        up_part = jnp.einsum("nesd,edf->nesf", arrived, w_up, preferred_element_type=jnp.float32)
        hidden = (jax.nn.silu(gate_part) * up_part).astype(jnp.bfloat16)
        arrived = jnp.einsum(
            "nesf,efd->nesd", hidden, w_down, preferred_element_type=jnp.float32
        ).astype(jnp.bfloat16)
        returned = lax.all_to_all(arrived, "sp", split_axis=0, concat_axis=0, tiled=True).reshape(
            experts_total * slot, width
        )
        parts.append(
            combine_rows(returned, place, route_weight[block_no * half : (block_no + 1) * half])
        )
    mixture = jnp.concatenate(parts, axis=0)
    return (stream + mixture).astype(jnp.bfloat16)


def solution(mesh):
    return jax.shard_map(
        body,
        mesh=mesh,
        in_specs=(
            P("tp", "sp"),
            P("tp", "sp"),
            P("tp", "sp"),
            P("sp"),
            P("tp", None),
            P("tp"),
            P("tp", None),
            P(("sp", "tp"), None),
            P(),
            P(("sp", "tp"), None),
            P(("sp", "tp"), None),
            P("sp", None, None),
            P("sp", None, None),
            P("sp", None, None),
        ),
        out_specs=P(("sp", "tp"), None),
        check_vma=False,
    )
```

```python
import functools

import jax
import jax.numpy as jnp
from jax import lax
from jax.experimental import pallas as pl
from jax.experimental.pallas import tpu as pltpu
from jax.sharding import PartitionSpec as P

HEAD = 64


norm_eps = 1e-06


def shifted(value, axis, steps):
    count = lax.axis_size(axis)
    leading, last = (max(0, -steps), min(count, count - steps))
    return lax.ppermute(value, axis, [(source, source + steps) for source in range(leading, last)])


def slot_places(ids_block, slot, experts):
    flat = ids_block.reshape(-1)
    marks = (flat[:, None] == jnp.arange(experts, dtype=jnp.int32)[None, :]).astype(jnp.int32)
    before = jnp.sum((jnp.cumsum(marks, axis=0) - 1) * marks, axis=1)
    return (flat * slot + before).reshape(ids_block.shape)


def pack_rows(places, normed_rows, total_slots):
    targets = jnp.arange(total_slots, dtype=jnp.int32)
    table = jnp.any(targets[:, None, None] == places[None, :, :], axis=2).astype(jnp.bfloat16)
    return jnp.dot(table, normed_rows, preferred_element_type=jnp.float32).astype(jnp.bfloat16)


def combine_rows(returned, places, weights):
    totals = jnp.zeros((places.shape[0], returned.shape[1]), jnp.float32)
    for choice_k in range(places.shape[1]):
        totals = totals + weights[:, choice_k : choice_k + 1] * returned[
            places[:, choice_k]
        ].astype(jnp.float32)
    return totals


MESH = pl.DeviceIdType.MESH
SUB = 128
EARLY = 64


def front_kernel(
    tp_count,
    conv_in,
    in_gate,
    out_gate,
    doc_ids,
    taps_in,
    gain_in,
    out_proj,
    resid,
    norm_gain_in,
    ids,
    weights,
    w_gate,
    w_up,
    w_down,
    out_low,
    out_high,
    ids_out,
    weights_out,
    in_buf,
    gate_buf,
    after_buf,
    doc_buf,
    taps,
    gain,
    norm_gain,
    proj,
    resid_buf,
    spread,
    outgoing,
    by_row,
    gathered,
    stream,
    gate_now,
    up_now,
    down_now,
    marks,
    share,
    rank,
    table,
    slot_weight,
    packed,
    hidden,
    partial,
    inbox,
    back,
    early_resid,
    early_normed,
    scales,
    tails,
    local_sem,
    edge_send,
    edge_recv,
    list_send,
    list_recv,
    slice_send,
    slice_recv,
    plane_send,
    plane_recv,
    corner_send,
    corner_recv,
    core_send,
    core_recv,
    trade_send,
    trade_recv,
    near_send,
    near_recv,
    far_send,
    far_recv,
    weight_sem,
    first_send,
    first_recv,
    back_send,
    straight_recv,
    merged_recv,
    resid_send,
    resid_recv,
    normed_send,
    normed_recv,
    scale_send,
    scale_recv,
):
    sp, tp = lax.axis_index("sp"), lax.axis_index("tp")
    z, core = tp // 2, tp % 2
    channels, width = out_proj.shape
    rows = resid.shape[0]
    half, subs = rows // 2, rows // SUB
    first = half // SUB
    planes = tp_count // 2
    near_of = [sp ^ 1, sp ^ 2]
    diagonal = sp ^ 3

    def remote(source, target, send_sem, recv_sem, to_sp, to_tp):
        return pltpu.make_async_remote_copy(
            src_ref=source,
            dst_ref=target,
            send_sem=send_sem,
            recv_sem=recv_sem,
            device_id=(to_sp, to_tp),
            device_id_type=MESH,
        )

    def send(source, target, send_sem, recv_sem, to_sp, to_tp):
        remote(source, target, send_sem, recv_sem, to_sp, to_tp).start()

    def left(region, send_sem):
        remote(region, region, send_sem, send_sem, near_of[0], tp).wait_send()

    def arrive(region, recv_sem):
        remote(region, region, recv_sem, recv_sem, near_of[0], tp).wait_recv()

    tail = conv_in.shape[1] - SUB
    loads = [
        pltpu.make_async_copy(conv_in, in_buf.at[:, pl.ds(SUB, conv_in.shape[1])], local_sem.at[0]),
        pltpu.make_async_copy(in_gate, gate_buf.at[:, pl.ds(SUB, conv_in.shape[1])], local_sem.at[1]),
        pltpu.make_async_copy(out_gate, after_buf, local_sem.at[2]),
        pltpu.make_async_copy(doc_ids, doc_buf.at[:, pl.ds(SUB, conv_in.shape[1])], local_sem.at[3]),
        pltpu.make_async_copy(taps_in, taps, local_sem.at[6]),
        pltpu.make_async_copy(gain_in, gain, local_sem.at[7]),
        pltpu.make_async_copy(
            out_proj, proj.at[pl.ds(pl.multiple_of(tp * channels, channels), channels)], local_sem.at[4]
        ),
        pltpu.make_async_copy(resid, resid_buf, local_sem.at[5]),
        pltpu.make_async_copy(norm_gain_in, norm_gain, local_sem.at[8]),
        pltpu.make_async_copy(ids, ids_out.at[0], local_sem.at[9]),
        pltpu.make_async_copy(weights, weights_out.at[0], local_sem.at[10]),
    ]
    for copy in loads:
        copy.start()

    barrier = pltpu.get_barrier_semaphore()
    for d in range(1, tp_count):
        pl.semaphore_signal(barrier, inc=1, device_id=(sp, tp ^ d), device_id_type=MESH)
    for d in range(1, 4):
        pl.semaphore_signal(barrier, inc=1, device_id=(sp ^ d, tp), device_id_type=MESH)
    pl.semaphore_wait(barrier, tp_count + 2)

    after, before = (sp + 1) % 4, (sp + 3) % 4
    edge = pl.ds(0, SUB)
    send(
        doc_ids.at[:, pl.ds(tail, SUB)],
        doc_buf.at[:, edge],
        edge_send.at[0],
        edge_recv.at[0],
        after,
        tp,
    )

    eighth = width // 8

    def columns(place, side):
        return pl.ds(pl.multiple_of(place * (2 * eighth) + side * eighth, eighth), eighth)

    my_rows = pl.ds(pl.multiple_of(tp * channels, channels), channels)
    early = EARLY
    slices = []
    for d in range(2, tp_count):
        side = core ^ (d & 1)
        copy = remote(
            out_proj.at[:, columns(sp, side)],
            proj.at[my_rows, columns(sp, side)],
            slice_send.at[1],
            slice_recv.at[d // 2],
            sp,
            tp ^ d,
        )
        slices.append(copy)

    for copy in slices:
        copy.start()
    for k in range(2):
        send(
            resid.at[pl.ds(rows - early, early)],
            early_resid.at[k],
            resid_send.at[0],
            resid_recv.at[0],
            near_of[k],
            tp,
        )
    send(out_proj, proj.at[my_rows], slice_send.at[0], slice_recv.at[0], sp, tp ^ 1)
    for d in range(1, 4):
        send(ids, ids_out.at[d], list_send.at[0], list_recv.at[0], sp ^ d, tp)
        send(weights, weights_out.at[d], list_send.at[1], list_recv.at[1], sp ^ d, tp)
    for copy in loads[:6]:
        copy.wait()
    for k in range(3):
        spread[k] = jnp.broadcast_to(taps[k : k + 1, :], (channels, channels)).T
    spread[3] = jnp.broadcast_to(gain[...], (channels, channels)).T
    for at, source in enumerate((in_buf, gate_buf)):
        last = source[:, pl.ds(tail + SUB, SUB)].astype(jnp.float32).T
        tails[0, at] = last[SUB - 8 :].astype(jnp.bfloat16)
    send(tails.at[0], tails.at[1], edge_send.at[1], edge_recv.at[1], after, tp)
    def piece(owner, q):
        base = pl.multiple_of(owner * rows + q * SUB, SUB)
        wide = pl.ds(base, 2 * SUB)
        gated = gate_buf[:, wide].astype(jnp.float32) * in_buf[:, wide].astype(jnp.float32)
        docs = jnp.broadcast_to(doc_buf[:, wide], (8, 2 * SUB))
        now = docs[:, SUB:]
        same_one = (pltpu.roll(docs, 1, 1)[:, SUB:] == now).astype(jnp.float32)[:1]
        same_two = (pltpu.roll(docs, 2, 1)[:, SUB:] == now).astype(jnp.float32)[:1]
        conv = (
            spread[2] * gated[:, SUB:]
            + spread[1] * (pltpu.roll(gated, 1, 1)[:, SUB:] * same_one)
            + spread[0] * (pltpu.roll(gated, 2, 1)[:, SUB:] * same_two)
        )
        gated_out = after_buf[:, pl.ds(base, SUB)].astype(jnp.float32) * conv
        by_head = gated_out.reshape(channels // HEAD, HEAD, SUB)
        by_head = by_head * lax.rsqrt(
            jnp.mean(by_head * by_head, axis=1, keepdims=True) + norm_eps
        )
        normed = by_head.reshape(channels, SUB) * spread[3]
        return normed.T.astype(jnp.bfloat16)

    my_channels = pl.ds(pl.multiple_of(tp * channels, channels), channels)

    def trade(q, d):
        return remote(
            outgoing.at[q, d],
            by_row.at[q, :, my_channels],
            trade_send.at[q],
            trade_recv.at[q],
            sp,
            tp ^ d,
        )

    def start_trade(q):
        def begin(at, carry):
            trade(q, tp_count - 1 - at).start()
            return carry

        lax.fori_loop(0, tp_count - 1, begin, 0)

    def sent_trade(q):
        left(outgoing.at[q, pl.ds(1, tp_count - 1)], trade_send.at[q])

    def block_rows(step):
        deep = 2 * channels
        return pl.ds(pl.multiple_of((z ^ step) * deep, deep), deep)

    def part_rows(step, upper):
        deep = 2 * channels
        return pl.ds(pl.multiple_of((z ^ step) * deep + upper * channels, channels), channels)

    def spread_slice(step):
        region = proj.at[block_rows(step), columns(sp, core)]
        arrive(region, slice_recv.at[step])
        for k in range(2):
            send(region, region, plane_send.at[0], plane_recv.at[k, step - 1], near_of[k], tp)
        send(region, region, core_send.at[0], core_recv.at[0], sp, tp ^ 1)

    def spread_plane(step):
        for k in range(2):
            region = proj.at[block_rows(step), columns(near_of[k], core)]
            arrive(region, plane_recv.at[k, step - 1])
            part = proj.at[part_rows(step, k), columns(near_of[k], core)]
            send(part, part, corner_send.at[0], corner_recv.at[step - 1], near_of[1 - k], tp)
            send(region, region, core_send.at[0], core_recv.at[1 + k], sp, tp ^ 1)

    def spread_corner(step):
        region = proj.at[block_rows(step), columns(diagonal, core)]
        arrive(region, corner_recv.at[step - 1])
        send(region, region, core_send.at[0], core_recv.at[3], sp, tp ^ 1)

    places = (sp, near_of[0], near_of[1], diagonal)

    def other_half(k):
        arrive(proj.at[pl.ds(0, (planes - 1) * channels // 4)], core_recv.at[k])

    order = [1, 0, *range(2, subs)]

    def convolve(q):
        def one(at, carry):
            d = tp_count - 1 - at
            outgoing[q, d] = piece(tp ^ d, q)
            return carry

        lax.fori_loop(0, tp_count - 1, one, 0)
        by_row[q, :, my_channels] = piece(tp, q)

    convolve(1)
    for step in range(1, planes):
        spread_slice(step)
    left(proj.at[pl.ds(0, 2 * (planes - 1) * channels // 8)], slice_send.at[1])
    start_trade(order[0])
    arrive(doc_buf.at[:, edge], edge_recv.at[0])
    arrive(tails.at[1], edge_recv.at[1])
    for at, target in enumerate((in_buf, gate_buf)):
        filler = jnp.zeros((SUB - 8, channels), jnp.float32)
        last = jnp.concatenate([filler, tails[1, at].astype(jnp.float32)], axis=0)
        target[:, edge] = last.T.astype(jnp.bfloat16)
    doc_buf[:, edge] = jnp.where(sp == 0, -1, doc_buf[:, edge])
    convolve(0)
    for step in range(1, planes):
        spread_plane(step)

    tile = width // 4
    local_experts, _, hidden_width = w_gate.shape
    slot = table.shape[2] // local_experts

    def load_weights(at):
        side, expert = at % 2, at % local_experts
        return [
            pltpu.make_async_copy(source.at[expert], target.at[side], weight_sem.at[k, side])
            for k, (source, target) in enumerate(
                ((w_gate, gate_now), (w_up, up_now), (w_down, down_now))
            )
        ]

    for at in range(2):
        for copy in load_weights(at):
            copy.start()

    def make_tables():
        arrive(ids_out.at[pl.ds(1, 3)], list_recv.at[0])
        arrive(weights_out.at[pl.ds(1, 3)], list_recv.at[1])
        deep = marks.shape[2]
        line = lax.broadcasted_iota(jnp.int32, (deep, half), 0)
        experts = sp * local_experts + line
        ahead = (
            lax.broadcasted_iota(jnp.int32, (half, half), 0)
            < lax.broadcasted_iota(jnp.int32, (half, half), 1)
        ).astype(jnp.bfloat16)
        for b in range(2):
            for n in range(4):
                hits, amount = jnp.zeros((deep, half)), jnp.zeros((deep, half))
                for k in range(ids.shape[0]):
                    here = pl.ds(b * half, half)
                    hit = (ids_out[n, pl.ds(k, 1), here] == experts) & (line < local_experts)
                    hits = hits + hit.astype(jnp.float32)
                    amount = amount + jnp.where(hit, weights_out[n, pl.ds(k, 1), here], 0.0)
                marks[b, n] = hits
                share[b, n] = amount
            flat = marks[b].reshape(4 * deep, half)
            order_of = jnp.dot(flat.astype(jnp.bfloat16), ahead, preferred_element_type=jnp.float32)
            rank[b] = jnp.where(flat > 0, order_of, -1.0).reshape(4, deep, half)

            def fill(n, carry, b=b):
                spots = lax.broadcasted_iota(jnp.int32, (slot, half), 0).astype(jnp.float32)
                for e in range(local_experts):
                    chosen = rank[b, n, pl.ds(e, 1), :] == spots
                    table[b, n, pl.ds(e * slot, slot), :] = chosen.astype(jnp.float32).astype(
                        jnp.bfloat16
                    )
                    total = jnp.sum(
                        jnp.where(chosen, share[b, n, pl.ds(e, 1), :], 0.0), axis=1, keepdims=True
                    )
                    slot_weight[b, e, pl.ds(pl.multiple_of(n * slot, slot), slot), :] = (
                        jnp.broadcast_to(total, (slot, slot_weight.shape[3]))
                    )
                return carry

            lax.fori_loop(0, 4, fill, 0)

    def early_region(place, k):
        part = pl.ds(half - early + k * (early // 2), early // 2)
        return gathered.at[1, place, part]

    def project_early():
        arrive(early_resid, resid_recv.at[0])
        arrive(early_normed, normed_recv.at[0])
        deep = 2 * early

        def stream_of(n):
            cols = pl.ds(pl.multiple_of(n * tile, tile), tile)
            value = early_resid[:, :, cols].astype(jnp.float32).reshape(deep, tile)
            return cols, value + jnp.dot(
                early_normed[...].reshape(deep, tp_count * channels),
                proj[:, cols],
                preferred_element_type=jnp.float32,
            )

        def project(n, total):
            value = stream_of(n)[1]
            return total + jnp.sum(value * value, axis=1, keepdims=True)

        total = lax.fori_loop(0, 4, project, jnp.zeros((deep, 1), jnp.float32))
        scale = lax.rsqrt(total / width + norm_eps)

        def normalize(n, carry):
            cols, value = stream_of(n)
            value = (value * scale * norm_gain[:, cols]).astype(jnp.bfloat16)
            for k in range(2):
                gathered[1, 1 + k, pl.ds(half - early, early), cols] = value[
                    k * early : (k + 1) * early
                ]
            return carry

        lax.fori_loop(0, 4, normalize, 0)
        for k in range(2):
            send(
                early_region(1 + k, k),
                early_region(3, k),
                normed_send.at[1],
                normed_recv.at[1],
                near_of[1 - k],
                tp,
            )

    def span(q):
        return SUB - early if q == subs - 1 else SUB

    def near_region(place, q):
        return gathered.at[q // first, place, pl.ds(q % first * SUB, span(q))]

    def far_region(q, k, place=3):
        part = span(q) // 2
        return gathered.at[q // first, place, pl.ds(q % first * SUB + k * part, part)]

    def got_rows(q):
        arrive(by_row.at[q, :, pl.ds(0, (tp_count - 1) * channels)], trade_recv.at[q])

    def project_tile(q, place):
        mine = pl.ds(q * SUB, SUB)
        cols = pl.ds(pl.multiple_of(place * tile, tile), tile)
        value = resid_buf[mine, cols].astype(jnp.float32) + jnp.dot(
            by_row[q], proj[:, cols], preferred_element_type=jnp.float32
        )
        stream[mine, cols] = value
        return jnp.sum(value * value, axis=1, keepdims=True)

    def normalize_rows(q, total):
        mine = pl.ds(q * SUB, SUB)
        there = pl.ds(q % first * SUB, SUB)
        scale = lax.rsqrt(total / width + norm_eps)

        def normalize(n, carry):
            cols = pl.ds(pl.multiple_of(n * tile, tile), tile)
            value = (stream[mine, cols] * scale * norm_gain[:, cols]).astype(jnp.bfloat16)
            gathered[q // first, 0, there, cols] = value
            return carry

        lax.fori_loop(0, 4, normalize, 0)

    def project_rows(q):
        got_rows(q)
        total = lax.fori_loop(
            0, 4, lambda n, total: total + project_tile(q, n), jnp.zeros((SUB, 1), jnp.float32)
        )
        normalize_rows(q, total)

    def spread_tile(q, place):
        cols = pl.ds(pl.multiple_of(place * tile, tile), tile)
        there = pl.ds(q % first * SUB, SUB)
        value = stream[pl.ds(q * SUB, SUB), cols] * norm_gain[:, cols]
        gathered[q // first, 0, there, cols] = value.astype(jnp.bfloat16)
        for k in range(2):
            send(
                gathered.at[q // first, 0, there, cols],
                gathered.at[q // first, 1 + k, there, cols],
                near_send.at[q],
                near_recv.at[k, q],
                near_of[k],
                tp,
            )

    def send_scales(total):
        scale = jnp.broadcast_to(lax.rsqrt(total / width + norm_eps), (SUB, SUB))
        scales[0] = scale.T[:8]
        for d in range(1, 4):
            send(scales.at[0], scales.at[d], scale_send.at[0], scale_recv.at[0], sp ^ d, tp)

    def place_scales():
        arrive(scales.at[pl.ds(1, 3)], scale_recv.at[0])

        def fill(n, carry):
            ones = jnp.ones((1, SUB), jnp.float32)
            line = jnp.concatenate(
                [scales[n, 0:1, :] if q == order[0] else ones for q in range(first)], axis=1
            )
            lanes = lax.broadcasted_iota(jnp.int32, (slot, slot_weight.shape[3]), 1)
            for e in range(local_experts):
                chosen = table[0, n, pl.ds(e * slot, slot), :].astype(jnp.float32)
                total = jnp.sum(chosen * line, axis=1, keepdims=True)
                here = pl.ds(pl.multiple_of(n * slot, slot), slot)
                slot_weight[0, e, here, :] = jnp.where(
                    lanes < slot_weight.shape[3] // 2, slot_weight[0, e, here, :], total
                )
            return carry

        lax.fori_loop(0, 4, fill, 0)

    def spread_rows(q):
        for k in range(2):
            send(
                near_region(0, q),
                near_region(1 + k, q),
                near_send.at[q],
                near_recv.at[k, q],
                near_of[k],
                tp,
            )

    def relay_rows(q):
        for k in range(2):
            arrive(near_region(1 + k, q), near_recv.at[k, q])
            send(
                far_region(q, k, 1 + k),
                far_region(q, k),
                far_send.at[q],
                far_recv.at[q],
                near_of[1 - k],
                tp,
            )

    def far_rows(q):
        arrive(near_region(3, q), far_recv.at[q])

    def run_experts(b, between=None):
        def pack(at, carry):
            n, cols = at // 4, pl.ds(pl.multiple_of(at % 4 * tile, tile), tile)
            rows_in = jnp.dot(
                table[b, n], gathered[b, n, :, cols], preferred_element_type=jnp.float32
            ).astype(jnp.bfloat16)
            for e in range(local_experts):
                packed[e, pl.ds(pl.multiple_of(n * slot, slot), slot), cols] = rows_in[
                    e * slot : (e + 1) * slot
                ]
            return carry

        lax.fori_loop(0, 16, pack, 0)

        def expert(e, carry):
            at = b * local_experts + e
            side = at % 2
            for copy in load_weights(at):
                copy.wait()
            piece_width = hidden_width // 2

            def up(c, carry):
                cols = pl.ds(pl.multiple_of(c * piece_width, piece_width), piece_width)
                gate = jnp.dot(
                    packed[e], gate_now[side, :, cols], preferred_element_type=jnp.float32
                )
                value = jnp.dot(
                    packed[e], up_now[side, :, cols], preferred_element_type=jnp.float32
                )
                if b == 0:
                    middle = slot_weight.shape[3] // 2
                    factor = slot_weight[b, e, :, middle : middle + 1]
                    gate, value = gate * factor, value * factor
                hidden[:, cols] = (gate / (1.0 + jnp.exp(-gate)) * value).astype(jnp.bfloat16)
                return carry

            lax.fori_loop(0, 2, up, 0)

            def down(c, carry):
                cols = pl.ds(pl.multiple_of(c * tile, tile), tile)
                value = jnp.dot(
                    hidden[...], down_now[side, :, cols], preferred_element_type=jnp.float32
                )
                packed[e, :, cols] = (value * slot_weight[b, e, :, 0:1]).astype(jnp.bfloat16)
                return carry

            lax.fori_loop(0, 4, down, 0)

            @pl.when(at + 2 < 2 * local_experts)
            def _():
                for copy in load_weights(at + 2):
                    copy.start()

            return carry

        middle = local_experts if between is None else local_experts // 2
        lax.fori_loop(0, middle, expert, 0)
        if between is not None:
            between()
            lax.fori_loop(middle, local_experts, expert, 0)

    def combine(b, n):
        def one(c, carry):
            cols = pl.ds(pl.multiple_of(c * tile, tile), tile)
            pieces = jnp.concatenate(
                [packed[e, pl.ds(n * slot, slot), cols] for e in range(local_experts)], axis=0
            )
            partial[b, n, :, cols] = lax.dot_general(
                table[b, n], pieces, (((0,), (0,)), ((), ())), preferred_element_type=jnp.float32
            ).astype(jnp.bfloat16)
            return carry

        lax.fori_loop(0, 4, one, 0)

    part_of = [pl.ds(k * (half // 2), half // 2) for k in range(2)]

    def send_first(b):
        for k in range(2):
            send(
                partial.at[b, 3, part_of[k]],
                inbox.at[b, k],
                first_send.at[b],
                first_recv.at[b, k],
                near_of[k],
                tp,
            )

    def send_straight(b):
        for k in range(2):
            send(
                partial.at[b, 1 + k, part_of[k]],
                back.at[b, k, part_of[k]],
                back_send.at[b],
                straight_recv.at[b],
                near_of[k],
                tp,
            )

    strip = 32

    def merge(b):
        for k in range(2):
            arrive(inbox.at[b, k], first_recv.at[b, k])

            def add(at, carry, k=k):
                there = pl.ds(pl.multiple_of(k * (half // 2) + at * strip, strip), strip)
                here = pl.ds(pl.multiple_of(at * strip, strip), strip)
                partial[b, 2 - k, there, :] = (
                    partial[b, 2 - k, there, :].astype(jnp.float32)
                    + inbox[b, k, here, :].astype(jnp.float32)
                ).astype(jnp.bfloat16)
                return carry

            lax.fori_loop(0, half // 2 // strip, add, 0)
            send(
                partial.at[b, 2 - k, part_of[k]],
                back.at[b, 1 - k, part_of[k]],
                back_send.at[b],
                merged_recv.at[b],
                near_of[1 - k],
                tp,
            )

    def finish(b):
        arrive(back.at[b, 0], straight_recv.at[b])
        arrive(back.at[b, 1], merged_recv.at[b])
        for k in range(2):

            def add(at, carry, k=k):
                here = pl.ds(pl.multiple_of(k * (half // 2) + at * strip, strip), strip)
                there = pl.ds(pl.multiple_of(b * half + k * (half // 2) + at * strip, strip), strip)
                value = stream[there, :] + partial[b, 0, here, :].astype(jnp.float32)
                value = value + back[b, 0, here, :].astype(jnp.float32)
                (out_low, out_high)[b][here, :] = (
                    value + back[b, 1, here, :].astype(jnp.float32)
                ).astype(jnp.bfloat16)
                return carry

            lax.fori_loop(0, half // 2 // strip, add, 0)

    got_rows(order[0])
    sent_trade(order[0])
    start_trade(order[1])
    for copy in loads[6:]:
        copy.wait()
    arrive(
        proj.at[pl.ds(pl.multiple_of((tp ^ 1) * channels, channels), channels)],
        slice_recv.at[0],
    )
    total = jnp.zeros((SUB, 1), jnp.float32)
    for k in range(4):
        if k == 3:
            for step in range(1, planes):
                spread_corner(step)
        other_half(k)
        total = total + project_tile(order[0], places[k])
        spread_tile(order[0], places[k])
    send_scales(total)
    make_tables()
    for q in range(2, subs):
        convolve(q)
    for at_q in range(1, first):
        sent_trade(order[at_q])
        if at_q + 1 < subs:
            start_trade(order[at_q + 1])
        project_rows(order[at_q])
        spread_rows(order[at_q])
    for at_q in range(first):
        relay_rows(order[at_q])
        late = order[first + at_q]
        sent_trade(late)
        if first + at_q + 1 < subs:
            start_trade(order[first + at_q + 1])
        project_rows(late)
    left(near_region(0, order[0]), far_send.at[order[0]])
    spread_rows(order[first])
    for at_q in range(first):
        far_rows(order[at_q])
    for at_q in range(1, first):
        spread_rows(order[first + at_q])
    for k in range(2):
        send(
            by_row.at[subs - 1, pl.ds(SUB - early, early)],
            early_normed.at[k],
            normed_send.at[0],
            normed_recv.at[0],
            near_of[k],
            tp,
        )
    place_scales()
    run_experts(0, lambda: relay_rows(order[first]))
    combine(0, 3)
    send_first(0)
    for at_q in range(1, first):
        relay_rows(order[first + at_q])
    project_early()
    combine(0, 1)
    combine(0, 2)
    send_straight(0)
    combine(0, 0)
    merge(0)
    for at_q in range(first):
        far_rows(order[first + at_q])
    arrive(gathered.at[1, 3, pl.ds(half - early, early)], normed_recv.at[1])
    run_experts(1)
    combine(1, 3)
    send_first(1)
    combine(1, 1)
    combine(1, 2)
    send_straight(1)
    combine(1, 0)
    finish(0)
    merge(1)
    finish(1)
    left(doc_buf.at[:, edge], edge_send.at[0])
    left(tails.at[0], edge_send.at[1])
    left(ids_out.at[pl.ds(1, 3)], list_send.at[0])
    left(weights_out.at[pl.ds(1, 3)], list_send.at[1])
    left(proj.at[my_rows], slice_send.at[0])
    left(proj.at[pl.ds(0, (planes - 1) * channels // 2)], plane_send.at[0])
    left(proj.at[pl.ds(0, (planes - 1) * channels // 4)], corner_send.at[0])
    left(proj.at[pl.ds(0, (planes - 1) * channels)], core_send.at[0])
    left(early_resid, resid_send.at[0])
    left(scales.at[pl.ds(1, 3)], scale_send.at[0])
    left(early_normed, normed_send.at[0])
    left(gathered.at[1, 3, pl.ds(half - early, early)], normed_send.at[1])
    for q in range(subs):
        left(
            gathered.at[q // first, pl.ds(0, 2), pl.ds(q % first * SUB, span(q))],
            near_send.at[q],
        )
        if q != order[0]:
            left(near_region(0, q), far_send.at[q])
    left(partial.at[0, 3], first_send.at[0])
    left(partial.at[1, 3], first_send.at[1])
    for b in range(2):
        left(back.at[b], back_send.at[b])


def front(
    conv_in, in_gate, out_gate, doc_ids, conv_taps, head_gain, out_proj, resid, norm_gain,
    route_ids, route_weight, w_gate, w_up, w_down,
):
    tp_count = lax.axis_size("tp")
    channels, width = out_proj.shape
    positions = conv_in.shape[1]
    rows = resid.shape[0]
    half, subs = rows // 2, rows // SUB
    first, planes = half // SUB, tp_count // 2
    top = route_ids.shape[1]
    local_experts, _, hidden_width = w_gate.shape
    slot = max(2, rows // 8)
    hbm = pl.BlockSpec(memory_space=pltpu.HBM)
    dma = pltpu.SemaphoreType.DMA
    return pl.pallas_call(
        functools.partial(front_kernel, tp_count),
        out_shape=[pltpu.VMEM((half, width), jnp.bfloat16)] * 2,
        in_specs=[hbm] * 14,
        out_specs=[pl.BlockSpec(memory_space=pltpu.VMEM)] * 2,
        scratch_shapes=[
            pltpu.VMEM((4, top, rows), jnp.int32),
            pltpu.VMEM((4, top, rows), jnp.float32),
            pltpu.VMEM((channels, SUB + positions), jnp.bfloat16),
            pltpu.VMEM((channels, SUB + positions), jnp.bfloat16),
            pltpu.VMEM((channels, positions), jnp.bfloat16),
            pltpu.VMEM((1, SUB + positions), jnp.int32),
            pltpu.VMEM((3, channels), jnp.float32),
            pltpu.VMEM((1, channels), jnp.float32),
            pltpu.VMEM((1, width), jnp.float32),
            pltpu.VMEM((tp_count * channels, width), jnp.bfloat16),
            pltpu.VMEM((rows, width), jnp.bfloat16),
            pltpu.VMEM((4, channels, SUB), jnp.float32),
            pltpu.VMEM((subs, tp_count, SUB, channels), jnp.bfloat16),
            pltpu.VMEM((subs, SUB, tp_count * channels), jnp.bfloat16),
            pltpu.VMEM((2, 4, half, width), jnp.bfloat16),
            pltpu.VMEM((rows, width), jnp.float32),
            pltpu.VMEM((2, width, hidden_width), jnp.bfloat16),
            pltpu.VMEM((2, width, hidden_width), jnp.bfloat16),
            pltpu.VMEM((2, hidden_width, width), jnp.bfloat16),
            pltpu.VMEM((2, 4, 8, half), jnp.float32),
            pltpu.VMEM((2, 4, 8, half), jnp.float32),
            pltpu.VMEM((2, 4, 8, half), jnp.float32),
            pltpu.VMEM((2, 4, local_experts * slot, half), jnp.bfloat16),
            pltpu.VMEM((2, local_experts, 4 * slot, 128), jnp.float32),
            pltpu.VMEM((local_experts, 4 * slot, width), jnp.bfloat16),
            pltpu.VMEM((4 * slot, hidden_width), jnp.bfloat16),
            pltpu.VMEM((2, 4, half, width), jnp.bfloat16),
            pltpu.VMEM((2, 2, half // 2, width), jnp.bfloat16),
            pltpu.VMEM((2, 2, half, width), jnp.bfloat16),
            pltpu.VMEM((2, EARLY, width), jnp.bfloat16),
            pltpu.VMEM((2, EARLY, tp_count * channels), jnp.bfloat16),
            pltpu.VMEM((4, 8, SUB), jnp.float32),
            pltpu.VMEM((2, 2, 8, SUB), jnp.bfloat16),
            dma((11,)),
            dma((2,)),
            dma((2,)),
            dma((2,)),
            dma((2,)),
            dma((2,)),
            dma((planes,)),
            dma((1,)),
            dma((2, planes - 1)),
            dma((1,)),
            dma((planes - 1,)),
            dma((1,)),
            dma((4,)),
            dma((subs,)),
            dma((subs,)),
            dma((subs,)),
            dma((2, subs)),
            dma((subs,)),
            dma((subs,)),
            dma((3, 2)),
            dma((2,)),
            dma((2, 2)),
            dma((2,)),
            dma((2,)),
            dma((2,)),
            dma((1,)),
            dma((1,)),
            dma((2,)),
            dma((2,)),
            dma((1,)),
            dma((1,)),
        ],
        compiler_params=pltpu.CompilerParams(
            collective_id=0, has_side_effects=True, vmem_limit_bytes=59944 * 1024
        ),
        name="front",
    )(
        conv_in,
        in_gate,
        out_gate,
        doc_ids[None],
        conv_taps.T,
        head_gain[None],
        out_proj,
        resid,
        norm_gain[None],
        route_ids.T,
        route_weight.T,
        w_gate,
        w_up,
        w_down,
    )


def body(
    conv_in,
    in_gate,
    out_gate,
    doc_ids,
    conv_taps,
    head_gain,
    out_proj,
    resid,
    norm_gain,
    route_ids,
    route_weight,
    w_gate,
    w_up,
    w_down,
):
    channels, width = out_proj.shape
    rows = resid.shape[0]
    half = rows // 2
    slot = max(2, rows // 8)
    sp_count, tp_count = lax.axis_size("sp"), lax.axis_size("tp")
    local_experts = w_gate.shape[0]
    if (
        sp_count == 4
        and tp_count >= 4
        and tp_count & (tp_count - 1) == 0
        and channels == SUB
        and channels % HEAD == 0
        and width % 1024 == 0
        and rows % (2 * SUB) == 0
        and conv_in.shape[1] == tp_count * rows
        and rows <= 2 * local_experts * slot
    ):
        halves = front(
            conv_in,
            in_gate,
            out_gate,
            doc_ids,
            conv_taps,
            head_gain,
            out_proj,
            resid,
            norm_gain,
            route_ids,
            route_weight,
            w_gate,
            w_up,
            w_down,
        )
        return jnp.concatenate(halves, axis=0)
    gated_in = in_gate.astype(jnp.float32) * conv_in.astype(jnp.float32)
    doc_value = doc_ids.astype(jnp.float32)
    edge = jnp.concatenate([gated_in[:, -2:], doc_value[None, -2:]], axis=0)
    edge = shifted(edge, "sp", 1)
    earlier_in, earlier_doc = edge[:-1], edge[-1]
    padded_in = jnp.concatenate([earlier_in, gated_in], axis=1)
    padded_doc = jnp.concatenate([earlier_doc, doc_value])
    same_one = (padded_doc[1:-1] == doc_value).astype(jnp.float32)
    same_two = (padded_doc[:-2] == doc_value).astype(jnp.float32)
    conv_out = (
        conv_taps[:, 2:3] * gated_in
        + conv_taps[:, 1:2] * (padded_in[:, 1:-1] * same_one)
        + conv_taps[:, 0:1] * (padded_in[:, :-2] * same_two)
    )
    gated_out = out_gate.astype(jnp.float32) * conv_out
    by_head = gated_out.reshape(channels // HEAD, HEAD, -1)
    by_head = by_head * lax.rsqrt(jnp.mean(by_head * by_head, axis=1, keepdims=True) + norm_eps)
    head_normed = (by_head.reshape(channels, -1) * head_gain[:, None]).astype(jnp.bfloat16)
    by_row = lax.all_to_all(head_normed, "tp", split_axis=1, concat_axis=0, tiled=True)
    mixed = lax.dot_general(
        by_row,
        lax.all_gather(out_proj, "tp", axis=0, tiled=True),
        (((0,), (0,)), ((), ())),
        preferred_element_type=jnp.float32,
    )
    stream = resid.astype(jnp.float32) + mixed
    expert_in = (
        stream * lax.rsqrt(jnp.mean(stream * stream, axis=1, keepdims=True) + norm_eps) * norm_gain
    ).astype(jnp.bfloat16)
    experts_total = local_experts * sp_count
    parts = []
    for block_no in range(2):
        block_ids = route_ids[block_no * half : (block_no + 1) * half]
        place = slot_places(block_ids, slot, experts_total)
        send = pack_rows(
            place, expert_in[block_no * half : (block_no + 1) * half], experts_total * slot
        ).reshape(sp_count, local_experts, slot, width)
        arrived = lax.all_to_all(send, "sp", split_axis=0, concat_axis=0, tiled=True)
        gate_part = jnp.einsum(
            "nesd,edf->nesf", arrived, w_gate, preferred_element_type=jnp.float32
        )
        up_part = jnp.einsum("nesd,edf->nesf", arrived, w_up, preferred_element_type=jnp.float32)
        hidden = (jax.nn.silu(gate_part) * up_part).astype(jnp.bfloat16)
        arrived = jnp.einsum(
            "nesf,efd->nesd", hidden, w_down, preferred_element_type=jnp.float32
        ).astype(jnp.bfloat16)
        returned = lax.all_to_all(arrived, "sp", split_axis=0, concat_axis=0, tiled=True).reshape(
            experts_total * slot, width
        )
        parts.append(
            combine_rows(returned, place, route_weight[block_no * half : (block_no + 1) * half])
        )
    mixture = jnp.concatenate(parts, axis=0)
    return (stream + mixture).astype(jnp.bfloat16)


def solution(mesh):
    return jax.shard_map(
        body,
        mesh=mesh,
        in_specs=(
            P("tp", "sp"),
            P("tp", "sp"),
            P("tp", "sp"),
            P("sp"),
            P("tp", None),
            P("tp"),
            P("tp", None),
            P(("sp", "tp"), None),
            P(),
            P(("sp", "tp"), None),
            P(("sp", "tp"), None),
            P("sp", None, None),
            P("sp", None, None),
            P("sp", None, None),
        ),
        out_specs=P(("sp", "tp"), None),
        check_vma=False,
    )
```
